32 devices in a mesh: sp: 8 (over z, x), tp: 4 (over y, core).
Axes of the slice: x: 2, y: 2, z: 4, core: 2. Of those that a mesh axis runs over, the one named last changes fastest.
Arguments:
- layer_input: bfloat16 [4, 2048, 2048], P(None, ('sp', 'tp')), as said below
- key_weight: bfloat16 [2048, 384], replicated, may hold values from -0.125 to 0.125
- value_weight: bfloat16 [2048, 384], replicated, may hold values from -0.125 to 0.125
- queries: bfloat16 [24, 5, 64], P('sp'), may hold values from -6 to 6
- head_bias: float32 [6, 5], replicated, as said below
Outputs:
- stored: bfloat16 [24, 8, 256, 128], P('sp', None, 'tp')
- first_read: bfloat16 [24, 320], P('sp')
The draws below stay inside these ranges and needn't reach their ends.
Inputs may be any that keep to these rules, and one draw needn't show every extreme that they name: `layer_input`: entries lie between -12.5 and 12.5. `head_bias`: entries lie between -1 minus the natural logarithm of 2048 and -3.
All inputs are finite; a program needn't handle non-finite values.
Results may differ from the reference program's by a relative error of at most 0.01.
Values may be sent and summed in bfloat16 or wider, within the bound.
A program may use at most 64 MiB of HBM per device.

```python
import math
import jax
import jax.numpy as jnp
from jax import lax

D = 2048
HD = 64
KVH = 6
GROUP = 5
SUB = 64
SEQS = 4
PAIRS = 24
LEN = 2048
BLOCKS = 8
SPAN = 256


def draw_layer_input(key, part):
    base_key, scale_key = jax.random.split(key)
    blocks = LEN // SUB
    log_scale = jax.random.uniform(scale_key, (SEQS, blocks, 1, 1), jnp.float32, -0.7, 0.7)
    base = jnp.clip(jax.random.normal(base_key, (SEQS, blocks, SUB, D), jnp.float32), -6.0, 6.0)
    return (base * jnp.exp(log_scale)).reshape(SEQS, LEN, D).astype(jnp.bfloat16)


def draw_head_bias(key, part):
    kind_key, fast_key, slow_key = jax.random.split(key, 3)
    quick = jax.random.randint(kind_key, (KVH, GROUP), 0, 2) == 1
    fast = -math.log(40.0) + jax.random.uniform(fast_key, (KVH, GROUP), jnp.float32, -0.5, 0.5)
    slow = -math.log(LEN) - 0.5 + jax.random.uniform(slow_key, (KVH, GROUP), jnp.float32, -0.5, 0.5)
    return jnp.where(quick, fast, slow).astype(jnp.float32)


def shard_levels(rng, dims, cuts, least, top_value):
    def one(axis_at, parts):
        steps = jax.random.uniform(jax.random.fold_in(jax.random.fold_in(rng, 6), axis_at), (parts,), jnp.float32, least / len(cuts), top_value / len(cuts))
        return jnp.repeat(jnp.exp(steps), dims[axis_at] // parts).reshape((-1,) + (1,) * (len(dims) - axis_at - 1))

    level = one(*cuts[0])
    for cut in cuts[1:]:
        level = level * one(*cut)
    return level


def noise(own_key, dims, scale, most, cuts=(), held_as=jnp.bfloat16):
    factor_of = shard_levels(own_key, dims, cuts, -0.22, 0.18) if cuts else 1.0
    array = jax.random.normal(own_key, dims, jnp.float32) * scale * factor_of
    return jnp.minimum(jnp.maximum(array, -most), most).astype(held_as)


def setup_inputs(seed: int = 0) -> dict:
    streams_of = jax.random.split(jax.random.key(seed), 6)
    return {
        "layer_input": draw_layer_input(jax.random.fold_in(streams_of[5], 71), 0),
        "key_weight": noise(streams_of[1], (D, KVH * HD), D ** -0.5, 0.125),
        "value_weight": noise(streams_of[2], (D, KVH * HD), D ** -0.5, 0.125),
        "queries": noise(streams_of[3], (PAIRS, GROUP, HD), 1.0, 6.0, ((0, 8),)),
        "head_bias": draw_head_bias(jax.random.fold_in(streams_of[5], 71), 0),
    }


EPS_NORM = 0.0001

def reference(layer_input, key_weight, value_weight, queries, head_bias):
    tokens_flat = layer_input.reshape(SEQS * LEN, D)
    key_rows = jnp.dot(tokens_flat, key_weight, preferred_element_type=jnp.float32).astype(jnp.bfloat16).reshape(SEQS, LEN, KVH, HD)
    value_rows = jnp.dot(tokens_flat, value_weight, preferred_element_type=jnp.float32).astype(jnp.bfloat16).reshape(SEQS, LEN, KVH, HD)
    kv_rows = jnp.concatenate([key_rows, value_rows], axis=-1).transpose(0, 2, 1, 3).reshape(PAIRS, LEN, 2 * HD)
    head_shift = jnp.tile(head_bias, (SEQS, 1))
    score_scale = 1.0 / math.sqrt(HD)

    def read_pair(item):
        query, pair_rows, shift = item
        scores = jnp.dot(query, pair_rows[:, :HD].T, preferred_element_type=jnp.float32) * score_scale + shift[:, None]
        keep_log = jax.nn.log_sigmoid(-scores)
        suffix_log = lax.cumsum(keep_log, axis=1, reverse=True) - keep_log
        weights = jnp.exp(jax.nn.log_sigmoid(scores) + suffix_log).astype(jnp.bfloat16)
        return jnp.dot(weights, pair_rows[:, HD:], preferred_element_type=jnp.float32)
    summed = lax.map(read_pair, (queries, kv_rows, head_shift))
    squares = lax.optimization_barrier(jnp.mean(summed * summed, axis=-1, keepdims=True))
    first_read = (summed * lax.rsqrt(squares + EPS_NORM)).reshape(PAIRS, GROUP * HD).astype(jnp.bfloat16)
    return (kv_rows.reshape(PAIRS, BLOCKS, SPAN, 2 * HD), first_read)
```

```python
import functools
import math

import jax
import jax.numpy as jnp
from jax import lax
from jax.experimental import pallas as pl
from jax.experimental.pallas import tpu as pltpu
from jax.sharding import PartitionSpec as P

EPS_NORM = 0.0001
MESH = pl.DeviceIdType.MESH
KC = 4
VMEM_BYTES = 60 * 1024 * 1024
ROWS = 8


def flip(index, k):
    bit = 1
    while bit <= k:
        if k & bit:
            index = index + (1 - 2 * ((index // bit) % 2)) * bit
        bit *= 2
    return index


def packed_rows(pairs, group):
    return pairs * group // 8 * 8 + 8


def kernel(
    sp, tp, seqs, sub, hd, kvh, group, pairs,
    x_hbm, wk_hbm, wv_hbm, q_hbm, bias_hbm,
    recv, msg,
    x_v, wk_v, wv_v, q_v, bias_v, send,
    x_sem, w_sem, small_sem, send_sem, recv_sem, msend_sem, mrecv_sem,
):
    me = lax.axis_index("sp")
    mt = lax.axis_index("tp")
    per_seq = kvh // pairs
    width = x_hbm.shape[1]
    kc = width // KC
    half_rows = seqs * sub // 2

    barrier = pltpu.get_barrier_semaphore()
    for k in range(1, sp):
        pl.semaphore_signal(barrier, inc=1, device_id={"sp": flip(me, k)}, device_id_type=MESH)
    for k in range(1, tp):
        pl.semaphore_signal(barrier, inc=1, device_id={"tp": lax.rem(mt + k, tp)}, device_id_type=MESH)

    top = me // (sp // 2)
    far_row = pl.multiple_of((1 - top) * half_rows, half_rows)
    near_row = pl.multiple_of(top * half_rows, half_rows)

    x_far = pltpu.make_async_copy(x_hbm.at[pl.ds(far_row, half_rows)], x_v.at[pl.ds(far_row, half_rows)], x_sem.at[0])
    x_near = pltpu.make_async_copy(x_hbm.at[pl.ds(near_row, half_rows)], x_v.at[pl.ds(near_row, half_rows)], x_sem.at[1])
    x_far.start()
    w_copies = []
    for c in range(KC):
        rows = pl.ds(c * kc, kc)
        a = pltpu.make_async_copy(wk_hbm.at[rows], wk_v.at[rows], w_sem.at[0, c])
        b = pltpu.make_async_copy(wv_hbm.at[rows], wv_v.at[rows], w_sem.at[1, c])
        a.start()
        b.start()
        w_copies.append((a, b))
    x_near.start()
    q_copy = pltpu.make_async_copy(q_hbm, q_v, small_sem.at[0])
    bias_copy = pltpu.make_async_copy(bias_hbm, bias_v, small_sem.at[1])
    q_copy.start()
    bias_copy.start()

    def pieces(keys, values, i, part):
        out = []
        for p in range(pairs):
            c0 = (part * pairs + p) * hd
            out.append(keys[i * sub:(i + 1) * sub, c0:c0 + hd])
            out.append(values[i * sub:(i + 1) * sub, c0:c0 + hd])
        return jnp.concatenate(out, axis=1).astype(jnp.bfloat16)

    x_far.wait()
    keys = values = None
    for c in range(KC):
        w_copies[c][0].wait()
        w_copies[c][1].wait()
        xc = x_v[pl.ds(far_row, half_rows), c * kc:(c + 1) * kc]
        dk = jnp.dot(xc, wk_v[c * kc:(c + 1) * kc, :], preferred_element_type=jnp.float32)
        dv = jnp.dot(xc, wv_v[c * kc:(c + 1) * kc, :], preferred_element_type=jnp.float32)
        keys = dk if keys is None else keys + dk
        values = dv if values is None else values + dv
    far_base = (1 - top) * (sp // 2)
    for i in range(seqs // 2):
        for part in range(per_seq):
            send[pl.ds(far_base + i * per_seq + part, 1)] = pieces(keys, values, i, part)[None]

    pl.semaphore_wait(barrier, sp + tp - 2)

    def block_copy(to):
        return pltpu.make_async_remote_copy(
            src_ref=send.at[to], dst_ref=recv.at[me],
            send_sem=send_sem, recv_sem=recv_sem.at[me],
            device_id={"sp": to}, device_id_type=MESH,
        )

    def arrived(frm):
        return pltpu.make_async_remote_copy(
            src_ref=send.at[frm], dst_ref=recv.at[frm],
            send_sem=send_sem, recv_sem=recv_sem.at[frm],
            device_id={"sp": frm}, device_id_type=MESH,
        )

    for j in range(sp // 2):
        block_copy(far_base + flip(lax.rem(me, 2), j)).start()

    x_near.wait()
    xn = x_v[pl.ds(near_row, half_rows), :]
    keys = jnp.dot(xn, wk_v[...], preferred_element_type=jnp.float32)
    values = jnp.dot(xn, wv_v[...], preferred_element_type=jnp.float32)
    near_base = top * (sp // 2)
    for i in range(seqs // 2):
        for part in range(per_seq):
            send[pl.ds(near_base + i * per_seq + part, 1)] = pieces(keys, values, i, part)[None]
    for k in range(1, sp // 2):
        block_copy(flip(me, k)).start()
    recv[pl.ds(me, 1)] = send[pl.ds(me, 1)]

    q_copy.wait()
    bias_copy.wait()
    h0 = lax.rem(me * pairs, kvh)
    eye = lax.broadcasted_iota(jnp.int32, (ROWS, group), 0) == lax.broadcasted_iota(jnp.int32, (ROWS, group), 1)
    q_pads = []
    shifts = []
    for p in range(pairs):
        qp = q_v[:, p, :].astype(jnp.float32)
        qp = jnp.concatenate([qp, jnp.zeros((group, hd), jnp.float32)], axis=1)
        qp = jnp.concatenate([qp, jnp.zeros((ROWS - group, 2 * hd), jnp.float32)], axis=0)
        q_pads.append(qp.astype(jnp.bfloat16))
        row = bias_v[pl.ds(h0 + p, 1), :]
        shifts.append(jnp.sum(jnp.where(eye, jnp.broadcast_to(row, (ROWS, group)), 0.0), axis=1, keepdims=True))
    shift = jnp.concatenate(shifts, axis=0)
    scale = 1.0 / math.sqrt(hd)
    later = lax.broadcasted_iota(jnp.int32, (sub, 256), 0)
    column = lax.broadcasted_iota(jnp.int32, (sub, 256), 1)
    tri = ((later > column) | (column >= 128)).astype(jnp.float32).astype(jnp.bfloat16)
    left_half = lax.broadcasted_iota(jnp.int32, (pairs * ROWS, 2 * hd), 1) < hd

    def msg_copy(b, t):
        return pltpu.make_async_remote_copy(
            src_ref=msg.at[mt, b], dst_ref=msg.at[mt, b],
            send_sem=msend_sem, recv_sem=mrecv_sem.at[mt],
            device_id={"tp": t}, device_id_type=MESH,
        )

    def all_msgs(t):
        return pltpu.make_async_remote_copy(
            src_ref=msg.at[t], dst_ref=msg.at[t],
            send_sem=msend_sem, recv_sem=mrecv_sem.at[t],
            device_id={"tp": t}, device_id_type=MESH,
        )

    def attend(b):
        scores = []
        for p in range(pairs):
            kv = recv[b, :, p * 2 * hd:(p + 1) * 2 * hd]
            scores.append(lax.dot_general(q_pads[p], kv, (((1,), (1,)), ((), ())), preferred_element_type=jnp.float32))
        s = jnp.concatenate(scores, axis=0) * scale + shift
        low = jnp.log1p(jnp.exp(-jnp.abs(s)))
        keep = -(jnp.maximum(s, 0.0) + low)
        sig = jnp.minimum(s, 0.0) - low
        hi = keep.astype(jnp.bfloat16)
        rest = keep - hi.astype(jnp.float32)
        mid = rest.astype(jnp.bfloat16)
        lo = (rest - mid.astype(jnp.float32)).astype(jnp.bfloat16)
        n = pairs * ROWS
        sums = (
            jnp.dot(hi, tri, preferred_element_type=jnp.float32)
            + jnp.dot(mid, tri, preferred_element_type=jnp.float32)
            + jnp.dot(lo, tri, preferred_element_type=jnp.float32)
        )
        weights = jnp.exp(sig + sums[:, :sub]).astype(jnp.bfloat16)
        reads = []
        for p in range(pairs):
            kv = recv[b, :, p * 2 * hd:(p + 1) * 2 * hd]
            reads.append(jnp.dot(weights[p * ROWS:(p + 1) * ROWS], kv, preferred_element_type=jnp.float32))
        read = jnp.concatenate(reads, axis=0)
        both = jnp.where(left_half, sums[:, 128:128 + 2 * hd], read)
        packed = [both[p * ROWS:p * ROWS + group] for p in range(pairs)]
        packed.append(jnp.zeros((packed_rows(pairs, group) - pairs * group, 2 * hd), jnp.float32))
        msg[mt, b] = jnp.concatenate(packed, axis=0)
        for t in range(1, tp):
            msg_copy(b, lax.rem(mt + t, tp)).start()

    order = [me]
    order += [flip(me, k) for k in range(1, sp // 2)]
    order += [(1 - top) * (sp - 1 - j) + top * j for j in range(sp // 2)]
    for i, b in enumerate(order):
        if i:
            arrived(b).wait_recv()
        attend(b)

    sent = send.at[pl.ds(0, sp - 1)]
    pltpu.make_async_copy(sent, sent, send_sem).wait()
    for t in range(1, tp):
        all_msgs(lax.rem(mt + t, tp)).wait_recv()
    for t in range(1, tp):
        all_msgs(lax.rem(mt + t, tp)).wait_send()


def finish(sp, tp, hd, group, pairs, recv, msg, stored_hbm, first_hbm, fin, first_v, out_sem, first_sem):
    copies = [
        pltpu.make_async_copy(recv.at[b, :, pl.ds(p * 2 * hd, 2 * hd)], stored_hbm.at[p, b], out_sem.at[b, p])
        for b in range(sp)
        for p in range(pairs)
    ]
    for copy in copies:
        copy.start()
    left_half = lax.broadcasted_iota(jnp.int32, (packed_rows(pairs, group), 2 * hd), 1) < hd

    def add_block(i, carry):
        total, acc = carry
        b = sp - 1 - i
        for j in range(tp - 1, -1, -1):
            m = msg[j, b]
            total = total + jnp.exp(acc) * m
            acc = acc + pltpu.roll(m, hd, 1)
        return total, acc

    zero = jnp.zeros((packed_rows(pairs, group), 2 * hd), jnp.float32)
    total, _ = lax.fori_loop(0, sp, add_block, (zero, zero), unroll=True)
    total = jnp.where(left_half, 0.0, total)
    squares = jnp.sum(total * total, axis=1, keepdims=True) * (1.0 / hd)
    fin[...] = pltpu.roll(total * lax.rsqrt(squares + EPS_NORM), hd, 1)
    cols = [fin[pl.ds(g, pairs, stride=group), :][:, :hd] for g in range(group)]
    first_v[...] = jnp.concatenate(cols, axis=1).astype(first_v.dtype)
    first_copy = pltpu.make_async_copy(first_v, first_hbm, first_sem)
    first_copy.start()

    for copy in copies:
        copy.wait()
    first_copy.wait()


def solution(mesh):
    sp, tp = mesh.shape["sp"], mesh.shape["tp"]

    def per_device(layer_input, key_weight, value_weight, queries, head_bias):
        seqs, sub, width = layer_input.shape
        pairs, group, hd = queries.shape
        kvh = head_bias.shape[0]
        x = layer_input.reshape(seqs * sub, width)
        block = pairs * 2 * hd
        any_spec = pl.BlockSpec(memory_space=pltpu.HBM)
        dma = pltpu.SemaphoreType.DMA
        handed = sp * sub * block * 2 + tp * sp * packed_rows(pairs, group) * 2 * hd * 4
        limit = VMEM_BYTES - handed
        vmem_spec = pl.BlockSpec(memory_space=pltpu.VMEM)
        recv, msg = pl.pallas_call(
            functools.partial(kernel, sp, tp, seqs, sub, hd, kvh, group, pairs),
            out_shape=(
                pltpu.VMEM((sp, sub, block), jnp.bfloat16),
                pltpu.VMEM((tp, sp, packed_rows(pairs, group), 2 * hd), jnp.float32),
            ),
            in_specs=[any_spec] * 5,
            out_specs=(vmem_spec, vmem_spec),
            scratch_shapes=[
                pltpu.VMEM(x.shape, jnp.bfloat16),
                pltpu.VMEM(key_weight.shape, jnp.bfloat16),
                pltpu.VMEM(value_weight.shape, jnp.bfloat16),
                pltpu.VMEM((group, pairs, hd), jnp.bfloat16),
                pltpu.VMEM(head_bias.shape, jnp.float32),
                pltpu.VMEM((sp, sub, block), jnp.bfloat16),
                dma((2,)),
                dma((2, KC)),
                dma((2,)),
                dma(()),
                dma((sp,)),
                dma(()),
                dma((tp,)),
            ],
            compiler_params=pltpu.CompilerParams(
                collective_id=0, has_side_effects=True, vmem_limit_bytes=limit
            ),
        )(x, key_weight, value_weight, queries.transpose(1, 0, 2), head_bias)
        return pl.pallas_call(
            functools.partial(finish, sp, tp, hd, group, pairs),
            out_shape=(
                jax.ShapeDtypeStruct((pairs, sp, sub, 2 * hd), jnp.bfloat16),
                jax.ShapeDtypeStruct((pairs, group * hd), jnp.bfloat16),
            ),
            in_specs=[vmem_spec, vmem_spec],
            out_specs=(any_spec, any_spec),
            scratch_shapes=[
                pltpu.VMEM((packed_rows(pairs, group), 2 * hd), jnp.float32),
                pltpu.VMEM((pairs, group * hd), jnp.bfloat16),
                dma((sp, pairs)),
                dma(()),
            ],
            compiler_params=pltpu.CompilerParams(vmem_limit_bytes=VMEM_BYTES // 4),
        )(recv, msg)

    in_specs = (P(None, ("sp", "tp"), None), P(), P(), P("sp", None, None), P())
    out_specs = (P("sp", None, "tp", None), P("sp", None))
    return jax.shard_map(per_device, mesh=mesh, in_specs=in_specs, out_specs=out_specs, check_vma=False)
```

```python
import functools
import math

import jax
import jax.numpy as jnp
from jax import lax
from jax.experimental import pallas as pl
from jax.experimental.pallas import tpu as pltpu
from jax.sharding import PartitionSpec as P

EPS_NORM = 0.0001
MESH = pl.DeviceIdType.MESH
KC = 4
VMEM_BYTES = 60 * 1024 * 1024
ROWS = 8


def flip(index, k):
    bit = 1
    while bit <= k:
        if k & bit:
            index = index + (1 - 2 * ((index // bit) % 2)) * bit
        bit *= 2
    return index


def packed_rows(pairs, group):
    return pairs * group // 8 * 8 + 8


def kernel(
    sp, tp, seqs, sub, hd, kvh, group, pairs,
    x_hbm, wk_hbm, wv_hbm, q_hbm, bias_hbm,
    recv, msg,
    x_v, w_v, q_v, bias_v, send,
    x_sem, w_sem, small_sem, send_sem, recv_sem, msend_sem, mrecv_sem,
):
    me = lax.axis_index("sp")
    mt = lax.axis_index("tp")
    per_seq = kvh // pairs
    width = x_hbm.shape[1]
    kc = width // KC
    half_rows = seqs * sub // 2

    barrier = pltpu.get_barrier_semaphore()
    for k in range(sp - 1, 0, -1):
        pl.semaphore_signal(barrier, inc=1, device_id={"sp": flip(me, k)}, device_id_type=MESH)
    for k in range(1, tp):
        pl.semaphore_signal(barrier, inc=1, device_id={"tp": lax.rem(mt + k, tp)}, device_id_type=MESH)

    top = me // (sp // 2)
    half = sp // 2
    kv_width = wk_hbm.shape[1]

    def x_copy(h, c):
        at = (pl.ds(h * half_rows, half_rows), pl.ds(c * kc, kc))
        return pltpu.make_async_copy(x_hbm.at[at], x_v.at[at], x_sem.at[h, c])

    def w_copy(i, c):
        rows = pl.ds(c * kc, kc)
        w_hbm = (wk_hbm, wv_hbm)[i]
        return pltpu.make_async_copy(w_hbm.at[rows], w_v.at[rows, pl.ds(i * kv_width, kv_width)], w_sem.at[i, c])

    for c in range(KC):
        x_copy(0, c).start()
        w_copy(0, c).start()
        w_copy(1, c).start()
    for c in range(KC):
        x_copy(1, c).start()
    q_copy = pltpu.make_async_copy(q_hbm, q_v, small_sem.at[0])
    bias_copy = pltpu.make_async_copy(bias_hbm, bias_v, small_sem.at[1])
    q_copy.start()
    bias_copy.start()

    def pack(rows, base):
        for i in range(seqs // 2):
            for part in range(per_seq):
                out = []
                for p in range(pairs):
                    c0 = (part * pairs + p) * hd
                    out.append(rows[i * sub:(i + 1) * sub, c0:c0 + hd])
                    out.append(rows[i * sub:(i + 1) * sub, kv_width + c0:kv_width + c0 + hd])
                send[base + i * per_seq + part] = jnp.concatenate(out, axis=1).astype(jnp.bfloat16)

    def block_copy(to):
        return pltpu.make_async_remote_copy(
            src_ref=send.at[to], dst_ref=recv.at[me],
            send_sem=send_sem, recv_sem=recv_sem.at[me],
            device_id={"sp": to}, device_id_type=MESH,
        )

    def arrived(frm):
        return pltpu.make_async_remote_copy(
            src_ref=send.at[frm], dst_ref=recv.at[frm],
            send_sem=send_sem, recv_sem=recv_sem.at[frm],
            device_id={"sp": frm}, device_id_type=MESH,
        )

    def send_half(base):
        for j in range(half):
            to = base + flip(lax.rem(me, 2), j)

            @pl.when(to != me)
            def _():
                block_copy(to).start()

    rows = None
    for c in range(KC):
        x_copy(0, c).wait()
        w_copy(0, c).wait()
        w_copy(1, c).wait()
        part = jnp.dot(
            x_v[:half_rows, c * kc:(c + 1) * kc], w_v[c * kc:(c + 1) * kc, :],
            preferred_element_type=jnp.float32,
        )
        rows = part if rows is None else rows + part
    pack(rows, 0)

    @pl.when(top == 1)
    def _():
        pl.semaphore_wait(barrier, sp + tp - 2)
        send_half(0)

    for c in range(KC):
        x_copy(1, c).wait()
    pack(jnp.dot(x_v[half_rows:, :], w_v[...], preferred_element_type=jnp.float32), half)

    @pl.when(top == 0)
    def _():
        pl.semaphore_wait(barrier, sp + tp - 2)
        send_half(0)

    send_half(half)
    recv[pl.ds(me, 1)] = send[pl.ds(me, 1)]

    q_copy.wait()
    bias_copy.wait()
    h0 = lax.rem(me * pairs, kvh)
    eye = lax.broadcasted_iota(jnp.int32, (ROWS, group), 0) == lax.broadcasted_iota(jnp.int32, (ROWS, group), 1)
    q_pads = []
    shifts = []
    for p in range(pairs):
        qp = q_v[:, p, :].astype(jnp.float32)
        qp = jnp.concatenate([qp, jnp.zeros((group, hd), jnp.float32)], axis=1)
        qp = jnp.concatenate([qp, jnp.zeros((ROWS - group, 2 * hd), jnp.float32)], axis=0)
        q_pads.append(qp.astype(jnp.bfloat16))
        row = bias_v[pl.ds(h0 + p, 1), :]
        shifts.append(jnp.sum(jnp.where(eye, jnp.broadcast_to(row, (ROWS, group)), 0.0), axis=1, keepdims=True))
    shift = jnp.concatenate(shifts, axis=0)
    scale = 1.0 / math.sqrt(hd)
    later = lax.broadcasted_iota(jnp.int32, (sub, 256), 0)
    column = lax.broadcasted_iota(jnp.int32, (sub, 256), 1)
    tri = ((later > column) | (column >= 128)).astype(jnp.float32).astype(jnp.bfloat16)
    left_half = lax.broadcasted_iota(jnp.int32, (pairs * ROWS, 2 * hd), 1) < hd

    def msg_copy(b, t):
        return pltpu.make_async_remote_copy(
            src_ref=msg.at[mt, b], dst_ref=msg.at[mt, b],
            send_sem=msend_sem, recv_sem=mrecv_sem.at[mt],
            device_id={"tp": t}, device_id_type=MESH,
        )

    def all_msgs(t):
        return pltpu.make_async_remote_copy(
            src_ref=msg.at[t], dst_ref=msg.at[t],
            send_sem=msend_sem, recv_sem=mrecv_sem.at[t],
            device_id={"tp": t}, device_id_type=MESH,
        )

    def attend(b):
        scores = []
        for p in range(pairs):
            kv = recv[b, :, p * 2 * hd:(p + 1) * 2 * hd]
            scores.append(lax.dot_general(q_pads[p], kv, (((1,), (1,)), ((), ())), preferred_element_type=jnp.float32))
        s = jnp.concatenate(scores, axis=0) * scale + shift
        low = jnp.log1p(jnp.exp(-jnp.abs(s)))
        keep = -(jnp.maximum(s, 0.0) + low)
        sig = jnp.minimum(s, 0.0) - low
        hi = keep.astype(jnp.bfloat16)
        rest = keep - hi.astype(jnp.float32)
        mid = rest.astype(jnp.bfloat16)
        lo = (rest - mid.astype(jnp.float32)).astype(jnp.bfloat16)
        n = pairs * ROWS
        sums = (
            jnp.dot(hi, tri, preferred_element_type=jnp.float32)
            + jnp.dot(mid, tri, preferred_element_type=jnp.float32)
            + jnp.dot(lo, tri, preferred_element_type=jnp.float32)
        )
        weights = jnp.exp(sig + sums[:, :sub]).astype(jnp.bfloat16)
        reads = []
        for p in range(pairs):
            kv = recv[b, :, p * 2 * hd:(p + 1) * 2 * hd]
            reads.append(jnp.dot(weights[p * ROWS:(p + 1) * ROWS], kv, preferred_element_type=jnp.float32))
        read = jnp.concatenate(reads, axis=0)
        both = jnp.where(left_half, sums[:, 128:128 + 2 * hd], read)
        packed = [both[p * ROWS:p * ROWS + group] for p in range(pairs)]
        packed.append(jnp.zeros((packed_rows(pairs, group) - pairs * group, 2 * hd), jnp.float32))
        msg[mt, b] = jnp.concatenate(packed, axis=0)
        for t in range(1, tp):
            msg_copy(b, lax.rem(mt + t, tp)).start()

    order = [me]
    order += [flip(me, k) for k in range(1, sp // 2)]
    order += [(1 - top) * (sp - 1 - j) + top * j for j in range(sp // 2)]
    for i, b in enumerate(order):
        if i:
            arrived(b).wait_recv()
        attend(b)

    sent = send.at[pl.ds(0, sp - 1)]
    pltpu.make_async_copy(sent, sent, send_sem).wait()
    for t in range(1, tp):
        all_msgs(lax.rem(mt + t, tp)).wait_recv()
    for t in range(1, tp):
        all_msgs(lax.rem(mt + t, tp)).wait_send()


def finish(sp, tp, hd, group, pairs, recv, msg, stored_hbm, first_hbm, fin, first_v, out_sem, first_sem):
    copies = [
        pltpu.make_async_copy(recv.at[b, :, pl.ds(p * 2 * hd, 2 * hd)], stored_hbm.at[p, b], out_sem.at[b, p])
        for b in range(sp)
        for p in range(pairs)
    ]
    for copy in copies:
        copy.start()
    left_half = lax.broadcasted_iota(jnp.int32, (packed_rows(pairs, group), 2 * hd), 1) < hd

    def add_block(i, carry):
        total, acc = carry
        b = sp - 1 - i
        for j in range(tp - 1, -1, -1):
            m = msg[j, b]
            total = total + jnp.exp(acc) * m
            acc = acc + pltpu.roll(m, hd, 1)
        return total, acc

    zero = jnp.zeros((packed_rows(pairs, group), 2 * hd), jnp.float32)
    total, _ = lax.fori_loop(0, sp, add_block, (zero, zero), unroll=True)
    total = jnp.where(left_half, 0.0, total)
    squares = jnp.sum(total * total, axis=1, keepdims=True) * (1.0 / hd)
    fin[...] = pltpu.roll(total * lax.rsqrt(squares + EPS_NORM), hd, 1)
    cols = [fin[pl.ds(g, pairs, stride=group), :][:, :hd] for g in range(group)]
    first_v[...] = jnp.concatenate(cols, axis=1).astype(first_v.dtype)
    first_copy = pltpu.make_async_copy(first_v, first_hbm, first_sem)
    first_copy.start()

    for copy in copies:
        copy.wait()
    first_copy.wait()


def solution(mesh):
    sp, tp = mesh.shape["sp"], mesh.shape["tp"]

    def per_device(layer_input, key_weight, value_weight, queries, head_bias):
        seqs, sub, width = layer_input.shape
        pairs, group, hd = queries.shape
        kvh = head_bias.shape[0]
        x = layer_input.reshape(seqs * sub, width)
        block = pairs * 2 * hd
        any_spec = pl.BlockSpec(memory_space=pltpu.HBM)
        dma = pltpu.SemaphoreType.DMA
        handed = sp * sub * block * 2 + tp * sp * packed_rows(pairs, group) * 2 * hd * 4
        limit = VMEM_BYTES - handed
        vmem_spec = pl.BlockSpec(memory_space=pltpu.VMEM)
        recv, msg = pl.pallas_call(
            functools.partial(kernel, sp, tp, seqs, sub, hd, kvh, group, pairs),
            out_shape=(
                pltpu.VMEM((sp, sub, block), jnp.bfloat16),
                pltpu.VMEM((tp, sp, packed_rows(pairs, group), 2 * hd), jnp.float32),
            ),
            in_specs=[any_spec] * 5,
            out_specs=(vmem_spec, vmem_spec),
            scratch_shapes=[
                pltpu.VMEM(x.shape, jnp.bfloat16),
                pltpu.VMEM((width, 2 * key_weight.shape[1]), jnp.bfloat16),
                pltpu.VMEM((group, pairs, hd), jnp.bfloat16),
                pltpu.VMEM(head_bias.shape, jnp.float32),
                pltpu.VMEM((sp, sub, block), jnp.bfloat16),
                dma((2, KC)),
                dma((2, KC)),
                dma((2,)),
                dma(()),
                dma((sp,)),
                dma(()),
                dma((tp,)),
            ],
            compiler_params=pltpu.CompilerParams(
                collective_id=0, has_side_effects=True, vmem_limit_bytes=limit
            ),
        )(x, key_weight, value_weight, queries.transpose(1, 0, 2), head_bias)
        return pl.pallas_call(
            functools.partial(finish, sp, tp, hd, group, pairs),
            out_shape=(
                jax.ShapeDtypeStruct((pairs, sp, sub, 2 * hd), jnp.bfloat16),
                jax.ShapeDtypeStruct((pairs, group * hd), jnp.bfloat16),
            ),
            in_specs=[vmem_spec, vmem_spec],
            out_specs=(any_spec, any_spec),
            scratch_shapes=[
                pltpu.VMEM((packed_rows(pairs, group), 2 * hd), jnp.float32),
                pltpu.VMEM((pairs, group * hd), jnp.bfloat16),
                dma((sp, pairs)),
                dma(()),
            ],
            compiler_params=pltpu.CompilerParams(vmem_limit_bytes=VMEM_BYTES // 4),
        )(recv, msg)

    in_specs = (P(None, ("sp", "tp"), None), P(), P(), P("sp", None, None), P())
    out_specs = (P("sp", None, "tp", None), P("sp", None))
    return jax.shard_map(per_device, mesh=mesh, in_specs=in_specs, out_specs=out_specs, check_vma=False)
```

```python
import functools
import math

import jax
import jax.numpy as jnp
from jax import lax
from jax.experimental import pallas as pl
from jax.experimental.pallas import tpu as pltpu
from jax.sharding import PartitionSpec as P

EPS_NORM = 0.0001
MESH = pl.DeviceIdType.MESH
KC = 4
VMEM_BYTES = 60 * 1024 * 1024
ROWS = 8


def flip(index, k):
    bit = 1
    while bit <= k:
        if k & bit:
            index = index + (1 - 2 * ((index // bit) % 2)) * bit
        bit *= 2
    return index


def packed_rows(pairs, group):
    return pairs * group // 8 * 8 + 8


def kernel(
    sp, tp, seqs, sub, hd, kvh, group, pairs,
    x_hbm, wk_hbm, wv_hbm, q_hbm, bias_hbm,
    recv, msg,
    x_v, w_v, q_v, bias_v, send,
    x_sem, w_sem, small_sem, send_sem, recv_sem, msend_sem, mrecv_sem,
):
    me = lax.axis_index("sp")
    mt = lax.axis_index("tp")
    per_seq = kvh // pairs
    width = x_hbm.shape[1]
    kc = width // KC
    half_rows = seqs * sub // 2

    barrier = pltpu.get_barrier_semaphore()
    for k in range(sp - 1, 0, -1):
        pl.semaphore_signal(barrier, inc=1, device_id={"sp": flip(me, k)}, device_id_type=MESH)
    for k in range(1, tp):
        pl.semaphore_signal(barrier, inc=1, device_id={"tp": lax.rem(mt + k, tp)}, device_id_type=MESH)

    top = me // (sp // 2)
    half = sp // 2
    quarter = sp // 4
    outer = lax.rem(me // quarter, 3) == 0
    far_outer = (1 - top) * 3 * quarter
    far_inner = quarter + (1 - top) * quarter
    kv_width = wk_hbm.shape[1]

    def x_copy(h, c):
        at = (pl.ds(h * half_rows, half_rows), pl.ds(c * kc, kc))
        return pltpu.make_async_copy(x_hbm.at[at], x_v.at[at], x_sem.at[h, c])

    def w_copy(i, c):
        rows = pl.ds(c * kc, kc)
        w_hbm = (wk_hbm, wv_hbm)[i]
        return pltpu.make_async_copy(w_hbm.at[rows], w_v.at[rows, pl.ds(i * kv_width, kv_width)], w_sem.at[i, c])

    for c in range(KC):
        x_copy(0, c).start()
        w_copy(0, c).start()
        w_copy(1, c).start()
    for c in range(KC):
        x_copy(1, c).start()
    q_copy = pltpu.make_async_copy(q_hbm, q_v, small_sem.at[0])
    bias_copy = pltpu.make_async_copy(bias_hbm, bias_v, small_sem.at[1])
    q_copy.start()
    bias_copy.start()

    def pack(rows, base):
        for i in range(seqs // 2):
            for part in range(per_seq):
                out = []
                for p in range(pairs):
                    c0 = (part * pairs + p) * hd
                    out.append(rows[i * sub:(i + 1) * sub, c0:c0 + hd])
                    out.append(rows[i * sub:(i + 1) * sub, kv_width + c0:kv_width + c0 + hd])
                send[base + i * per_seq + part] = jnp.concatenate(out, axis=1).astype(jnp.bfloat16)

    def block_copy(to, sem):
        return pltpu.make_async_remote_copy(
            src_ref=send.at[to], dst_ref=recv.at[me],
            send_sem=send_sem.at[sem], recv_sem=recv_sem.at[me],
            device_id={"sp": to}, device_id_type=MESH,
        )

    def arrived(frm):
        return pltpu.make_async_remote_copy(
            src_ref=send.at[frm], dst_ref=recv.at[frm],
            send_sem=send_sem.at[1], recv_sem=recv_sem.at[frm],
            device_id={"sp": frm}, device_id_type=MESH,
        )

    def send_blocks(base, count, sem):
        for j in range(count):
            to = base + flip(lax.rem(me, 2), j)

            @pl.when(to != me)
            def _():
                block_copy(to, sem).start()

    def send_far():
        send_blocks(far_outer, quarter, 0)

        @pl.when(jnp.logical_not(outer))
        def _():
            send_blocks(far_inner, quarter, 1)

    def sent(count, sem):
        part = send.at[pl.ds(0, count)]
        pltpu.make_async_copy(part, part, send_sem.at[sem]).wait()

    rows = None
    for c in range(KC):
        x_copy(0, c).wait()
        w_copy(0, c).wait()
        w_copy(1, c).wait()
        part = jnp.dot(
            x_v[:half_rows, c * kc:(c + 1) * kc], w_v[c * kc:(c + 1) * kc, :],
            preferred_element_type=jnp.float32,
        )
        rows = part if rows is None else rows + part
    pack(rows, 0)

    @pl.when(top == 1)
    def _():
        pl.semaphore_wait(barrier, sp + tp - 2)
        send_far()

    for c in range(KC):
        x_copy(1, c).wait()
    pack(jnp.dot(x_v[half_rows:, :], w_v[...], preferred_element_type=jnp.float32), half)

    @pl.when(top == 0)
    def _():
        pl.semaphore_wait(barrier, sp + tp - 2)

    send_blocks(top * half, half, 1)

    @pl.when(top == 0)
    def _():
        send_far()

    recv[pl.ds(me, 1)] = send[pl.ds(me, 1)]

    q_copy.wait()
    bias_copy.wait()
    h0 = lax.rem(me * pairs, kvh)
    eye = lax.broadcasted_iota(jnp.int32, (ROWS, group), 0) == lax.broadcasted_iota(jnp.int32, (ROWS, group), 1)
    q_pads = []
    shifts = []
    for p in range(pairs):
        qp = q_v[:, p, :].astype(jnp.float32)
        qp = jnp.concatenate([qp, jnp.zeros((group, hd), jnp.float32)], axis=1)
        qp = jnp.concatenate([qp, jnp.zeros((ROWS - group, 2 * hd), jnp.float32)], axis=0)
        q_pads.append(qp.astype(jnp.bfloat16))
        row = bias_v[pl.ds(h0 + p, 1), :]
        shifts.append(jnp.sum(jnp.where(eye, jnp.broadcast_to(row, (ROWS, group)), 0.0), axis=1, keepdims=True))
    shift = jnp.concatenate(shifts, axis=0)
    scale = 1.0 / math.sqrt(hd)
    later = lax.broadcasted_iota(jnp.int32, (sub, 256), 0)
    column = lax.broadcasted_iota(jnp.int32, (sub, 256), 1)
    tri = ((later > column) | (column >= 128)).astype(jnp.float32).astype(jnp.bfloat16)
    left_half = lax.broadcasted_iota(jnp.int32, (pairs * ROWS, 2 * hd), 1) < hd

    def msg_copy(b, t):
        return pltpu.make_async_remote_copy(
            src_ref=msg.at[mt, b], dst_ref=msg.at[mt, b],
            send_sem=msend_sem, recv_sem=mrecv_sem.at[mt],
            device_id={"tp": t}, device_id_type=MESH,
        )

    def all_msgs(t):
        return pltpu.make_async_remote_copy(
            src_ref=msg.at[t], dst_ref=msg.at[t],
            send_sem=msend_sem, recv_sem=mrecv_sem.at[t],
            device_id={"tp": t}, device_id_type=MESH,
        )

    def attend(blocks):
        scores = []
        for b in blocks:
            for p in range(pairs):
                kv = recv[b, :, p * 2 * hd:(p + 1) * 2 * hd]
                scores.append(lax.dot_general(q_pads[p], kv, (((1,), (1,)), ((), ())), preferred_element_type=jnp.float32))
        s = jnp.concatenate(scores, axis=0) * scale + jnp.concatenate([shift] * len(blocks), axis=0)
        low = jnp.log1p(jnp.exp(-jnp.abs(s)))
        keep = -(jnp.maximum(s, 0.0) + low)
        sig = jnp.minimum(s, 0.0) - low
        hi = keep.astype(jnp.bfloat16)
        rest = keep - hi.astype(jnp.float32)
        mid = rest.astype(jnp.bfloat16)
        lo = (rest - mid.astype(jnp.float32)).astype(jnp.bfloat16)
        sums = (
            jnp.dot(hi, tri, preferred_element_type=jnp.float32)
            + jnp.dot(mid, tri, preferred_element_type=jnp.float32)
            + jnp.dot(lo, tri, preferred_element_type=jnp.float32)
        )
        weights = jnp.exp(sig + sums[:, :sub]).astype(jnp.bfloat16)
        n = pairs * ROWS
        for i, b in enumerate(blocks):
            reads = []
            for p in range(pairs):
                kv = recv[b, :, p * 2 * hd:(p + 1) * 2 * hd]
                at = i * n + p * ROWS
                reads.append(jnp.dot(weights[at:at + ROWS], kv, preferred_element_type=jnp.float32))
            read = jnp.concatenate(reads, axis=0)
            both = jnp.where(left_half, sums[i * n:(i + 1) * n, 128:128 + 2 * hd], read)
            packed = [both[p * ROWS:p * ROWS + group] for p in range(pairs)]
            packed.append(jnp.zeros((packed_rows(pairs, group) - pairs * group, 2 * hd), jnp.float32))
            msg[mt, b] = jnp.concatenate(packed, axis=0)
            for t in range(1, tp):
                msg_copy(b, lax.rem(mt + t, tp)).start()

    near = [flip(me, k) for k in range(quarter, half)]
    far = [far_outer + flip(lax.rem(me, 2), j) for j in range(quarter)]
    far += [far_inner + flip(lax.rem(me, 2), j) for j in range(quarter)]
    order = [me] + [flip(me, k) for k in range(1, quarter)]
    order += [jnp.where(outer, a, b) for a, b in zip(far + near, near + far)]
    steps = [order[:1]] + [order[i:i + 1] for i in range(1, quarter)]
    steps += [order[i:i + 2] for i in range(quarter, sp, 2)]
    for i, blocks in enumerate(steps):
        if i:
            for b in blocks:
                arrived(b).wait_recv()
        attend(blocks)
        if i == 0:

            @pl.when(outer)
            def _():
                sent(quarter, 0)
                send_blocks(far_inner, quarter, 1)

    @pl.when(jnp.logical_not(outer))
    def _():
        sent(quarter, 0)

    sent(sp - 1 - quarter, 1)
    for t in range(1, tp):
        all_msgs(lax.rem(mt + t, tp)).wait_recv()
    for t in range(1, tp):
        all_msgs(lax.rem(mt + t, tp)).wait_send()


def finish(sp, tp, hd, group, pairs, recv, msg, stored_hbm, first_hbm, fin, first_v, out_sem, first_sem):
    copies = [
        pltpu.make_async_copy(recv.at[b, :, pl.ds(p * 2 * hd, 2 * hd)], stored_hbm.at[p, b], out_sem.at[b, p])
        for b in range(sp)
        for p in range(pairs)
    ]
    for copy in copies:
        copy.start()
    left_half = lax.broadcasted_iota(jnp.int32, (packed_rows(pairs, group), 2 * hd), 1) < hd

    def add_block(i, carry):
        total, acc = carry
        b = sp - 1 - i
        for j in range(tp - 1, -1, -1):
            m = msg[j, b]
            total = total + jnp.exp(acc) * m
            acc = acc + pltpu.roll(m, hd, 1)
        return total, acc

    zero = jnp.zeros((packed_rows(pairs, group), 2 * hd), jnp.float32)
    total, _ = lax.fori_loop(0, sp, add_block, (zero, zero), unroll=True)
    total = jnp.where(left_half, 0.0, total)
    squares = jnp.sum(total * total, axis=1, keepdims=True) * (1.0 / hd)
    fin[...] = pltpu.roll(total * lax.rsqrt(squares + EPS_NORM), hd, 1)
    cols = [fin[pl.ds(g, pairs, stride=group), :][:, :hd] for g in range(group)]
    first_v[...] = jnp.concatenate(cols, axis=1).astype(first_v.dtype)
    first_copy = pltpu.make_async_copy(first_v, first_hbm, first_sem)
    first_copy.start()

    for copy in copies:
        copy.wait()
    first_copy.wait()


def solution(mesh):
    sp, tp = mesh.shape["sp"], mesh.shape["tp"]

    def per_device(layer_input, key_weight, value_weight, queries, head_bias):
        seqs, sub, width = layer_input.shape
        pairs, group, hd = queries.shape
        kvh = head_bias.shape[0]
        x = layer_input.reshape(seqs * sub, width)
        block = pairs * 2 * hd
        any_spec = pl.BlockSpec(memory_space=pltpu.HBM)
        dma = pltpu.SemaphoreType.DMA
        handed = sp * sub * block * 2 + tp * sp * packed_rows(pairs, group) * 2 * hd * 4
        limit = VMEM_BYTES - handed
        vmem_spec = pl.BlockSpec(memory_space=pltpu.VMEM)
        recv, msg = pl.pallas_call(
            functools.partial(kernel, sp, tp, seqs, sub, hd, kvh, group, pairs),
            out_shape=(
                pltpu.VMEM((sp, sub, block), jnp.bfloat16),
                pltpu.VMEM((tp, sp, packed_rows(pairs, group), 2 * hd), jnp.float32),
            ),
            in_specs=[any_spec] * 5,
            out_specs=(vmem_spec, vmem_spec),
            scratch_shapes=[
                pltpu.VMEM(x.shape, jnp.bfloat16),
                pltpu.VMEM((width, 2 * key_weight.shape[1]), jnp.bfloat16),
                pltpu.VMEM((group, pairs, hd), jnp.bfloat16),
                pltpu.VMEM(head_bias.shape, jnp.float32),
                pltpu.VMEM((sp, sub, block), jnp.bfloat16),
                dma((2, KC)),
                dma((2, KC)),
                dma((2,)),
                dma((2,)),
                dma((sp,)),
                dma(()),
                dma((tp,)),
            ],
            compiler_params=pltpu.CompilerParams(
                collective_id=0, has_side_effects=True, vmem_limit_bytes=limit
            ),
        )(x, key_weight, value_weight, queries.transpose(1, 0, 2), head_bias)
        return pl.pallas_call(
            functools.partial(finish, sp, tp, hd, group, pairs),
            out_shape=(
                jax.ShapeDtypeStruct((pairs, sp, sub, 2 * hd), jnp.bfloat16),
                jax.ShapeDtypeStruct((pairs, group * hd), jnp.bfloat16),
            ),
            in_specs=[vmem_spec, vmem_spec],
            out_specs=(any_spec, any_spec),
            scratch_shapes=[
                pltpu.VMEM((packed_rows(pairs, group), 2 * hd), jnp.float32),
                pltpu.VMEM((pairs, group * hd), jnp.bfloat16),
                dma((sp, pairs)),
                dma(()),
            ],
            compiler_params=pltpu.CompilerParams(vmem_limit_bytes=VMEM_BYTES // 4),
        )(recv, msg)

    in_specs = (P(None, ("sp", "tp"), None), P(), P(), P("sp", None, None), P())
    out_specs = (P("sp", None, "tp", None), P("sp", None))
    return jax.shard_map(per_device, mesh=mesh, in_specs=in_specs, out_specs=out_specs, check_vma=False)
```

```python
import functools
import math

import jax
import jax.numpy as jnp
from jax import lax
from jax.experimental import pallas as pl
from jax.experimental.pallas import tpu as pltpu
from jax.sharding import PartitionSpec as P

EPS_NORM = 0.0001
MESH = pl.DeviceIdType.MESH
KC = 4
VMEM_BYTES = 60 * 1024 * 1024
ROWS = 8


def flip(index, k):
    bit = 1
    while bit <= k:
        if k & bit:
            index = index + (1 - 2 * ((index // bit) % 2)) * bit
        bit *= 2
    return index


def packed_rows(pairs, group):
    return pairs * group // 8 * 8 + 8


def kernel(
    sp, tp, seqs, sub, hd, kvh, group, pairs,
    x_hbm, wk_hbm, wv_hbm, q_hbm, bias_hbm,
    recv, msg,
    x_v, w_v, q_v, bias_v, send, q_pad, q_all, part_v, late_v,
    x_sem, w_sem, small_sem, send_sem, recv_sem, msend_sem, mrecv_sem,
    qsend_sem, qrecv_sem, psend_sem, precv_sem, lsend_sem, lrecv_sem,
):
    me = lax.axis_index("sp")
    mt = lax.axis_index("tp")
    per_seq = kvh // pairs
    width = x_hbm.shape[1]
    kc = width // KC
    half_rows = seqs * sub // 2

    q_copy = pltpu.make_async_copy(q_hbm, q_v, small_sem.at[0])
    bias_copy = pltpu.make_async_copy(bias_hbm, bias_v, small_sem.at[1])
    q_copy.start()
    bias_copy.start()
    msg[...] = jnp.zeros_like(msg)
    barrier = pltpu.get_barrier_semaphore()
    for k in range(sp - 1, 0, -1):
        pl.semaphore_signal(barrier, inc=1, device_id={"sp": flip(me, k)}, device_id_type=MESH)
    for k in range(1, tp):
        pl.semaphore_signal(barrier, inc=1, device_id={"tp": lax.rem(mt + k, tp)}, device_id_type=MESH)

    top = me // (sp // 2)
    half = sp // 2
    quarter = sp // 4
    outer = lax.rem(me // quarter, 3) == 0
    far_outer = (1 - top) * 3 * quarter
    far_inner = quarter + (1 - top) * quarter
    kv_width = wk_hbm.shape[1]

    def x_copy(h, c):
        at = (pl.ds(h * half_rows, half_rows), pl.ds(c * kc, kc))
        return pltpu.make_async_copy(x_hbm.at[at], x_v.at[at], x_sem.at[h, c])

    def w_copy(i, c):
        rows = pl.ds(c * kc, kc)
        w_hbm = (wk_hbm, wv_hbm)[i]
        return pltpu.make_async_copy(w_hbm.at[rows], w_v.at[rows, pl.ds(i * kv_width, kv_width)], w_sem.at[i, c])

    for c in range(KC):
        x_copy(0, c).start()
        w_copy(0, c).start()
        w_copy(1, c).start()
    for c in range(KC):
        x_copy(1, c).start()

    def pack(rows, base):
        for i in range(seqs // 2):
            for part in range(per_seq):
                out = []
                for p in range(pairs):
                    c0 = (part * pairs + p) * hd
                    out.append(rows[i * sub:(i + 1) * sub, c0:c0 + hd])
                    out.append(rows[i * sub:(i + 1) * sub, kv_width + c0:kv_width + c0 + hd])
                send[base + i * per_seq + part] = jnp.concatenate(out, axis=1).astype(jnp.bfloat16)

    def block_copy(to, sem):
        return pltpu.make_async_remote_copy(
            src_ref=send.at[to], dst_ref=recv.at[me],
            send_sem=send_sem.at[sem], recv_sem=recv_sem.at[me],
            device_id={"sp": to}, device_id_type=MESH,
        )

    def arrived(frm):
        return pltpu.make_async_remote_copy(
            src_ref=send.at[frm], dst_ref=recv.at[frm],
            send_sem=send_sem.at[1], recv_sem=recv_sem.at[frm],
            device_id={"sp": frm}, device_id_type=MESH,
        )

    def query_copy(to):
        return pltpu.make_async_remote_copy(
            src_ref=q_pad, dst_ref=q_all.at[me],
            send_sem=qsend_sem, recv_sem=qrecv_sem.at[me],
            device_id={"sp": to}, device_id_type=MESH,
        )

    def query_arrived(frm):
        return pltpu.make_async_remote_copy(
            src_ref=q_pad, dst_ref=q_all.at[frm],
            send_sem=qsend_sem, recv_sem=qrecv_sem.at[frm],
            device_id={"sp": frm}, device_id_type=MESH,
        )

    near = [flip(me, k) for k in range(quarter, half)]
    inward = [far_inner + flip(lax.rem(me, 2), j) for j in range(quarter)]
    outward = [far_outer + flip(lax.rem(me, 2), j) for j in range(quarter)]
    early = [me] + [flip(me, k) for k in range(1, quarter)]
    early += [jnp.where(outer, a, b) for a, b in zip(outward, near)]
    late = [jnp.where(outer, a, b) for a, b in zip(near, outward)] + inward

    def enter():
        pl.semaphore_wait(barrier, sp + tp - 2)
        for to in late:
            query_copy(to).start()

    def send_blocks(base, count, sem):
        for j in range(count):
            to = base + flip(lax.rem(me, 2), j)

            @pl.when(to != me)
            def _():
                block_copy(to, sem).start()

    def send_far():
        send_blocks(far_outer, quarter, 0)

        @pl.when(jnp.logical_or(top == 0, jnp.logical_not(outer)))
        def _():
            send_blocks(far_inner, quarter, 1)

    def sent(count, sem):
        part = send.at[pl.ds(0, count)]
        pltpu.make_async_copy(part, part, send_sem.at[sem]).wait()

    q_copy.wait()
    for p in range(pairs):
        qp = q_v[:, p, :].astype(jnp.float32)
        qp = jnp.concatenate([qp, jnp.zeros((group, hd), jnp.float32)], axis=1)
        qp = jnp.concatenate([qp, jnp.zeros((ROWS - group, 2 * hd), jnp.float32)], axis=0)
        q_pad[p * ROWS:(p + 1) * ROWS, :] = qp.astype(jnp.bfloat16)

    rows = None
    for c in range(KC):
        if c == KC - 1:

            @pl.when(top == 1)
            def _():
                enter()

        x_copy(0, c).wait()
        w_copy(0, c).wait()
        w_copy(1, c).wait()
        part = jnp.dot(
            x_v[:half_rows, c * kc:(c + 1) * kc], w_v[c * kc:(c + 1) * kc, :],
            preferred_element_type=jnp.float32,
        )
        rows = part if rows is None else rows + part
    pack(rows, 0)

    @pl.when(top == 1)
    def _():
        send_far()

    for c in range(KC):
        x_copy(1, c).wait()
    pack(jnp.dot(x_v[half_rows:, :], w_v[...], preferred_element_type=jnp.float32), half)

    @pl.when(top == 0)
    def _():
        enter()

    send_blocks(top * half, half, 1)

    @pl.when(jnp.logical_and(top == 1, outer))
    def _():
        send_blocks(far_inner, quarter, 1)

    @pl.when(top == 0)
    def _():
        send_far()

    recv[pl.ds(me, 1)] = send[pl.ds(me, 1)]

    bias_copy.wait()
    eye = lax.broadcasted_iota(jnp.int32, (ROWS, group), 0) == lax.broadcasted_iota(jnp.int32, (ROWS, group), 1)

    def shift_of(owner):
        h0 = lax.rem(owner * pairs, kvh)
        shifts = []
        for p in range(pairs):
            row = bias_v[pl.ds(h0 + p, 1), :]
            shifts.append(jnp.sum(jnp.where(eye, jnp.broadcast_to(row, (ROWS, group)), 0.0), axis=1, keepdims=True))
        return jnp.concatenate(shifts, axis=0)

    scale = 1.0 / math.sqrt(hd)
    later = lax.broadcasted_iota(jnp.int32, (sub, 256), 0)
    column = lax.broadcasted_iota(jnp.int32, (sub, 256), 1)
    tri = ((later > column) | (column >= 128)).astype(jnp.float32).astype(jnp.bfloat16)
    left_half = lax.broadcasted_iota(jnp.int32, (pairs * ROWS, 2 * hd), 1) < hd

    late_half = lax.broadcasted_iota(jnp.int32, (2 * packed_rows(pairs, group), 2 * hd), 1) < hd

    def msg_copy(b, t):
        return pltpu.make_async_remote_copy(
            src_ref=msg.at[mt, b], dst_ref=msg.at[mt, b],
            send_sem=msend_sem, recv_sem=mrecv_sem.at[mt],
            device_id={"tp": t}, device_id_type=MESH,
        )

    def part_copy(i, t):
        return pltpu.make_async_remote_copy(
            src_ref=part_v.at[mt, i], dst_ref=part_v.at[mt, i],
            send_sem=psend_sem.at[i], recv_sem=precv_sem.at[mt, i],
            device_id={"tp": t}, device_id_type=MESH,
        )

    def part_arrived(i, t):
        return pltpu.make_async_remote_copy(
            src_ref=part_v.at[t, i], dst_ref=part_v.at[t, i],
            send_sem=psend_sem.at[i], recv_sem=precv_sem.at[t, i],
            device_id={"tp": t}, device_id_type=MESH,
        )

    def late_copy(i, j, to):
        return pltpu.make_async_remote_copy(
            src_ref=late_v.at[i, j], dst_ref=msg.at[tp - 1, me],
            send_sem=lsend_sem.at[i], recv_sem=lrecv_sem,
            device_id={"sp": to}, device_id_type=MESH,
        )

    def wait_bytes(ref, sem):
        pltpu.make_async_copy(ref, ref, sem).wait()

    def attend(items):
        scores = []
        shifts = []
        for queries, shift, rows, b in items:
            shifts.append(shift)
            for p in range(pairs):
                q = queries[p * ROWS:(p + 1) * ROWS, :]
                kv = rows[b, :, p * 2 * hd:(p + 1) * 2 * hd]
                scores.append(lax.dot_general(q, kv, (((1,), (1,)), ((), ())), preferred_element_type=jnp.float32))
        s = jnp.concatenate(scores, axis=0) * scale + jnp.concatenate(shifts, axis=0)
        low = jnp.log1p(jnp.exp(-jnp.abs(s)))
        keep = -(jnp.maximum(s, 0.0) + low)
        sig = jnp.minimum(s, 0.0) - low
        hi = keep.astype(jnp.bfloat16)
        rest = keep - hi.astype(jnp.float32)
        mid = rest.astype(jnp.bfloat16)
        lo = (rest - mid.astype(jnp.float32)).astype(jnp.bfloat16)
        sums = (
            jnp.dot(hi, tri, preferred_element_type=jnp.float32)
            + jnp.dot(mid, tri, preferred_element_type=jnp.float32)
            + jnp.dot(lo, tri, preferred_element_type=jnp.float32)
        )
        weights = jnp.exp(sig + sums[:, :sub]).astype(jnp.bfloat16)
        n = pairs * ROWS
        out = []
        for i, (_, _, rows, b) in enumerate(items):
            reads = []
            for p in range(pairs):
                kv = rows[b, :, p * 2 * hd:(p + 1) * 2 * hd]
                at = i * n + p * ROWS
                reads.append(jnp.dot(weights[at:at + ROWS], kv, preferred_element_type=jnp.float32))
            read = jnp.concatenate(reads, axis=0)
            both = jnp.where(left_half, sums[i * n:(i + 1) * n, 128:128 + 2 * hd], read)
            packed = [both[p * ROWS:p * ROWS + group] for p in range(pairs)]
            packed.append(jnp.zeros((packed_rows(pairs, group) - pairs * group, 2 * hd), jnp.float32))
            out.append(jnp.concatenate(packed, axis=0))
        return out

    shift = shift_of(me)

    def attend_blocks(blocks):
        for b, m in zip(blocks, attend([(q_pad, shift, recv, b) for b in blocks])):
            msg[mt, b] = m
            for t in range(1, tp):
                msg_copy(b, lax.rem(mt + t, tp)).start()

    def attend_late(i, owners):
        for owner in owners:
            query_arrived(owner).wait_recv()
        part_v[mt, i] = jnp.concatenate(
            attend([(q_all.at[owner], shift_of(owner), send, owner) for owner in owners]), axis=0
        )
        for t in range(1, tp):
            part_copy(i, lax.rem(mt + t, tp)).start()

    def send_late(i, owners):
        for t in range(1, tp):
            part_arrived(i, lax.rem(mt + t, tp)).wait_recv()
        wait_bytes(part_v.at[pl.ds(0, tp - 1), i], psend_sem.at[i])
        total = part_v[tp - 1, i]
        acc = pltpu.roll(total, hd, 1)
        for j in range(tp - 2, -1, -1):
            m = part_v[j, i]
            total = total + jnp.exp(acc) * m
            acc = acc + pltpu.roll(m, hd, 1)
        block = jnp.where(late_half, pltpu.roll(acc, hd, 1), total)
        late_v[i] = block.reshape(late_v.shape[1:])
        for j, owner in enumerate(owners):
            late_copy(i, j, owner).start()

    owners = inward + near + outward
    owners = [owners[i:i + 2] for i in range(0, 3 * quarter, 2)]
    first = quarter // 2
    for i in range(first):
        attend_late(i, owners[i])

    @pl.when(jnp.logical_not(outer))
    def _():
        for i in range(first, len(owners)):
            attend_late(i, owners[i])

    for i in range(0, half, 2):
        for b in early[max(i, 1):i + 2]:
            arrived(b).wait_recv()
        attend_blocks(early[i:i + 2])

    for i in range(first):
        send_late(i, owners[i])

    @pl.when(jnp.logical_not(outer))
    def _():
        for i in range(first, len(owners)):
            send_late(i, owners[i])
        for i in range(first, len(owners)):
            wait_bytes(late_v.at[i], lsend_sem.at[i])

    wait_bytes(q_all.at[pl.ds(0, half)], qsend_sem)
    sent(quarter, 0)
    sent(sp - 1 - quarter, 1)
    for i in range(first):
        wait_bytes(late_v.at[i], lsend_sem.at[i])
    for b in late:
        arrived(b).wait_recv()
    some = msg.at[0, pl.ds(0, half)]
    for t in range(1, tp):
        wait_bytes(some, mrecv_sem.at[lax.rem(mt + t, tp)])
    for t in range(1, tp):
        wait_bytes(some, msend_sem)
    wait_bytes(some, lrecv_sem)


def finish(sp, tp, hd, group, pairs, recv, msg, stored_hbm, first_hbm, fin, first_v, out_sem, first_sem):
    copies = [
        pltpu.make_async_copy(recv.at[b, :, pl.ds(p * 2 * hd, 2 * hd)], stored_hbm.at[p, b], out_sem.at[b, p])
        for b in range(sp)
        for p in range(pairs)
    ]
    for copy in copies:
        copy.start()
    left_half = lax.broadcasted_iota(jnp.int32, (packed_rows(pairs, group), 2 * hd), 1) < hd

    def add_block(i, carry):
        total, acc = carry
        b = sp - 1 - i
        for j in range(tp - 1, -1, -1):
            m = msg[j, b]
            total = total + jnp.exp(acc) * m
            acc = acc + pltpu.roll(m, hd, 1)
        return total, acc

    zero = jnp.zeros((packed_rows(pairs, group), 2 * hd), jnp.float32)
    total, _ = lax.fori_loop(0, sp, add_block, (zero, zero), unroll=True)
    total = jnp.where(left_half, 0.0, total)
    squares = jnp.sum(total * total, axis=1, keepdims=True) * (1.0 / hd)
    fin[...] = pltpu.roll(total * lax.rsqrt(squares + EPS_NORM), hd, 1)
    cols = [fin[pl.ds(g, pairs, stride=group), :][:, :hd] for g in range(group)]
    first_v[...] = jnp.concatenate(cols, axis=1).astype(first_v.dtype)
    first_copy = pltpu.make_async_copy(first_v, first_hbm, first_sem)
    first_copy.start()

    for copy in copies:
        copy.wait()
    first_copy.wait()


def solution(mesh):
    sp, tp = mesh.shape["sp"], mesh.shape["tp"]

    def per_device(layer_input, key_weight, value_weight, queries, head_bias):
        seqs, sub, width = layer_input.shape
        pairs, group, hd = queries.shape
        kvh = head_bias.shape[0]
        x = layer_input.reshape(seqs * sub, width)
        block = pairs * 2 * hd
        any_spec = pl.BlockSpec(memory_space=pltpu.HBM)
        dma = pltpu.SemaphoreType.DMA
        handed = sp * sub * block * 2 + tp * sp * packed_rows(pairs, group) * 2 * hd * 4
        limit = VMEM_BYTES - handed
        late = sp // 4 * 3 // 2
        vmem_spec = pl.BlockSpec(memory_space=pltpu.VMEM)
        recv, msg = pl.pallas_call(
            functools.partial(kernel, sp, tp, seqs, sub, hd, kvh, group, pairs),
            out_shape=(
                pltpu.VMEM((sp, sub, block), jnp.bfloat16),
                pltpu.VMEM((tp, sp, packed_rows(pairs, group), 2 * hd), jnp.float32),
            ),
            in_specs=[any_spec] * 5,
            out_specs=(vmem_spec, vmem_spec),
            scratch_shapes=[
                pltpu.VMEM(x.shape, jnp.bfloat16),
                pltpu.VMEM((width, 2 * key_weight.shape[1]), jnp.bfloat16),
                pltpu.VMEM((group, pairs, hd), jnp.bfloat16),
                pltpu.VMEM(head_bias.shape, jnp.float32),
                pltpu.VMEM((sp, sub, block), jnp.bfloat16),
                pltpu.VMEM((pairs * ROWS, 2 * hd), jnp.bfloat16),
                pltpu.VMEM((sp, pairs * ROWS, 2 * hd), jnp.bfloat16),
                pltpu.VMEM((tp, late, 2 * packed_rows(pairs, group), 2 * hd), jnp.float32),
                pltpu.VMEM((late, 2, packed_rows(pairs, group), 2 * hd), jnp.float32),
                dma((2, KC)),
                dma((2, KC)),
                dma((2,)),
                dma((2,)),
                dma((sp,)),
                dma(()),
                dma((tp,)),
                dma(()),
                dma((sp,)),
                dma((late,)),
                dma((tp, late)),
                dma((late,)),
                dma(()),
            ],
            compiler_params=pltpu.CompilerParams(
                collective_id=0, has_side_effects=True, vmem_limit_bytes=limit
            ),
        )(x, key_weight, value_weight, queries.transpose(1, 0, 2), head_bias)
        return pl.pallas_call(
            functools.partial(finish, sp, tp, hd, group, pairs),
            out_shape=(
                jax.ShapeDtypeStruct((pairs, sp, sub, 2 * hd), jnp.bfloat16),
                jax.ShapeDtypeStruct((pairs, group * hd), jnp.bfloat16),
            ),
            in_specs=[vmem_spec, vmem_spec],
            out_specs=(any_spec, any_spec),
            scratch_shapes=[
                pltpu.VMEM((packed_rows(pairs, group), 2 * hd), jnp.float32),
                pltpu.VMEM((pairs, group * hd), jnp.bfloat16),
                dma((sp, pairs)),
                dma(()),
            ],
            compiler_params=pltpu.CompilerParams(vmem_limit_bytes=VMEM_BYTES // 4),
        )(recv, msg)

    in_specs = (P(None, ("sp", "tp"), None), P(), P(), P("sp", None, None), P())
    out_specs = (P("sp", None, "tp", None), P("sp", None))
    return jax.shard_map(per_device, mesh=mesh, in_specs=in_specs, out_specs=out_specs, check_vma=False)
```

```python
import functools
import math

import jax
import jax.numpy as jnp
from jax import lax
from jax.experimental import pallas as pl
from jax.experimental.pallas import tpu as pltpu
from jax.sharding import PartitionSpec as P

EPS_NORM = 0.0001
MESH = pl.DeviceIdType.MESH
KC = 4
VMEM_BYTES = 60 * 1024 * 1024
ROWS = 8


def flip(index, k):
    bit = 1
    while bit <= k:
        if k & bit:
            index = index + (1 - 2 * ((index // bit) % 2)) * bit
        bit *= 2
    return index


def packed_rows(pairs, group):
    return pairs * group // 8 * 8 + 8


def kernel(
    sp, tp, seqs, sub, hd, kvh, group, pairs,
    x_hbm, wk_hbm, wv_hbm, q_hbm, bias_hbm,
    recv, msg,
    x_v, w_v, q_v, bias_v, send, q_pad, q_all, part_v, late_v,
    x_sem, w_sem, small_sem, send_sem, recv_sem, mrecv_sem, qrecv_sem, precv_sem, lrecv_sem,
):
    me = lax.axis_index("sp")
    mt = lax.axis_index("tp")
    per_seq = kvh // pairs
    width = x_hbm.shape[1]
    kc = width // KC
    half_rows = seqs * sub // 2

    q_copy = pltpu.make_async_copy(q_hbm, q_v, small_sem.at[0])
    bias_copy = pltpu.make_async_copy(bias_hbm, bias_v, small_sem.at[1])
    q_copy.start()
    bias_copy.start()
    kv_width = wk_hbm.shape[1]

    def x_copy(c):
        at = (pl.ds(0, half_rows), pl.ds(c * kc, kc))
        return pltpu.make_async_copy(x_hbm.at[at], x_v.at[at], x_sem.at[c])

    def w_copy(i, c):
        rows = pl.ds(c * kc, kc)
        w_hbm = (wk_hbm, wv_hbm)[i]
        return pltpu.make_async_copy(w_hbm.at[rows], w_v.at[rows, pl.ds(i * kv_width, kv_width)], w_sem.at[c])

    rest = pl.ds(half_rows, half_rows)
    x_rest = pltpu.make_async_copy(x_hbm.at[rest], x_v.at[rest], x_sem.at[KC])
    for c in range(KC):
        x_copy(c).start()
        w_copy(0, c).start()
        w_copy(1, c).start()
    x_rest.start()

    msg[...] = jnp.zeros_like(msg)

    top = me // (sp // 2)
    half = sp // 2
    quarter = sp // 4
    lead = lax.rem(mt, 2)
    outer = lax.rem(me // quarter, 3) == 0
    inner = jnp.logical_not(outer)
    held = jnp.logical_and(inner, jnp.logical_and(top == 1, lead == 0))
    far_outer = (1 - top) * 3 * quarter
    far_inner = quarter + (1 - top) * quarter
    near = [flip(me, k) for k in range(quarter, half)]
    inward = [far_inner + flip(lax.rem(me, 2), j) for j in range(quarter)]
    outward = [far_outer + flip(lax.rem(me, 2), j) for j in range(quarter)]
    same = [flip(me, k) for k in range(1, quarter)]
    early = [jnp.where(outer, a, b) for a, b in zip(outward, near)]
    late = [jnp.where(outer, a, b) for a, b in zip(near, outward)]
    urgent = [jnp.where(top == 0, a, b) for a, b in zip(near, outward)]
    relaxed = [jnp.where(top == 0, a, b) for a, b in zip(outward, near)]

    barrier = pltpu.get_barrier_semaphore()
    for k in range(sp - 1, 0, -1):
        pl.semaphore_signal(barrier, inc=1, device_id={"sp": flip(me, k)}, device_id_type=MESH)
    for k in range(1, tp):
        pl.semaphore_signal(barrier, inc=1, device_id={"tp": lax.rem(mt + k, tp)}, device_id_type=MESH)

    def ask(owners):
        for owner in owners:
            pl.semaphore_signal(barrier, inc=1, device_id={"sp": owner, "tp": mt + 1}, device_id_type=MESH)

    @pl.when(lead == 0)
    def _():
        ask(inward)

        @pl.when(inner)
        def _():
            ask(near + outward)

    def wait_bytes(ref, sem):
        pltpu.make_async_copy(ref, ref, sem).wait()

    def pack(rows, base):
        for i in range(seqs // 2):
            for part in range(per_seq):
                out = []
                for p in range(pairs):
                    c0 = (part * pairs + p) * hd
                    out.append(rows[i * sub:(i + 1) * sub, c0:c0 + hd])
                    out.append(rows[i * sub:(i + 1) * sub, kv_width + c0:kv_width + c0 + hd])
                send[base + i * per_seq + part] = jnp.concatenate(out, axis=1).astype(jnp.bfloat16)

    def send_block(to):
        near_class = jnp.where(outer, 1, 2)
        place = jnp.where(to // half == top, near_class, jnp.where(to // quarter == far_outer // quarter, near_class, 2))
        place = jnp.where(to // quarter == me // quarter, 0, place)

        @pl.when(to != me)
        def _():
            pltpu.make_async_remote_copy(
                src_ref=send.at[to], dst_ref=recv.at[me],
                send_sem=send_sem, recv_sem=recv_sem.at[place],
                device_id={"sp": to}, device_id_type=MESH,
            ).start()

    def send_blocks(base, count):
        for j in range(count):
            send_block(base + j)

    def query_copy(to, core, place):
        return pltpu.make_async_remote_copy(
            src_ref=q_pad, dst_ref=q_all.at[me],
            send_sem=send_sem, recv_sem=qrecv_sem.at[place],
            device_id={"sp": to, "tp": mt - core}, device_id_type=MESH,
        )

    def enter():
        pl.semaphore_wait(barrier, sp + tp - 2 + half * lead)

        @pl.when(lead == 1)
        def _():
            for core in range(2):
                for to in late + inward:
                    query_copy(to, core, jnp.where(outer, 1 + top, 0)).start()

    def send_far():
        send_blocks(far_outer, quarter)

        @pl.when(jnp.logical_or(top == 0, jnp.logical_and(inner, lead == 1)))
        def _():
            send_blocks(far_inner, quarter)

    q_copy.wait()
    for p in range(pairs):
        qp = q_v[:, p, :].astype(jnp.float32)
        qp = jnp.concatenate([qp, jnp.zeros((group, hd), jnp.float32)], axis=1)
        qp = jnp.concatenate([qp, jnp.zeros((ROWS - group, 2 * hd), jnp.float32)], axis=0)
        q_pad[p * ROWS:(p + 1) * ROWS, :] = qp.astype(jnp.bfloat16)

    rows = None
    for c in range(KC):
        x_copy(c).wait()
        wait_bytes(w_v.at[pl.ds(c * kc, kc)], w_sem.at[c])
        part = jnp.dot(
            x_v[:half_rows, c * kc:(c + 1) * kc], w_v[c * kc:(c + 1) * kc, :],
            preferred_element_type=jnp.float32,
        )
        rows = part if rows is None else rows + part
    pack(rows, 0)

    @pl.when(top == 1)
    def _():
        enter()
        send_far()

    x_rest.wait()
    pack(jnp.dot(x_v[half_rows:, :], w_v[...], preferred_element_type=jnp.float32), half)

    @pl.when(top == 0)
    def _():
        enter()

    send_blocks(top * half, half)

    @pl.when(jnp.logical_and(top == 1, outer))
    def _():
        send_blocks(far_inner, quarter)

    @pl.when(top == 0)
    def _():
        send_far()

    recv[pl.ds(me, 1)] = send[pl.ds(me, 1)]

    bias_copy.wait()
    eye = lax.broadcasted_iota(jnp.int32, (ROWS, group), 0) == lax.broadcasted_iota(jnp.int32, (ROWS, group), 1)

    def shift_of(owner):
        h0 = lax.rem(owner * pairs, kvh)
        shifts = []
        for p in range(pairs):
            row = bias_v[pl.ds(h0 + p, 1), :]
            shifts.append(jnp.sum(jnp.where(eye, jnp.broadcast_to(row, (ROWS, group)), 0.0), axis=1, keepdims=True))
        return jnp.concatenate(shifts, axis=0)

    scale = 1.0 / math.sqrt(hd)
    later = lax.broadcasted_iota(jnp.int32, (sub, 256), 0)
    column = lax.broadcasted_iota(jnp.int32, (sub, 256), 1)
    tri = ((later > column) | (column >= 128)).astype(jnp.float32).astype(jnp.bfloat16)
    left_half = lax.broadcasted_iota(jnp.int32, (pairs * ROWS, 2 * hd), 1) < hd

    late_half = lax.broadcasted_iota(jnp.int32, (2 * packed_rows(pairs, group), 2 * hd), 1) < hd

    def msg_copy(b, t):
        return pltpu.make_async_remote_copy(
            src_ref=msg.at[mt, b], dst_ref=msg.at[mt, b],
            send_sem=send_sem, recv_sem=mrecv_sem,
            device_id={"tp": t}, device_id_type=MESH,
        )

    def part_copy(i, t):
        return pltpu.make_async_remote_copy(
            src_ref=part_v.at[mt, i], dst_ref=part_v.at[mt, i],
            send_sem=send_sem, recv_sem=precv_sem.at[i],
            device_id={"tp": t}, device_id_type=MESH,
        )

    def late_copy(i, j, to):
        return pltpu.make_async_remote_copy(
            src_ref=late_v.at[i, j], dst_ref=msg.at[tp - 1, me],
            send_sem=send_sem, recv_sem=lrecv_sem,
            device_id={"sp": to}, device_id_type=MESH,
        )

    def attend(items):
        scores = []
        shifts = []
        for queries, shift, rows, b in items:
            shifts.append(shift)
            for p in range(pairs):
                q = queries[p * ROWS:(p + 1) * ROWS, :]
                kv = rows[b, :, p * 2 * hd:(p + 1) * 2 * hd]
                scores.append(lax.dot_general(q, kv, (((1,), (1,)), ((), ())), preferred_element_type=jnp.float32))
        s = jnp.concatenate(scores, axis=0) * scale + jnp.concatenate(shifts, axis=0)
        low = jnp.log1p(jnp.exp(-jnp.abs(s)))
        keep = -(jnp.maximum(s, 0.0) + low)
        sig = jnp.minimum(s, 0.0) - low
        hi = keep.astype(jnp.bfloat16)
        rest = keep - hi.astype(jnp.float32)
        mid = rest.astype(jnp.bfloat16)
        lo = (rest - mid.astype(jnp.float32)).astype(jnp.bfloat16)
        sums = (
            jnp.dot(hi, tri, preferred_element_type=jnp.float32)
            + jnp.dot(mid, tri, preferred_element_type=jnp.float32)
            + jnp.dot(lo, tri, preferred_element_type=jnp.float32)
        )
        weights = jnp.exp(sig + sums[:, :sub]).astype(jnp.bfloat16)
        n = pairs * ROWS
        out = []
        for i, (_, _, rows, b) in enumerate(items):
            reads = []
            for p in range(pairs):
                kv = rows[b, :, p * 2 * hd:(p + 1) * 2 * hd]
                at = i * n + p * ROWS
                reads.append(jnp.dot(weights[at:at + ROWS], kv, preferred_element_type=jnp.float32))
            read = jnp.concatenate(reads, axis=0)
            both = jnp.where(left_half, sums[i * n:(i + 1) * n, 128:128 + 2 * hd], read)
            packed = [both[p * ROWS:p * ROWS + group] for p in range(pairs)]
            packed.append(jnp.zeros((packed_rows(pairs, group) - pairs * group, 2 * hd), jnp.float32))
            out.append(jnp.concatenate(packed, axis=0))
        return out

    shift = shift_of(me)

    def attend_blocks(blocks):
        for b, m in zip(blocks, attend([(q_pad, shift, recv, b) for b in blocks])):
            msg[mt, b] = m
            for t in range(1, tp):
                msg_copy(b, lax.rem(mt + t, tp)).start()

    def attend_late(i, owners):
        part_v[mt, i] = jnp.concatenate(
            attend([(q_all.at[owner], shift_of(owner), send, owner) for owner in owners]), axis=0
        )
        for t in range(1, tp):
            part_copy(i, lax.rem(mt + t, tp)).start()

    def send_late(i, owners):
        wait_bytes(part_v.at[pl.ds(0, tp - 1), i], precv_sem.at[i])
        total = part_v[tp - 1, i]
        acc = pltpu.roll(total, hd, 1)
        for j in range(tp - 2, -1, -1):
            m = part_v[j, i]
            total = total + jnp.exp(acc) * m
            acc = acc + pltpu.roll(m, hd, 1)
        block = jnp.where(late_half, pltpu.roll(acc, hd, 1), total)
        late_v[i] = block.reshape(late_v.shape[1:])
        for j, owner in enumerate(owners):
            late_copy(i, j, owner).start()

    owners = inward + urgent + relaxed
    owners = [owners[i:i + 2] for i in range(0, 3 * quarter, 2)]
    first = quarter // 2

    def attend_class(place):
        wait_bytes(q_all.at[pl.ds(0, quarter)], qrecv_sem.at[place])
        for i in range(place * first, (place + 1) * first):
            attend_late(i, owners[i])

    @pl.when(inner)
    def _():
        attend_class(1)

    attend_class(0)

    @pl.when(inner)
    def _():
        attend_class(2)

    landed = [me] + same
    wait_bytes(recv.at[pl.ds(0, quarter - 1)], recv_sem.at[0])
    for i in range(0, quarter, 2):
        attend_blocks(landed[i:i + 2])
    @pl.when(inner)
    def _():
        for i in range(first, 2 * first):
            send_late(i, owners[i])

    @pl.when(held)
    def _():
        send_blocks(far_inner, quarter)

    for i in range(first):
        send_late(i, owners[i])

    @pl.when(inner)
    def _():
        for i in range(2 * first, 3 * first):
            send_late(i, owners[i])

    wait_bytes(recv.at[pl.ds(0, quarter)], recv_sem.at[1])
    for i in range(0, quarter, 2):
        attend_blocks(early[i:i + 2])

    some = pl.ds(0, half)
    others = pl.ds(0, tp - 1)
    wait_bytes(recv.at[some], recv_sem.at[2])
    wait_bytes(send.at[pl.ds(0, sp - 1)], send_sem)
    wait_bytes(part_v.at[others, pl.ds(0, first)], send_sem)
    wait_bytes(late_v.at[pl.ds(0, first)], send_sem)

    @pl.when(inner)
    def _():
        wait_bytes(part_v.at[others, pl.ds(first, 2 * first)], send_sem)
        wait_bytes(late_v.at[pl.ds(first, 2 * first)], send_sem)

    @pl.when(lead == 1)
    def _():
        wait_bytes(q_all, send_sem)

    wait_bytes(msg.at[others, some], send_sem)
    wait_bytes(msg.at[others, some], mrecv_sem)
    wait_bytes(msg.at[0, some], lrecv_sem)


def finish(sp, tp, hd, group, pairs, recv, msg, stored_hbm, first_hbm, fin, first_v, out_sem, first_sem):
    copies = [
        pltpu.make_async_copy(recv.at[b, :, pl.ds(p * 2 * hd, 2 * hd)], stored_hbm.at[p, b], out_sem)
        for b in range(sp)
        for p in range(pairs)
    ]
    for copy in copies:
        copy.start()
    left_half = lax.broadcasted_iota(jnp.int32, (packed_rows(pairs, group), 2 * hd), 1) < hd

    def add_block(i, carry):
        total, acc = carry
        b = sp - 1 - i
        for j in range(tp - 1, -1, -1):
            m = msg[j, b]
            total = total + jnp.exp(acc) * m
            acc = acc + pltpu.roll(m, hd, 1)
        return total, acc

    zero = jnp.zeros((packed_rows(pairs, group), 2 * hd), jnp.float32)
    total, _ = lax.fori_loop(0, sp, add_block, (zero, zero), unroll=True)
    total = jnp.where(left_half, 0.0, total)
    squares = jnp.sum(total * total, axis=1, keepdims=True) * (1.0 / hd)
    fin[...] = pltpu.roll(total * lax.rsqrt(squares + EPS_NORM), hd, 1)
    cols = [fin[pl.ds(g, pairs, stride=group), :][:, :hd] for g in range(group)]
    first_v[...] = jnp.concatenate(cols, axis=1).astype(first_v.dtype)
    first_copy = pltpu.make_async_copy(first_v, first_hbm, first_sem)
    first_copy.start()

    pltpu.make_async_copy(recv, recv, out_sem).wait()
    first_copy.wait()


def solution(mesh):
    sp, tp = mesh.shape["sp"], mesh.shape["tp"]

    def per_device(layer_input, key_weight, value_weight, queries, head_bias):
        seqs, sub, width = layer_input.shape
        pairs, group, hd = queries.shape
        kvh = head_bias.shape[0]
        x = layer_input.reshape(seqs * sub, width)
        block = pairs * 2 * hd
        any_spec = pl.BlockSpec(memory_space=pltpu.HBM)
        dma = pltpu.SemaphoreType.DMA
        handed = sp * sub * block * 2 + tp * sp * packed_rows(pairs, group) * 2 * hd * 4
        limit = VMEM_BYTES - handed
        late = sp // 4 * 3 // 2
        vmem_spec = pl.BlockSpec(memory_space=pltpu.VMEM)
        recv, msg = pl.pallas_call(
            functools.partial(kernel, sp, tp, seqs, sub, hd, kvh, group, pairs),
            out_shape=(
                pltpu.VMEM((sp, sub, block), jnp.bfloat16),
                pltpu.VMEM((tp, sp, packed_rows(pairs, group), 2 * hd), jnp.float32),
            ),
            in_specs=[any_spec] * 5,
            out_specs=(vmem_spec, vmem_spec),
            scratch_shapes=[
                pltpu.VMEM(x.shape, jnp.bfloat16),
                pltpu.VMEM((width, 2 * key_weight.shape[1]), jnp.bfloat16),
                pltpu.VMEM((group, pairs, hd), jnp.bfloat16),
                pltpu.VMEM(head_bias.shape, jnp.float32),
                pltpu.VMEM((sp, sub, block), jnp.bfloat16),
                pltpu.VMEM((pairs * ROWS, 2 * hd), jnp.bfloat16),
                pltpu.VMEM((sp, pairs * ROWS, 2 * hd), jnp.bfloat16),
                pltpu.VMEM((tp, late, 2 * packed_rows(pairs, group), 2 * hd), jnp.float32),
                pltpu.VMEM((late, 2, packed_rows(pairs, group), 2 * hd), jnp.float32),
                dma((KC + 1,)),
                dma((KC,)),
                dma((2,)),
                dma(()),
                dma((3,)),
                dma(()),
                dma((3,)),
                dma((late,)),
                dma(()),
            ],
            compiler_params=pltpu.CompilerParams(
                collective_id=0, has_side_effects=True, vmem_limit_bytes=limit
            ),
        )(x, key_weight, value_weight, queries.transpose(1, 0, 2), head_bias)
        return pl.pallas_call(
            functools.partial(finish, sp, tp, hd, group, pairs),
            out_shape=(
                jax.ShapeDtypeStruct((pairs, sp, sub, 2 * hd), jnp.bfloat16),
                jax.ShapeDtypeStruct((pairs, group * hd), jnp.bfloat16),
            ),
            in_specs=[vmem_spec, vmem_spec],
            out_specs=(any_spec, any_spec),
            scratch_shapes=[
                pltpu.VMEM((packed_rows(pairs, group), 2 * hd), jnp.float32),
                pltpu.VMEM((pairs, group * hd), jnp.bfloat16),
                dma(()),
                dma(()),
            ],
            compiler_params=pltpu.CompilerParams(vmem_limit_bytes=VMEM_BYTES // 4),
        )(recv, msg)

    in_specs = (P(None, ("sp", "tp"), None), P(), P(), P("sp", None, None), P())
    out_specs = (P("sp", None, "tp", None), P("sp", None))
    return jax.shard_map(per_device, mesh=mesh, in_specs=in_specs, out_specs=out_specs, check_vma=False)
```

```python
import functools
import math

import jax
import jax.numpy as jnp
from jax import lax
from jax.experimental import pallas as pl
from jax.experimental.pallas import tpu as pltpu
from jax.sharding import PartitionSpec as P

EPS_NORM = 0.0001
MESH = pl.DeviceIdType.MESH
KC = 4
VMEM_BYTES = 60 * 1024 * 1024
ROWS = 8


def flip(index, k):
    bit = 1
    while bit <= k:
        if k & bit:
            index = index + (1 - 2 * ((index // bit) % 2)) * bit
        bit *= 2
    return index


def packed_rows(pairs, group):
    return pairs * group // 8 * 8 + 8


def kernel(
    sp, tp, seqs, sub, hd, kvh, group, pairs,
    x_hbm, wk_hbm, wv_hbm, q_hbm, bias_hbm,
    recv, msg,
    x_v, w_v, q_v, bias_v, send, q_pad, q_all, part_v, late_v,
    x_sem, w_sem, small_sem, send_sem, recv_sem, mrecv_sem, qrecv_sem, precv_sem, lrecv_sem,
):
    me = lax.axis_index("sp")
    mt = lax.axis_index("tp")
    per_seq = kvh // pairs
    width = x_hbm.shape[1]
    kc = width // KC
    half_rows = seqs * sub // 2

    q_copy = pltpu.make_async_copy(q_hbm, q_v, small_sem.at[0])
    bias_copy = pltpu.make_async_copy(bias_hbm, bias_v, small_sem.at[1])
    q_copy.start()
    bias_copy.start()
    kv_width = wk_hbm.shape[1]

    def x_copy(c):
        at = (pl.ds(0, half_rows), pl.ds(c * kc, kc))
        return pltpu.make_async_copy(x_hbm.at[at], x_v.at[at], x_sem.at[c])

    def w_copy(i, c):
        rows = pl.ds(c * kc, kc)
        w_hbm = (wk_hbm, wv_hbm)[i]
        return pltpu.make_async_copy(w_hbm.at[rows], w_v.at[rows, pl.ds(i * kv_width, kv_width)], w_sem.at[c])

    rest = pl.ds(half_rows, half_rows)
    x_rest = pltpu.make_async_copy(x_hbm.at[rest], x_v.at[rest], x_sem.at[KC])
    for c in range(KC):
        x_copy(c).start()
        w_copy(0, c).start()
        w_copy(1, c).start()
    x_rest.start()

    msg[...] = jnp.zeros_like(msg)

    top = me // (sp // 2)
    half = sp // 2
    quarter = sp // 4
    lead = lax.rem(mt, 2)
    outer = lax.rem(me // quarter, 3) == 0
    inner = jnp.logical_not(outer)
    home = me // quarter == 0
    chips = tp // 2
    far_outer = (1 - top) * 3 * quarter
    far_inner = quarter + (1 - top) * quarter
    near = [flip(me, k) for k in range(quarter, half)]
    inward = [far_inner + flip(lax.rem(me, 2), j) for j in range(quarter)]
    outward = [far_outer + flip(lax.rem(me, 2), j) for j in range(quarter)]
    same = [flip(me, k) for k in range(1, quarter)]
    early = [jnp.where(outer, a, b) for a, b in zip(outward, near)]
    late = [jnp.where(outer, a, b) for a, b in zip(near, outward)]
    urgent = [jnp.where(top == 0, a, b) for a, b in zip(near, outward)]
    relaxed = [jnp.where(top == 0, a, b) for a, b in zip(outward, near)]

    barrier = pltpu.get_barrier_semaphore()
    for k in range(sp - 1, 0, -1):
        pl.semaphore_signal(barrier, inc=1, device_id={"sp": flip(me, k)}, device_id_type=MESH)
    for k in range(1, tp):
        pl.semaphore_signal(barrier, inc=1, device_id={"tp": lax.rem(mt + k, tp)}, device_id_type=MESH)

    @pl.when(home)
    def _():
        for t in range(1, tp, 2):
            for to in range(quarter, 3 * quarter):

                @pl.when(t != mt)
                def _():
                    pl.semaphore_signal(barrier, inc=1, device_id={"sp": to, "tp": t}, device_id_type=MESH)

    def ask(owners):
        for owner in owners:
            pl.semaphore_signal(barrier, inc=1, device_id={"sp": owner, "tp": mt + 1}, device_id_type=MESH)

    @pl.when(lead == 0)
    def _():
        ask(inward)

        @pl.when(inner)
        def _():
            ask(near + outward)

    def wait_bytes(ref, sem):
        pltpu.make_async_copy(ref, ref, sem).wait()

    def pack(rows, base):
        for i in range(seqs // 2):
            for part in range(per_seq):
                out = []
                for p in range(pairs):
                    c0 = (part * pairs + p) * hd
                    out.append(rows[i * sub:(i + 1) * sub, c0:c0 + hd])
                    out.append(rows[i * sub:(i + 1) * sub, kv_width + c0:kv_width + c0 + hd])
                send[base + i * per_seq + part] = jnp.concatenate(out, axis=1).astype(jnp.bfloat16)

    def send_block(to):
        near_class = jnp.where(outer, 1, 2)
        place = jnp.where(to // half == top, near_class, jnp.where(to // quarter == far_outer // quarter, near_class, 2))
        place = jnp.where(to // quarter == me // quarter, 0, place)

        @pl.when(to != me)
        def _():
            pltpu.make_async_remote_copy(
                src_ref=send.at[to], dst_ref=recv.at[me],
                send_sem=send_sem, recv_sem=recv_sem.at[place],
                device_id={"sp": to}, device_id_type=MESH,
            ).start()

    def send_blocks(base, count):
        for j in range(count):
            send_block(base + j)

    def query_copy(to, core, place):
        return pltpu.make_async_remote_copy(
            src_ref=q_pad, dst_ref=q_all.at[me],
            send_sem=send_sem, recv_sem=qrecv_sem.at[place],
            device_id={"sp": to, "tp": mt - core}, device_id_type=MESH,
        )

    def enter():
        pl.semaphore_wait(barrier, sp + tp - 2 + lead * (half + jnp.where(inner, quarter * (tp - 1), 0)))

        @pl.when(lead == 1)
        def _():
            for core in range(2):
                for to in late + inward:
                    query_copy(to, core, jnp.where(outer, 1 + top, 0)).start()

    q_copy.wait()
    for p in range(pairs):
        qp = q_v[:, p, :].astype(jnp.float32)
        qp = jnp.concatenate([qp, jnp.zeros((group, hd), jnp.float32)], axis=1)
        qp = jnp.concatenate([qp, jnp.zeros((ROWS - group, 2 * hd), jnp.float32)], axis=0)
        q_pad[p * ROWS:(p + 1) * ROWS, :] = qp.astype(jnp.bfloat16)

    rows = None
    for c in range(KC):
        x_copy(c).wait()
        wait_bytes(w_v.at[pl.ds(c * kc, kc)], w_sem.at[c])
        part = jnp.dot(
            x_v[:half_rows, c * kc:(c + 1) * kc], w_v[c * kc:(c + 1) * kc, :],
            preferred_element_type=jnp.float32,
        )
        rows = part if rows is None else rows + part
    pack(rows, 0)

    @pl.when(top == 1)
    def _():
        enter()
        send_blocks(far_outer, quarter)

    x_rest.wait()
    pack(jnp.dot(x_v[half_rows:, :], w_v[...], preferred_element_type=jnp.float32), half)

    @pl.when(top == 0)
    def _():
        enter()

    send_blocks(top * half, half)

    @pl.when(top == 0)
    def _():
        send_blocks(far_outer, quarter)

    @pl.when(outer)
    def _():
        send_blocks(far_inner, quarter)

    recv[pl.ds(me, 1)] = send[pl.ds(me, 1)]

    bias_copy.wait()
    eye = lax.broadcasted_iota(jnp.int32, (ROWS, group), 0) == lax.broadcasted_iota(jnp.int32, (ROWS, group), 1)

    def shift_of(owner):
        h0 = lax.rem(owner * pairs, kvh)
        shifts = []
        for p in range(pairs):
            row = bias_v[pl.ds(h0 + p, 1), :]
            shifts.append(jnp.sum(jnp.where(eye, jnp.broadcast_to(row, (ROWS, group)), 0.0), axis=1, keepdims=True))
        return jnp.concatenate(shifts, axis=0)

    scale = 1.0 / math.sqrt(hd)
    later = lax.broadcasted_iota(jnp.int32, (sub, 256), 0)
    column = lax.broadcasted_iota(jnp.int32, (sub, 256), 1)
    tri = ((later > column) | (column >= 128)).astype(jnp.float32).astype(jnp.bfloat16)
    left_half = lax.broadcasted_iota(jnp.int32, (pairs * ROWS, 2 * hd), 1) < hd

    late_half = lax.broadcasted_iota(jnp.int32, (2 * packed_rows(pairs, group), 2 * hd), 1) < hd

    def msg_copy(b, t):
        return pltpu.make_async_remote_copy(
            src_ref=msg.at[mt, b], dst_ref=msg.at[mt, b],
            send_sem=send_sem, recv_sem=mrecv_sem,
            device_id={"tp": t}, device_id_type=MESH,
        )

    def part_copy(i, t):
        return pltpu.make_async_remote_copy(
            src_ref=part_v.at[mt, i], dst_ref=part_v.at[mt, i],
            send_sem=send_sem, recv_sem=precv_sem.at[i],
            device_id={"tp": t}, device_id_type=MESH,
        )

    def late_copy(i, j, to, slot, there):
        return pltpu.make_async_remote_copy(
            src_ref=late_v.at[i, j], dst_ref=msg.at[slot, me],
            send_sem=send_sem, recv_sem=lrecv_sem,
            device_id={"sp": to, "tp": there}, device_id_type=MESH,
        )

    def attend(items):
        scores = []
        shifts = []
        for queries, shift, rows, b in items:
            shifts.append(shift)
            for p in range(pairs):
                q = queries[p * ROWS:(p + 1) * ROWS, :]
                kv = rows[b, :, p * 2 * hd:(p + 1) * 2 * hd]
                scores.append(lax.dot_general(q, kv, (((1,), (1,)), ((), ())), preferred_element_type=jnp.float32))
        s = jnp.concatenate(scores, axis=0) * scale + jnp.concatenate(shifts, axis=0)
        low = jnp.log1p(jnp.exp(-jnp.abs(s)))
        keep = -(jnp.maximum(s, 0.0) + low)
        sig = jnp.minimum(s, 0.0) - low
        hi = keep.astype(jnp.bfloat16)
        rest = keep - hi.astype(jnp.float32)
        mid = rest.astype(jnp.bfloat16)
        lo = (rest - mid.astype(jnp.float32)).astype(jnp.bfloat16)
        sums = (
            jnp.dot(hi, tri, preferred_element_type=jnp.float32)
            + jnp.dot(mid, tri, preferred_element_type=jnp.float32)
            + jnp.dot(lo, tri, preferred_element_type=jnp.float32)
        )
        weights = jnp.exp(sig + sums[:, :sub]).astype(jnp.bfloat16)
        n = pairs * ROWS
        out = []
        for i, (_, _, rows, b) in enumerate(items):
            reads = []
            for p in range(pairs):
                kv = rows[b, :, p * 2 * hd:(p + 1) * 2 * hd]
                at = i * n + p * ROWS
                reads.append(jnp.dot(weights[at:at + ROWS], kv, preferred_element_type=jnp.float32))
            read = jnp.concatenate(reads, axis=0)
            both = jnp.where(left_half, sums[i * n:(i + 1) * n, 128:128 + 2 * hd], read)
            packed = [both[p * ROWS:p * ROWS + group] for p in range(pairs)]
            packed.append(jnp.zeros((packed_rows(pairs, group) - pairs * group, 2 * hd), jnp.float32))
            out.append(jnp.concatenate(packed, axis=0))
        return out

    shift = shift_of(me)

    def attend_blocks(blocks):
        for b, m in zip(blocks, attend([(q_pad, shift, recv, b) for b in blocks])):
            msg[mt, b] = m
            for t in range(1, tp):
                msg_copy(b, lax.rem(mt + t, tp)).start()

    def attend_late(i, owners):
        part_v[mt, i] = jnp.concatenate(
            attend([(q_all.at[owner], shift_of(owner), send, owner) for owner in owners]), axis=0
        )

    def store_late(i, parts):
        total = parts[0]
        acc = pltpu.roll(total, hd, 1)
        for m in parts[1:]:
            total = total + jnp.exp(acc) * m
            acc = acc + pltpu.roll(m, hd, 1)
        block = jnp.where(late_half, pltpu.roll(acc, hd, 1), total)
        late_v[i] = block.reshape(late_v.shape[1:])

    def send_late(i, owners):
        wait_bytes(part_v.at[pl.ds(0, tp - 1), i], precv_sem.at[i])
        store_late(i, [part_v[j, i] for j in range(tp - 1, -1, -1)])
        for j, owner in enumerate(owners):
            late_copy(i, j, owner, tp - 1, mt).start()

    def send_urgent(i, owners):
        wait_bytes(part_v.at[0, i], precv_sem.at[i])
        store_late(i, [part_v[mt, i], part_v[mt - 1, i]])
        for j, owner in enumerate(owners):
            for t in range(tp):
                late_copy(i, j, owner, mt, t).start()

    owners = inward + urgent + relaxed
    owners = [owners[i:i + 2] for i in range(0, 3 * quarter, 2)]
    first = quarter // 2

    def attend_class(place):
        wait_bytes(q_all.at[pl.ds(0, quarter)], qrecv_sem.at[place])
        for i in range(place * first, (place + 1) * first):
            attend_late(i, owners[i])
            if place != 1:
                for t in range(1, tp):
                    part_copy(i, lax.rem(mt + t, tp)).start()
            else:

                @pl.when(lead == 0)
                def _():
                    part_copy(i, mt + 1).start()

    @pl.when(inner)
    def _():
        attend_class(1)

    attend_class(0)

    @pl.when(inner)
    def _():
        attend_class(2)

    landed = [me] + same
    wait_bytes(recv.at[pl.ds(0, quarter - 1)], recv_sem.at[0])
    for i in range(0, quarter, 2):
        attend_blocks(landed[i:i + 2])
    @pl.when(jnp.logical_and(inner, lead == 1))
    def _():
        for i in range(first, 2 * first):
            send_urgent(i, owners[i])

    @pl.when(inner)
    def _():
        send_blocks(far_inner, first)

    for i in range(first):
        send_late(i, owners[i])

    @pl.when(inner)
    def _():
        send_blocks(far_inner + first, quarter - first)

    @pl.when(inner)
    def _():
        for i in range(2 * first, 3 * first):
            send_late(i, owners[i])

    wait_bytes(recv.at[pl.ds(0, quarter)], recv_sem.at[1])
    for i in range(0, quarter, 2):
        attend_blocks(early[i:i + 2])

    some = pl.ds(0, half)
    others = pl.ds(0, tp - 1)
    wait_bytes(recv.at[some], recv_sem.at[2])
    wait_bytes(send.at[pl.ds(0, sp - 1)], send_sem)
    wait_bytes(part_v.at[others, pl.ds(0, first)], send_sem)
    wait_bytes(late_v.at[pl.ds(0, first)], send_sem)

    @pl.when(inner)
    def _():
        wait_bytes(part_v.at[others, pl.ds(2 * first, first)], send_sem)
        wait_bytes(late_v.at[pl.ds(2 * first, first)], send_sem)

        @pl.when(lead == 0)
        def _():
            wait_bytes(part_v.at[0, pl.ds(first, first)], send_sem)

        @pl.when(lead == 1)
        def _():
            for _ in range(tp):
                wait_bytes(late_v.at[pl.ds(first, first)], send_sem)

    @pl.when(lead == 1)
    def _():
        wait_bytes(q_all, send_sem)

    wait_bytes(msg.at[others, some], send_sem)
    wait_bytes(msg.at[others, some], mrecv_sem)

    @pl.when(home)
    def _():
        wait_bytes(msg.at[pl.ds(0, chips), some], lrecv_sem)

    @pl.when(jnp.logical_not(home))
    def _():
        wait_bytes(msg.at[0, some], lrecv_sem)


def finish(sp, tp, hd, group, pairs, recv, msg, stored_hbm, first_hbm, fin, first_v, out_sem, first_sem):
    copies = [
        pltpu.make_async_copy(recv.at[b, :, pl.ds(p * 2 * hd, 2 * hd)], stored_hbm.at[p, b], out_sem)
        for b in range(sp)
        for p in range(pairs)
    ]
    for copy in copies:
        copy.start()
    left_half = lax.broadcasted_iota(jnp.int32, (packed_rows(pairs, group), 2 * hd), 1) < hd

    def add_block(i, carry):
        total, acc = carry
        b = sp - 1 - i
        for j in range(tp - 1, -1, -1):
            m = msg[j, b]
            total = total + jnp.exp(acc) * m
            acc = acc + pltpu.roll(m, hd, 1)
        return total, acc

    zero = jnp.zeros((packed_rows(pairs, group), 2 * hd), jnp.float32)
    total, _ = lax.fori_loop(0, sp, add_block, (zero, zero), unroll=True)
    total = jnp.where(left_half, 0.0, total)
    squares = jnp.sum(total * total, axis=1, keepdims=True) * (1.0 / hd)
    fin[...] = pltpu.roll(total * lax.rsqrt(squares + EPS_NORM), hd, 1)
    cols = [fin[pl.ds(g, pairs, stride=group), :][:, :hd] for g in range(group)]
    first_v[...] = jnp.concatenate(cols, axis=1).astype(first_v.dtype)
    first_copy = pltpu.make_async_copy(first_v, first_hbm, first_sem)
    first_copy.start()

    pltpu.make_async_copy(recv, recv, out_sem).wait()
    first_copy.wait()


def solution(mesh):
    sp, tp = mesh.shape["sp"], mesh.shape["tp"]

    def per_device(layer_input, key_weight, value_weight, queries, head_bias):
        seqs, sub, width = layer_input.shape
        pairs, group, hd = queries.shape
        kvh = head_bias.shape[0]
        x = layer_input.reshape(seqs * sub, width)
        block = pairs * 2 * hd
        any_spec = pl.BlockSpec(memory_space=pltpu.HBM)
        dma = pltpu.SemaphoreType.DMA
        handed = sp * sub * block * 2 + tp * sp * packed_rows(pairs, group) * 2 * hd * 4
        limit = VMEM_BYTES - handed
        late = sp // 4 * 3 // 2
        vmem_spec = pl.BlockSpec(memory_space=pltpu.VMEM)
        recv, msg = pl.pallas_call(
            functools.partial(kernel, sp, tp, seqs, sub, hd, kvh, group, pairs),
            out_shape=(
                pltpu.VMEM((sp, sub, block), jnp.bfloat16),
                pltpu.VMEM((tp, sp, packed_rows(pairs, group), 2 * hd), jnp.float32),
            ),
            in_specs=[any_spec] * 5,
            out_specs=(vmem_spec, vmem_spec),
            scratch_shapes=[
                pltpu.VMEM(x.shape, jnp.bfloat16),
                pltpu.VMEM((width, 2 * key_weight.shape[1]), jnp.bfloat16),
                pltpu.VMEM((group, pairs, hd), jnp.bfloat16),
                pltpu.VMEM(head_bias.shape, jnp.float32),
                pltpu.VMEM((sp, sub, block), jnp.bfloat16),
                pltpu.VMEM((pairs * ROWS, 2 * hd), jnp.bfloat16),
                pltpu.VMEM((sp, pairs * ROWS, 2 * hd), jnp.bfloat16),
                pltpu.VMEM((tp, late, 2 * packed_rows(pairs, group), 2 * hd), jnp.float32),
                pltpu.VMEM((late, 2, packed_rows(pairs, group), 2 * hd), jnp.float32),
                dma((KC + 1,)),
                dma((KC,)),
                dma((2,)),
                dma(()),
                dma((3,)),
                dma(()),
                dma((3,)),
                dma((late,)),
                dma(()),
            ],
            compiler_params=pltpu.CompilerParams(
                collective_id=0, has_side_effects=True, vmem_limit_bytes=limit
            ),
        )(x, key_weight, value_weight, queries.transpose(1, 0, 2), head_bias)
        return pl.pallas_call(
            functools.partial(finish, sp, tp, hd, group, pairs),
            out_shape=(
                jax.ShapeDtypeStruct((pairs, sp, sub, 2 * hd), jnp.bfloat16),
                jax.ShapeDtypeStruct((pairs, group * hd), jnp.bfloat16),
            ),
            in_specs=[vmem_spec, vmem_spec],
            out_specs=(any_spec, any_spec),
            scratch_shapes=[
                pltpu.VMEM((packed_rows(pairs, group), 2 * hd), jnp.float32),
                pltpu.VMEM((pairs, group * hd), jnp.bfloat16),
                dma(()),
                dma(()),
            ],
            compiler_params=pltpu.CompilerParams(vmem_limit_bytes=VMEM_BYTES // 4),
        )(recv, msg)

    in_specs = (P(None, ("sp", "tp"), None), P(), P(), P("sp", None, None), P())
    out_specs = (P("sp", None, "tp", None), P("sp", None))
    return jax.shard_map(per_device, mesh=mesh, in_specs=in_specs, out_specs=out_specs, check_vma=False)
```

```python
import functools
import math

import jax
import jax.numpy as jnp
from jax import lax
from jax.experimental import pallas as pl
from jax.experimental.pallas import tpu as pltpu
from jax.sharding import PartitionSpec as P

EPS_NORM = 0.0001
MESH = pl.DeviceIdType.MESH
KC = 4
VMEM_BYTES = 60 * 1024 * 1024
ROWS = 8


def flip(index, k):
    bit = 1
    while bit <= k:
        if k & bit:
            index = index + (1 - 2 * ((index // bit) % 2)) * bit
        bit *= 2
    return index


def packed_rows(pairs, group):
    return pairs * group // 8 * 8 + 8


def kernel(
    sp, tp, seqs, sub, hd, kvh, group, pairs,
    x_hbm, wk_hbm, wv_hbm, q_hbm, bias_hbm,
    recv, msg,
    x_v, w_v, q_v, bias_v, send, q_pad, q_all, part_v, late_v, late_b, late_in,
    x_sem, w_sem, small_sem, send_sem, recv_sem, mrecv_sem, qrecv_sem, precv_sem, lrecv_sem,
):
    me = lax.axis_index("sp")
    mt = lax.axis_index("tp")
    per_seq = kvh // pairs
    width = x_hbm.shape[1]
    kc = width // KC
    half_rows = seqs * sub // 2

    q_copy = pltpu.make_async_copy(q_hbm, q_v, small_sem.at[0])
    bias_copy = pltpu.make_async_copy(bias_hbm, bias_v, small_sem.at[1])
    q_copy.start()
    bias_copy.start()
    kv_width = wk_hbm.shape[1]

    def x_copy(c):
        at = (pl.ds(0, half_rows), pl.ds(c * kc, kc))
        return pltpu.make_async_copy(x_hbm.at[at], x_v.at[at], x_sem.at[c])

    def w_copy(i, c):
        rows = pl.ds(c * kc, kc)
        w_hbm = (wk_hbm, wv_hbm)[i]
        return pltpu.make_async_copy(w_hbm.at[rows], w_v.at[rows, pl.ds(i * kv_width, kv_width)], w_sem.at[c])

    rest = pl.ds(half_rows, half_rows)
    x_rest = pltpu.make_async_copy(x_hbm.at[rest], x_v.at[rest], x_sem.at[KC])
    for c in range(KC):
        x_copy(c).start()
        w_copy(0, c).start()
        w_copy(1, c).start()
    x_rest.start()

    msg[...] = jnp.zeros_like(msg)

    top = me // (sp // 2)
    half = sp // 2
    quarter = sp // 4
    lead = lax.rem(mt, 2)
    outer = lax.rem(me // quarter, 3) == 0
    inner = jnp.logical_not(outer)
    home = me // quarter == 0
    chips = tp // 2
    far_outer = (1 - top) * 3 * quarter
    far_inner = quarter + (1 - top) * quarter
    near = [flip(me, k) for k in range(quarter, half)]
    inward = [far_inner + flip(lax.rem(me, 2), j) for j in range(quarter)]
    outward = [far_outer + flip(lax.rem(me, 2), j) for j in range(quarter)]
    same = [flip(me, k) for k in range(1, quarter)]
    early = [jnp.where(outer, a, b) for a, b in zip(outward, near)]
    late = [jnp.where(outer, a, b) for a, b in zip(near, outward)]
    urgent = [jnp.where(top == 0, a, b) for a, b in zip(near, outward)]
    relaxed = [jnp.where(top == 0, a, b) for a, b in zip(outward, near)]

    barrier = pltpu.get_barrier_semaphore()
    for k in range(sp - 1, 0, -1):
        pl.semaphore_signal(barrier, inc=1, device_id={"sp": flip(me, k)}, device_id_type=MESH)
    for k in range(1, tp):
        pl.semaphore_signal(barrier, inc=1, device_id={"tp": lax.rem(mt + k, tp)}, device_id_type=MESH)

    @pl.when(home)
    def _():
        for t in range(1, tp, 2):
            for to in range(quarter, 3 * quarter):

                @pl.when(t != mt)
                def _():
                    pl.semaphore_signal(barrier, inc=1, device_id={"sp": to, "tp": t}, device_id_type=MESH)

    def ask(owners):
        for owner in owners:
            pl.semaphore_signal(barrier, inc=1, device_id={"sp": owner, "tp": mt + 1}, device_id_type=MESH)

    @pl.when(lead == 0)
    def _():
        ask(inward)

        @pl.when(inner)
        def _():
            ask(near + outward)

    def wait_bytes(ref, sem):
        pltpu.make_async_copy(ref, ref, sem).wait()

    def pack(rows, base):
        for i in range(seqs // 2):
            for part in range(per_seq):
                out = []
                for p in range(pairs):
                    c0 = (part * pairs + p) * hd
                    out.append(rows[i * sub:(i + 1) * sub, c0:c0 + hd])
                    out.append(rows[i * sub:(i + 1) * sub, kv_width + c0:kv_width + c0 + hd])
                send[base + i * per_seq + part] = jnp.concatenate(out, axis=1).astype(jnp.bfloat16)

    def send_block(to):
        near_class = jnp.where(outer, 1, 2)
        place = jnp.where(to // half == top, near_class, jnp.where(to // quarter == far_outer // quarter, near_class, 2))
        place = jnp.where(to // quarter == me // quarter, 0, place)

        @pl.when(to != me)
        def _():
            pltpu.make_async_remote_copy(
                src_ref=send.at[to], dst_ref=recv.at[me],
                send_sem=send_sem, recv_sem=recv_sem.at[place],
                device_id={"sp": to}, device_id_type=MESH,
            ).start()

    def send_blocks(base, count):
        for j in range(count):
            send_block(base + j)

    def query_copy(to, core, place):
        return pltpu.make_async_remote_copy(
            src_ref=q_pad, dst_ref=q_all.at[me],
            send_sem=send_sem, recv_sem=qrecv_sem.at[place],
            device_id={"sp": to, "tp": mt - core}, device_id_type=MESH,
        )

    def enter():
        pl.semaphore_wait(barrier, sp + tp - 2 + lead * (half + jnp.where(inner, quarter * (tp - 1), 0)))

        @pl.when(lead == 1)
        def _():
            for core in range(2):
                for to in late + inward:
                    query_copy(to, core, jnp.where(outer, 1 + top, 0)).start()

    q_copy.wait()
    for p in range(pairs):
        qp = q_v[:, p, :].astype(jnp.float32)
        qp = jnp.concatenate([qp, jnp.zeros((group, hd), jnp.float32)], axis=1)
        qp = jnp.concatenate([qp, jnp.zeros((ROWS - group, 2 * hd), jnp.float32)], axis=0)
        q_pad[p * ROWS:(p + 1) * ROWS, :] = qp.astype(jnp.bfloat16)

    rows = None
    for c in range(KC):
        x_copy(c).wait()
        wait_bytes(w_v.at[pl.ds(c * kc, kc)], w_sem.at[c])
        part = jnp.dot(
            x_v[:half_rows, c * kc:(c + 1) * kc], w_v[c * kc:(c + 1) * kc, :],
            preferred_element_type=jnp.float32,
        )
        rows = part if rows is None else rows + part
    pack(rows, 0)

    @pl.when(top == 1)
    def _():
        enter()
        send_blocks(far_outer, quarter)

    x_rest.wait()
    pack(jnp.dot(x_v[half_rows:, :], w_v[...], preferred_element_type=jnp.float32), half)

    @pl.when(top == 0)
    def _():
        enter()

    send_blocks(top * half, half)

    @pl.when(top == 0)
    def _():
        send_blocks(far_outer, quarter)

    @pl.when(outer)
    def _():
        send_blocks(far_inner, quarter)

    recv[pl.ds(me, 1)] = send[pl.ds(me, 1)]

    bias_copy.wait()
    eye = lax.broadcasted_iota(jnp.int32, (ROWS, group), 0) == lax.broadcasted_iota(jnp.int32, (ROWS, group), 1)

    def shift_of(owner):
        h0 = lax.rem(owner * pairs, kvh)
        shifts = []
        for p in range(pairs):
            row = bias_v[pl.ds(h0 + p, 1), :]
            shifts.append(jnp.sum(jnp.where(eye, jnp.broadcast_to(row, (ROWS, group)), 0.0), axis=1, keepdims=True))
        return jnp.concatenate(shifts, axis=0)

    scale = 1.0 / math.sqrt(hd)
    later = lax.broadcasted_iota(jnp.int32, (sub, 256), 0)
    column = lax.broadcasted_iota(jnp.int32, (sub, 256), 1)
    tri = ((later > column) | (column >= 128)).astype(jnp.float32).astype(jnp.bfloat16)
    left_half = lax.broadcasted_iota(jnp.int32, (pairs * ROWS, 2 * hd), 1) < hd

    late_lane = lax.broadcasted_iota(jnp.int32, (2 * packed_rows(pairs, group), 2 * hd), 1)

    def msg_copy(b, t):
        return pltpu.make_async_remote_copy(
            src_ref=msg.at[mt, b], dst_ref=msg.at[mt, b],
            send_sem=send_sem, recv_sem=mrecv_sem,
            device_id={"tp": t}, device_id_type=MESH,
        )

    def part_copy(i, t):
        return pltpu.make_async_remote_copy(
            src_ref=part_v.at[mt, i], dst_ref=part_v.at[mt, i],
            send_sem=send_sem, recv_sem=precv_sem.at[i],
            device_id={"tp": t}, device_id_type=MESH,
        )

    def late_copy(i, j, to):
        return pltpu.make_async_remote_copy(
            src_ref=late_v.at[i, j], dst_ref=msg.at[tp - 1, me],
            send_sem=send_sem, recv_sem=lrecv_sem,
            device_id={"sp": to}, device_id_type=MESH,
        )

    def urgent_copy(i, j, to, there):
        return pltpu.make_async_remote_copy(
            src_ref=late_b.at[i, j], dst_ref=late_in.at[mt // 2, me - quarter],
            send_sem=send_sem, recv_sem=lrecv_sem,
            device_id={"sp": to, "tp": there}, device_id_type=MESH,
        )

    def attend(items):
        scores = []
        shifts = []
        for queries, shift, rows, b in items:
            shifts.append(shift)
            for p in range(pairs):
                q = queries[p * ROWS:(p + 1) * ROWS, :]
                kv = rows[b, :, p * 2 * hd:(p + 1) * 2 * hd]
                scores.append(lax.dot_general(q, kv, (((1,), (1,)), ((), ())), preferred_element_type=jnp.float32))
        s = jnp.concatenate(scores, axis=0) * scale + jnp.concatenate(shifts, axis=0)
        low = jnp.log1p(jnp.exp(-jnp.abs(s)))
        keep = -(jnp.maximum(s, 0.0) + low)
        sig = jnp.minimum(s, 0.0) - low
        hi = keep.astype(jnp.bfloat16)
        rest = keep - hi.astype(jnp.float32)
        mid = rest.astype(jnp.bfloat16)
        lo = (rest - mid.astype(jnp.float32)).astype(jnp.bfloat16)
        sums = (
            jnp.dot(hi, tri, preferred_element_type=jnp.float32)
            + jnp.dot(mid, tri, preferred_element_type=jnp.float32)
            + jnp.dot(lo, tri, preferred_element_type=jnp.float32)
        )
        weights = jnp.exp(sig + sums[:, :sub]).astype(jnp.bfloat16)
        n = pairs * ROWS
        out = []
        for i, (_, _, rows, b) in enumerate(items):
            reads = []
            for p in range(pairs):
                kv = rows[b, :, p * 2 * hd:(p + 1) * 2 * hd]
                at = i * n + p * ROWS
                reads.append(jnp.dot(weights[at:at + ROWS], kv, preferred_element_type=jnp.float32))
            read = jnp.concatenate(reads, axis=0)
            both = jnp.where(left_half, sums[i * n:(i + 1) * n, 128:128 + 2 * hd], read)
            packed = [both[p * ROWS:p * ROWS + group] for p in range(pairs)]
            packed.append(jnp.zeros((packed_rows(pairs, group) - pairs * group, 2 * hd), jnp.float32))
            out.append(jnp.concatenate(packed, axis=0))
        return out

    shift = shift_of(me)

    def attend_blocks(blocks):
        for b, m in zip(blocks, attend([(q_pad, shift, recv, b) for b in blocks])):
            msg[mt, b] = m
            for t in range(1, tp):
                msg_copy(b, lax.rem(mt + t, tp)).start()

    def attend_late(i, owners):
        part_v[mt, i] = jnp.concatenate(
            attend([(q_all.at[owner], shift_of(owner), send, owner) for owner in owners]), axis=0
        )

    def combine(parts):
        total = parts[0]
        acc = pltpu.roll(total, hd, 1)
        for m in parts[1:]:
            total = total + jnp.exp(acc) * m
            acc = acc + pltpu.roll(m, hd, 1)
        return pltpu.roll(acc, hd, 1), total

    def send_late(i, owners):
        wait_bytes(part_v.at[pl.ds(0, tp - 1), i], precv_sem.at[i])
        keep, total = combine([part_v[j, i] for j in range(tp - 1, -1, -1)])
        late_v[i] = jnp.where(late_lane < hd, keep, total).reshape(late_v.shape[1:])
        for j, owner in enumerate(owners):
            late_copy(i, j, owner).start()

    def send_urgent(i, owners):
        wait_bytes(part_v.at[0, first + i], precv_sem.at[first + i])
        keep, total = combine([part_v[mt, first + i], part_v[mt - 1, first + i]])
        high = keep.astype(jnp.bfloat16).astype(jnp.float32)
        keep = jnp.where(late_lane < hd // 2, high, keep - high)
        block = jnp.where(late_lane < hd, keep, total).astype(jnp.bfloat16)
        late_b[i] = block.reshape(late_b.shape[1:])
        for j, owner in enumerate(owners):
            for t in range(tp):
                urgent_copy(i, j, owner, t).start()

    def unpack(k, b):
        m = late_in[k, b - quarter].astype(jnp.float32)
        lane = late_lane[:m.shape[0]]
        other = jnp.where(lane < hd // 2, pltpu.roll(m, 2 * hd - hd // 2, 1), pltpu.roll(m, hd // 2, 1))
        msg[2 * k + 1, b] = jnp.where(lane < hd, m + other, m)

    owners = inward + urgent + relaxed
    owners = [owners[i:i + 2] for i in range(0, 3 * quarter, 2)]
    first = quarter // 2

    def attend_class(place):
        wait_bytes(q_all.at[pl.ds(0, quarter)], qrecv_sem.at[place])
        for i in range(place * first, (place + 1) * first):
            attend_late(i, owners[i])
            if place != 1:
                for t in range(1, tp):
                    part_copy(i, lax.rem(mt + t, tp)).start()
            else:

                @pl.when(lead == 0)
                def _():
                    part_copy(i, mt + 1).start()

    @pl.when(inner)
    def _():
        attend_class(1)

    attend_class(0)

    @pl.when(inner)
    def _():
        attend_class(2)

    landed = [me] + same
    wait_bytes(recv.at[pl.ds(0, quarter - 1)], recv_sem.at[0])
    for i in range(0, quarter, 2):
        attend_blocks(landed[i:i + 2])

    def attend_early():
        wait_bytes(recv.at[pl.ds(0, quarter)], recv_sem.at[1])
        for i in range(0, quarter, 2):
            attend_blocks(early[i:i + 2])

    @pl.when(home)
    def _():
        attend_early()

    @pl.when(jnp.logical_and(inner, lead == 1))
    def _():
        for i in range(first):
            send_urgent(i, owners[first + i])

    @pl.when(inner)
    def _():
        send_blocks(far_inner, first)

    for i in range(first):
        send_late(i, owners[i])

    @pl.when(inner)
    def _():
        send_blocks(far_inner + first, quarter - first)

    @pl.when(inner)
    def _():
        for i in range(2 * first, 3 * first):
            send_late(i, owners[i])

    @pl.when(jnp.logical_not(home))
    def _():
        attend_early()

    some = pl.ds(0, half)
    others = pl.ds(0, tp - 1)
    wait_bytes(recv.at[some], recv_sem.at[2])
    wait_bytes(send.at[pl.ds(0, sp - 1)], send_sem)
    wait_bytes(part_v.at[others, pl.ds(0, first)], send_sem)
    wait_bytes(late_v.at[pl.ds(0, first)], send_sem)

    @pl.when(inner)
    def _():
        wait_bytes(part_v.at[others, pl.ds(2 * first, first)], send_sem)
        wait_bytes(late_v.at[pl.ds(2 * first, first)], send_sem)

        @pl.when(lead == 0)
        def _():
            wait_bytes(part_v.at[0, pl.ds(first, first)], send_sem)

        @pl.when(lead == 1)
        def _():
            for _ in range(tp):
                wait_bytes(late_b, send_sem)

    @pl.when(lead == 1)
    def _():
        wait_bytes(q_all, send_sem)

    wait_bytes(msg.at[others, some], send_sem)
    wait_bytes(msg.at[others, some], mrecv_sem)

    @pl.when(home)
    def _():
        wait_bytes(late_in, lrecv_sem)
        for b in range(quarter, 3 * quarter):
            for k in range(chips):
                unpack(k, b)

    @pl.when(jnp.logical_not(home))
    def _():
        wait_bytes(msg.at[0, some], lrecv_sem)


def finish(sp, tp, hd, group, pairs, recv, msg, stored_hbm, first_hbm, fin, first_v, out_sem, first_sem):
    copies = [
        pltpu.make_async_copy(recv.at[b, :, pl.ds(p * 2 * hd, 2 * hd)], stored_hbm.at[p, b], out_sem)
        for b in range(sp)
        for p in range(pairs)
    ]
    for copy in copies:
        copy.start()
    left_half = lax.broadcasted_iota(jnp.int32, (packed_rows(pairs, group), 2 * hd), 1) < hd

    def add_block(i, carry):
        total, acc = carry
        b = sp - 1 - i
        for j in range(tp - 1, -1, -1):
            m = msg[j, b]
            total = total + jnp.exp(acc) * m
            acc = acc + pltpu.roll(m, hd, 1)
        return total, acc

    zero = jnp.zeros((packed_rows(pairs, group), 2 * hd), jnp.float32)
    total, _ = lax.fori_loop(0, sp, add_block, (zero, zero), unroll=True)
    total = jnp.where(left_half, 0.0, total)
    squares = jnp.sum(total * total, axis=1, keepdims=True) * (1.0 / hd)
    fin[...] = pltpu.roll(total * lax.rsqrt(squares + EPS_NORM), hd, 1)
    cols = [fin[pl.ds(g, pairs, stride=group), :][:, :hd] for g in range(group)]
    first_v[...] = jnp.concatenate(cols, axis=1).astype(first_v.dtype)
    first_copy = pltpu.make_async_copy(first_v, first_hbm, first_sem)
    first_copy.start()

    pltpu.make_async_copy(recv, recv, out_sem).wait()
    first_copy.wait()


def solution(mesh):
    sp, tp = mesh.shape["sp"], mesh.shape["tp"]

    def per_device(layer_input, key_weight, value_weight, queries, head_bias):
        seqs, sub, width = layer_input.shape
        pairs, group, hd = queries.shape
        kvh = head_bias.shape[0]
        x = layer_input.reshape(seqs * sub, width)
        block = pairs * 2 * hd
        any_spec = pl.BlockSpec(memory_space=pltpu.HBM)
        dma = pltpu.SemaphoreType.DMA
        handed = sp * sub * block * 2 + tp * sp * packed_rows(pairs, group) * 2 * hd * 4
        limit = VMEM_BYTES - handed
        late = sp // 4 * 3 // 2
        vmem_spec = pl.BlockSpec(memory_space=pltpu.VMEM)
        recv, msg = pl.pallas_call(
            functools.partial(kernel, sp, tp, seqs, sub, hd, kvh, group, pairs),
            out_shape=(
                pltpu.VMEM((sp, sub, block), jnp.bfloat16),
                pltpu.VMEM((tp, sp, packed_rows(pairs, group), 2 * hd), jnp.float32),
            ),
            in_specs=[any_spec] * 5,
            out_specs=(vmem_spec, vmem_spec),
            scratch_shapes=[
                pltpu.VMEM(x.shape, jnp.bfloat16),
                pltpu.VMEM((width, 2 * key_weight.shape[1]), jnp.bfloat16),
                pltpu.VMEM((group, pairs, hd), jnp.bfloat16),
                pltpu.VMEM(head_bias.shape, jnp.float32),
                pltpu.VMEM((sp, sub, block), jnp.bfloat16),
                pltpu.VMEM((pairs * ROWS, 2 * hd), jnp.bfloat16),
                pltpu.VMEM((sp, pairs * ROWS, 2 * hd), jnp.bfloat16),
                pltpu.VMEM((tp, late, 2 * packed_rows(pairs, group), 2 * hd), jnp.float32),
                pltpu.VMEM((late, 2, packed_rows(pairs, group), 2 * hd), jnp.float32),
                pltpu.VMEM((sp // 8, 2, packed_rows(pairs, group), 2 * hd), jnp.bfloat16),
                pltpu.VMEM((tp // 2, sp // 2, packed_rows(pairs, group), 2 * hd), jnp.bfloat16),
                dma((KC + 1,)),
                dma((KC,)),
                dma((2,)),
                dma(()),
                dma((3,)),
                dma(()),
                dma((3,)),
                dma((late,)),
                dma(()),
            ],
            compiler_params=pltpu.CompilerParams(
                collective_id=0, has_side_effects=True, vmem_limit_bytes=limit
            ),
        )(x, key_weight, value_weight, queries.transpose(1, 0, 2), head_bias)
        return pl.pallas_call(
            functools.partial(finish, sp, tp, hd, group, pairs),
            out_shape=(
                jax.ShapeDtypeStruct((pairs, sp, sub, 2 * hd), jnp.bfloat16),
                jax.ShapeDtypeStruct((pairs, group * hd), jnp.bfloat16),
            ),
            in_specs=[vmem_spec, vmem_spec],
            out_specs=(any_spec, any_spec),
            scratch_shapes=[
                pltpu.VMEM((packed_rows(pairs, group), 2 * hd), jnp.float32),
                pltpu.VMEM((pairs, group * hd), jnp.bfloat16),
                dma(()),
                dma(()),
            ],
            compiler_params=pltpu.CompilerParams(vmem_limit_bytes=VMEM_BYTES // 4),
        )(recv, msg)

    in_specs = (P(None, ("sp", "tp"), None), P(), P(), P("sp", None, None), P())
    out_specs = (P("sp", None, "tp", None), P("sp", None))
    return jax.shard_map(per_device, mesh=mesh, in_specs=in_specs, out_specs=out_specs, check_vma=False)
```

```python
import functools
import math

import jax
import jax.numpy as jnp
from jax import lax
from jax.experimental import pallas as pl
from jax.experimental.pallas import tpu as pltpu
from jax.sharding import PartitionSpec as P

EPS_NORM = 0.0001
MESH = pl.DeviceIdType.MESH
KC = 4
VMEM_BYTES = 60 * 1024 * 1024
ROWS = 8


def flip(index, k):
    bit = 1
    while bit <= k:
        if k & bit:
            index = index + (1 - 2 * ((index // bit) % 2)) * bit
        bit *= 2
    return index


def packed_rows(pairs, group):
    return pairs * group // 8 * 8 + 8


def kernel(
    sp, tp, seqs, sub, hd, kvh, group, pairs,
    x_hbm, wk_hbm, wv_hbm, q_hbm, bias_hbm,
    recv, msg,
    x_v, w_v, q_v, bias_v, send, q_pad, q_all, part_v, late_v, late_b, late_in,
    x_sem, w_sem, small_sem, send_sem, recv_sem, mrecv_sem, qrecv_sem, precv_sem, lrecv_sem,
):
    me = lax.axis_index("sp")
    mt = lax.axis_index("tp")
    per_seq = kvh // pairs
    width = x_hbm.shape[1]
    kc = width // KC
    half_rows = seqs * sub // 2

    q_copy = pltpu.make_async_copy(q_hbm, q_v, small_sem.at[0])
    bias_copy = pltpu.make_async_copy(bias_hbm, bias_v, small_sem.at[1])
    q_copy.start()
    bias_copy.start()
    kv_width = wk_hbm.shape[1]

    def x_copy(c):
        at = (pl.ds(0, half_rows), pl.ds(c * kc, kc))
        return pltpu.make_async_copy(x_hbm.at[at], x_v.at[at], x_sem.at[c])

    def w_copy(i, c):
        rows = pl.ds(c * kc, kc)
        w_hbm = (wk_hbm, wv_hbm)[i]
        return pltpu.make_async_copy(w_hbm.at[rows], w_v.at[rows, pl.ds(i * kv_width, kv_width)], w_sem.at[c])

    rest = pl.ds(half_rows, half_rows)
    x_rest = pltpu.make_async_copy(x_hbm.at[rest], x_v.at[rest], x_sem.at[KC])
    for c in range(KC):
        x_copy(c).start()
        w_copy(0, c).start()
        w_copy(1, c).start()
    x_rest.start()

    msg[...] = jnp.zeros_like(msg)

    top = me // (sp // 2)
    half = sp // 2
    quarter = sp // 4
    lead = lax.rem(mt, 2)
    outer = lax.rem(me // quarter, 3) == 0
    inner = jnp.logical_not(outer)
    home = me // quarter == 0
    chips = tp // 2
    far_outer = (1 - top) * 3 * quarter
    far_inner = quarter + (1 - top) * quarter
    near = [flip(me, k) for k in range(quarter, half)]
    inward = [far_inner + flip(lax.rem(me, 2), j) for j in range(quarter)]
    outward = [far_outer + flip(lax.rem(me, 2), j) for j in range(quarter)]
    same = [flip(me, k) for k in range(1, quarter)]
    early = [jnp.where(outer, a, b) for a, b in zip(outward, near)]
    late = [jnp.where(outer, a, b) for a, b in zip(near, outward)]
    urgent = [jnp.where(top == 0, a, b) for a, b in zip(near, outward)]
    relaxed = [jnp.where(top == 0, a, b) for a, b in zip(outward, near)]

    barrier = pltpu.get_barrier_semaphore()
    for k in range(sp - 1, 0, -1):
        pl.semaphore_signal(barrier, inc=1, device_id={"sp": flip(me, k)}, device_id_type=MESH)
    for k in range(1, tp):
        pl.semaphore_signal(barrier, inc=1, device_id={"tp": lax.rem(mt + k, tp)}, device_id_type=MESH)

    @pl.when(home)
    def _():
        for t in range(1, tp, 2):
            for to in range(quarter, 3 * quarter):

                @pl.when(t != mt)
                def _():
                    pl.semaphore_signal(barrier, inc=1, device_id={"sp": to, "tp": t}, device_id_type=MESH)

    def ask(owners):
        for owner in owners:
            pl.semaphore_signal(barrier, inc=1, device_id={"sp": owner, "tp": mt + 1}, device_id_type=MESH)

    @pl.when(lead == 0)
    def _():
        ask(inward)

        @pl.when(inner)
        def _():
            ask(near + outward)

    def wait_bytes(ref, sem):
        pltpu.make_async_copy(ref, ref, sem).wait()

    def pack(rows, base):
        for i in range(seqs // 2):
            for part in range(per_seq):
                out = []
                for p in range(pairs):
                    c0 = (part * pairs + p) * hd
                    out.append(rows[i * sub:(i + 1) * sub, c0:c0 + hd])
                    out.append(rows[i * sub:(i + 1) * sub, kv_width + c0:kv_width + c0 + hd])
                send[base + i * per_seq + part] = jnp.concatenate(out, axis=1).astype(jnp.bfloat16)

    def send_block(to):
        near_class = jnp.where(outer, 1, 2)
        place = jnp.where(to // half == top, near_class, jnp.where(to // quarter == far_outer // quarter, near_class, 2))
        place = jnp.where(to // quarter == me // quarter, 0, place)

        @pl.when(to != me)
        def _():
            pltpu.make_async_remote_copy(
                src_ref=send.at[to], dst_ref=recv.at[me],
                send_sem=send_sem, recv_sem=recv_sem.at[place],
                device_id={"sp": to}, device_id_type=MESH,
            ).start()

    def send_blocks(base, count):
        for j in range(count):
            send_block(base + j)

    def query_copy(to, core, place):
        return pltpu.make_async_remote_copy(
            src_ref=q_pad, dst_ref=q_all.at[me],
            send_sem=send_sem, recv_sem=qrecv_sem.at[place],
            device_id={"sp": to, "tp": mt - core}, device_id_type=MESH,
        )

    def enter():
        pl.semaphore_wait(barrier, sp + tp - 2 + lead * (half + jnp.where(inner, quarter * (tp - 1), 0)))

        @pl.when(lead == 1)
        def _():
            for group_of in (inward, late):
                for core in range(2):
                    for to in group_of:
                        query_copy(to, core, jnp.where(outer, 1 + top, 0)).start()

    q_copy.wait()
    for p in range(pairs):
        qp = q_v[:, p, :].astype(jnp.float32)
        qp = jnp.concatenate([qp, jnp.zeros((group, hd), jnp.float32)], axis=1)
        qp = jnp.concatenate([qp, jnp.zeros((ROWS - group, 2 * hd), jnp.float32)], axis=0)
        q_pad[p * ROWS:(p + 1) * ROWS, :] = qp.astype(jnp.bfloat16)

    rows = None
    for c in range(KC):
        x_copy(c).wait()
        wait_bytes(w_v.at[pl.ds(c * kc, kc)], w_sem.at[c])
        part = jnp.dot(
            x_v[:half_rows, c * kc:(c + 1) * kc], w_v[c * kc:(c + 1) * kc, :],
            preferred_element_type=jnp.float32,
        )
        rows = part if rows is None else rows + part
    pack(rows, 0)

    @pl.when(top == 1)
    def _():
        enter()
        send_blocks(far_outer, quarter)

    x_rest.wait()
    pack(jnp.dot(x_v[half_rows:, :], w_v[...], preferred_element_type=jnp.float32), half)

    @pl.when(top == 0)
    def _():
        enter()

    own_base = me // quarter * quarter
    near_base = top * half + quarter - lax.rem(me // quarter, 2) * quarter
    send_blocks(own_base, quarter)

    @pl.when(jnp.logical_or(outer, lead == 0))
    def _():
        send_blocks(near_base, quarter)


    @pl.when(top == 0)
    def _():
        send_blocks(far_outer, quarter)

    @pl.when(outer)
    def _():
        send_blocks(far_inner, quarter)

    recv[pl.ds(me, 1)] = send[pl.ds(me, 1)]

    bias_copy.wait()
    eye = lax.broadcasted_iota(jnp.int32, (ROWS, group), 0) == lax.broadcasted_iota(jnp.int32, (ROWS, group), 1)

    def shift_of(owner):
        h0 = lax.rem(owner * pairs, kvh)
        shifts = []
        for p in range(pairs):
            row = bias_v[pl.ds(h0 + p, 1), :]
            shifts.append(jnp.sum(jnp.where(eye, jnp.broadcast_to(row, (ROWS, group)), 0.0), axis=1, keepdims=True))
        return jnp.concatenate(shifts, axis=0)

    scale = 1.0 / math.sqrt(hd)
    later = lax.broadcasted_iota(jnp.int32, (sub, 256), 0)
    column = lax.broadcasted_iota(jnp.int32, (sub, 256), 1)
    tri = ((later > column) | (column >= 128)).astype(jnp.float32).astype(jnp.bfloat16)
    left_half = lax.broadcasted_iota(jnp.int32, (pairs * ROWS, 2 * hd), 1) < hd

    late_lane = lax.broadcasted_iota(jnp.int32, (2 * packed_rows(pairs, group), 2 * hd), 1)

    def msg_copy(b, t):
        return pltpu.make_async_remote_copy(
            src_ref=msg.at[mt, b], dst_ref=msg.at[mt, b],
            send_sem=send_sem, recv_sem=mrecv_sem,
            device_id={"tp": t}, device_id_type=MESH,
        )

    def part_copy(i, t):
        return pltpu.make_async_remote_copy(
            src_ref=part_v.at[mt, i], dst_ref=part_v.at[mt, i],
            send_sem=send_sem, recv_sem=precv_sem.at[i],
            device_id={"tp": t}, device_id_type=MESH,
        )

    def late_copy(i, j, to):
        return pltpu.make_async_remote_copy(
            src_ref=late_v.at[i, j], dst_ref=msg.at[tp - 1, me],
            send_sem=send_sem, recv_sem=lrecv_sem,
            device_id={"sp": to}, device_id_type=MESH,
        )

    def urgent_copy(i, j, to, there):
        return pltpu.make_async_remote_copy(
            src_ref=late_b.at[i, j], dst_ref=late_in.at[mt // 2, me - quarter],
            send_sem=send_sem, recv_sem=lrecv_sem,
            device_id={"sp": to, "tp": there}, device_id_type=MESH,
        )

    def attend(items):
        scores = []
        shifts = []
        for queries, shift, rows, b in items:
            shifts.append(shift)
            for p in range(pairs):
                q = queries[p * ROWS:(p + 1) * ROWS, :]
                kv = rows[b, :, p * 2 * hd:(p + 1) * 2 * hd]
                scores.append(lax.dot_general(q, kv, (((1,), (1,)), ((), ())), preferred_element_type=jnp.float32))
        s = jnp.concatenate(scores, axis=0) * scale + jnp.concatenate(shifts, axis=0)
        low = jnp.log1p(jnp.exp(-jnp.abs(s)))
        keep = -(jnp.maximum(s, 0.0) + low)
        sig = jnp.minimum(s, 0.0) - low
        hi = keep.astype(jnp.bfloat16)
        rest = keep - hi.astype(jnp.float32)
        mid = rest.astype(jnp.bfloat16)
        lo = (rest - mid.astype(jnp.float32)).astype(jnp.bfloat16)
        sums = (
            jnp.dot(hi, tri, preferred_element_type=jnp.float32)
            + jnp.dot(mid, tri, preferred_element_type=jnp.float32)
            + jnp.dot(lo, tri, preferred_element_type=jnp.float32)
        )
        weights = jnp.exp(sig + sums[:, :sub]).astype(jnp.bfloat16)
        n = pairs * ROWS
        out = []
        for i, (_, _, rows, b) in enumerate(items):
            reads = []
            for p in range(pairs):
                kv = rows[b, :, p * 2 * hd:(p + 1) * 2 * hd]
                at = i * n + p * ROWS
                reads.append(jnp.dot(weights[at:at + ROWS], kv, preferred_element_type=jnp.float32))
            read = jnp.concatenate(reads, axis=0)
            both = jnp.where(left_half, sums[i * n:(i + 1) * n, 128:128 + 2 * hd], read)
            packed = [both[p * ROWS:p * ROWS + group] for p in range(pairs)]
            packed.append(jnp.zeros((packed_rows(pairs, group) - pairs * group, 2 * hd), jnp.float32))
            out.append(jnp.concatenate(packed, axis=0))
        return out

    shift = shift_of(me)

    def attend_blocks(blocks):
        for b, m in zip(blocks, attend([(q_pad, shift, recv, b) for b in blocks])):
            msg[mt, b] = m
            for t in range(1, tp):
                msg_copy(b, lax.rem(mt + t, tp)).start()

    def narrow(block):
        lane = late_lane[:block.shape[0]]
        high = block.astype(jnp.bfloat16).astype(jnp.float32)
        keep = jnp.where(lane < hd // 2, high, block - high)
        return jnp.where(lane < hd, keep, block).astype(jnp.bfloat16)

    def widen(ref):
        m = ref[...].astype(jnp.float32)
        lane = late_lane[:m.shape[0]]
        other = jnp.where(lane < hd // 2, pltpu.roll(m, 2 * hd - hd // 2, 1), pltpu.roll(m, hd // 2, 1))
        return jnp.where(lane < hd, m + other, m)

    def attend_late(i, owners):
        part_v[mt, i] = narrow(jnp.concatenate(
            attend([(q_all.at[owner], shift_of(owner), send, owner) for owner in owners]), axis=0
        ))

    def combine(parts):
        total = parts[0]
        acc = pltpu.roll(total, hd, 1)
        for m in parts[1:]:
            total = total + jnp.exp(acc) * m
            acc = acc + pltpu.roll(m, hd, 1)
        return jnp.where(late_lane < hd, pltpu.roll(acc, hd, 1), total)

    def send_late(i, owners):
        wait_bytes(part_v.at[pl.ds(0, tp - 1), i], precv_sem.at[i])
        block = combine([widen(part_v.at[j, i]) for j in range(tp - 1, -1, -1)])
        late_v[i] = block.reshape(late_v.shape[1:])
        for j, owner in enumerate(owners):
            late_copy(i, j, owner).start()

    def send_urgent(i, owners):
        wait_bytes(part_v.at[0, first + i], precv_sem.at[first + i])
        block = combine([widen(part_v.at[mt, first + i]), widen(part_v.at[mt - 1, first + i])])
        late_b[i] = narrow(block).reshape(late_b.shape[1:])
        for j, owner in enumerate(owners):
            for t in range(tp):
                urgent_copy(i, j, owner, t).start()

    owners = inward + urgent + relaxed
    owners = [owners[i:i + 2] for i in range(0, 3 * quarter, 2)]
    first = quarter // 2

    def attend_class(place):
        wait_bytes(q_all.at[pl.ds(0, quarter)], qrecv_sem.at[place])
        for i in range(place * first, (place + 1) * first):
            attend_late(i, owners[i])
            if place != 1:
                for t in range(1, tp):
                    part_copy(i, lax.rem(mt + t, tp)).start()
            else:

                @pl.when(lead == 0)
                def _():
                    part_copy(i, mt + 1).start()

    @pl.when(inner)
    def _():
        attend_class(1)

    attend_class(0)

    @pl.when(inner)
    def _():
        attend_class(2)

    @pl.when(jnp.logical_and(inner, lead == 1))
    def _():
        for i in range(first):
            send_urgent(i, owners[first + i])
        send_blocks(near_base, quarter)

    @pl.when(inner)
    def _():
        send_blocks(far_inner, first)

    landed = [me] + same
    wait_bytes(recv.at[pl.ds(0, quarter - 1)], recv_sem.at[0])
    for i in range(0, quarter, 2):
        attend_blocks(landed[i:i + 2])

    def attend_early():
        wait_bytes(recv.at[pl.ds(0, quarter)], recv_sem.at[1])
        for i in range(0, quarter, 2):
            attend_blocks(early[i:i + 2])

    @pl.when(home)
    def _():
        attend_early()

    for i in range(first):
        send_late(i, owners[i])

    @pl.when(inner)
    def _():
        send_blocks(far_inner + first, quarter - first)

    @pl.when(inner)
    def _():
        for i in range(2 * first, 3 * first):
            send_late(i, owners[i])

    @pl.when(jnp.logical_not(home))
    def _():
        attend_early()

    some = pl.ds(0, half)
    others = pl.ds(0, tp - 1)
    wait_bytes(recv.at[some], recv_sem.at[2])
    wait_bytes(send.at[pl.ds(0, sp - 1)], send_sem)
    wait_bytes(part_v.at[others, pl.ds(0, first)], send_sem)
    wait_bytes(late_v.at[pl.ds(0, first)], send_sem)

    @pl.when(inner)
    def _():
        wait_bytes(part_v.at[others, pl.ds(2 * first, first)], send_sem)
        wait_bytes(late_v.at[pl.ds(2 * first, first)], send_sem)

        @pl.when(lead == 0)
        def _():
            wait_bytes(part_v.at[0, pl.ds(first, first)], send_sem)

        @pl.when(lead == 1)
        def _():
            for _ in range(tp):
                wait_bytes(late_b, send_sem)

    @pl.when(lead == 1)
    def _():
        wait_bytes(q_all, send_sem)

    wait_bytes(msg.at[others, some], send_sem)
    wait_bytes(msg.at[others, some], mrecv_sem)

    @pl.when(home)
    def _():
        wait_bytes(late_in, lrecv_sem)
        for b in range(quarter, 3 * quarter):
            for k in range(chips):
                msg[2 * k + 1, b] = widen(late_in.at[k, b - quarter])

    @pl.when(jnp.logical_not(home))
    def _():
        wait_bytes(msg.at[0, some], lrecv_sem)


def finish(sp, tp, hd, group, pairs, recv, msg, stored_hbm, first_hbm, fin, first_v, out_sem, first_sem):
    copies = [
        pltpu.make_async_copy(recv.at[b, :, pl.ds(p * 2 * hd, 2 * hd)], stored_hbm.at[p, b], out_sem)
        for b in range(sp)
        for p in range(pairs)
    ]
    for copy in copies:
        copy.start()
    left_half = lax.broadcasted_iota(jnp.int32, (packed_rows(pairs, group), 2 * hd), 1) < hd

    def add_block(i, carry):
        total, acc = carry
        b = sp - 1 - i
        for j in range(tp - 1, -1, -1):
            m = msg[j, b]
            total = total + jnp.exp(acc) * m
            acc = acc + pltpu.roll(m, hd, 1)
        return total, acc

    zero = jnp.zeros((packed_rows(pairs, group), 2 * hd), jnp.float32)
    total, _ = lax.fori_loop(0, sp, add_block, (zero, zero), unroll=True)
    total = jnp.where(left_half, 0.0, total)
    squares = jnp.sum(total * total, axis=1, keepdims=True) * (1.0 / hd)
    fin[...] = pltpu.roll(total * lax.rsqrt(squares + EPS_NORM), hd, 1)
    cols = [fin[pl.ds(g, pairs, stride=group), :][:, :hd] for g in range(group)]
    first_v[...] = jnp.concatenate(cols, axis=1).astype(first_v.dtype)
    first_copy = pltpu.make_async_copy(first_v, first_hbm, first_sem)
    first_copy.start()

    pltpu.make_async_copy(recv, recv, out_sem).wait()
    first_copy.wait()


def solution(mesh):
    sp, tp = mesh.shape["sp"], mesh.shape["tp"]

    def per_device(layer_input, key_weight, value_weight, queries, head_bias):
        seqs, sub, width = layer_input.shape
        pairs, group, hd = queries.shape
        kvh = head_bias.shape[0]
        x = layer_input.reshape(seqs * sub, width)
        block = pairs * 2 * hd
        any_spec = pl.BlockSpec(memory_space=pltpu.HBM)
        dma = pltpu.SemaphoreType.DMA
        handed = sp * sub * block * 2 + tp * sp * packed_rows(pairs, group) * 2 * hd * 4
        limit = VMEM_BYTES - handed
        late = sp // 4 * 3 // 2
        vmem_spec = pl.BlockSpec(memory_space=pltpu.VMEM)
        recv, msg = pl.pallas_call(
            functools.partial(kernel, sp, tp, seqs, sub, hd, kvh, group, pairs),
            out_shape=(
                pltpu.VMEM((sp, sub, block), jnp.bfloat16),
                pltpu.VMEM((tp, sp, packed_rows(pairs, group), 2 * hd), jnp.float32),
            ),
            in_specs=[any_spec] * 5,
            out_specs=(vmem_spec, vmem_spec),
            scratch_shapes=[
                pltpu.VMEM(x.shape, jnp.bfloat16),
                pltpu.VMEM((width, 2 * key_weight.shape[1]), jnp.bfloat16),
                pltpu.VMEM((group, pairs, hd), jnp.bfloat16),
                pltpu.VMEM(head_bias.shape, jnp.float32),
                pltpu.VMEM((sp, sub, block), jnp.bfloat16),
                pltpu.VMEM((pairs * ROWS, 2 * hd), jnp.bfloat16),
                pltpu.VMEM((sp, pairs * ROWS, 2 * hd), jnp.bfloat16),
                pltpu.VMEM((tp, late, 2 * packed_rows(pairs, group), 2 * hd), jnp.bfloat16),
                pltpu.VMEM((late, 2, packed_rows(pairs, group), 2 * hd), jnp.float32),
                pltpu.VMEM((sp // 8, 2, packed_rows(pairs, group), 2 * hd), jnp.bfloat16),
                pltpu.VMEM((tp // 2, sp // 2, packed_rows(pairs, group), 2 * hd), jnp.bfloat16),
                dma((KC + 1,)),
                dma((KC,)),
                dma((2,)),
                dma(()),
                dma((3,)),
                dma(()),
                dma((3,)),
                dma((late,)),
                dma(()),
            ],
            compiler_params=pltpu.CompilerParams(
                collective_id=0, has_side_effects=True, vmem_limit_bytes=limit
            ),
        )(x, key_weight, value_weight, queries.transpose(1, 0, 2), head_bias)
        return pl.pallas_call(
            functools.partial(finish, sp, tp, hd, group, pairs),
            out_shape=(
                jax.ShapeDtypeStruct((pairs, sp, sub, 2 * hd), jnp.bfloat16),
                jax.ShapeDtypeStruct((pairs, group * hd), jnp.bfloat16),
            ),
            in_specs=[vmem_spec, vmem_spec],
            out_specs=(any_spec, any_spec),
            scratch_shapes=[
                pltpu.VMEM((packed_rows(pairs, group), 2 * hd), jnp.float32),
                pltpu.VMEM((pairs, group * hd), jnp.bfloat16),
                dma(()),
                dma(()),
            ],
            compiler_params=pltpu.CompilerParams(vmem_limit_bytes=VMEM_BYTES // 4),
        )(recv, msg)

    in_specs = (P(None, ("sp", "tp"), None), P(), P(), P("sp", None, None), P())
    out_specs = (P("sp", None, "tp", None), P("sp", None))
    return jax.shard_map(per_device, mesh=mesh, in_specs=in_specs, out_specs=out_specs, check_vma=False)
```

```python
import functools
import math

import jax
import jax.numpy as jnp
from jax import lax
from jax.experimental import pallas as pl
from jax.experimental.pallas import tpu as pltpu
from jax.sharding import PartitionSpec as P

EPS_NORM = 0.0001
MESH = pl.DeviceIdType.MESH
KC = 4
VMEM_BYTES = 60 * 1024 * 1024
ROWS = 8


def flip(index, k):
    bit = 1
    while bit <= k:
        if k & bit:
            index = index + (1 - 2 * ((index // bit) % 2)) * bit
        bit *= 2
    return index


def packed_rows(pairs, group):
    return pairs * group // 8 * 8 + 8


def kernel(
    sp, tp, seqs, sub, hd, kvh, group, pairs,
    x_hbm, wk_hbm, wv_hbm, q_hbm, bias_hbm,
    recv, msg,
    x_v, w_v, q_v, bias_v, send, q_pad, q_all, part_v, late_b, late_in,
    x_sem, w_sem, small_sem, send_sem, recv_sem, mrecv_sem, qrecv_sem, precv_sem, lrecv_sem,
):
    me = lax.axis_index("sp")
    mt = lax.axis_index("tp")
    per_seq = kvh // pairs
    width = x_hbm.shape[1]
    kc = width // KC
    half_rows = seqs * sub // 2

    q_copy = pltpu.make_async_copy(q_hbm, q_v, small_sem.at[0])
    bias_copy = pltpu.make_async_copy(bias_hbm, bias_v, small_sem.at[1])
    q_copy.start()
    bias_copy.start()
    kv_width = wk_hbm.shape[1]

    def x_copy(c):
        at = (pl.ds(0, half_rows), pl.ds(c * kc, kc))
        return pltpu.make_async_copy(x_hbm.at[at], x_v.at[at], x_sem.at[c])

    def w_copy(i, c):
        rows = pl.ds(c * kc, kc)
        w_hbm = (wk_hbm, wv_hbm)[i]
        return pltpu.make_async_copy(w_hbm.at[rows], w_v.at[rows, pl.ds(i * kv_width, kv_width)], w_sem.at[c])

    rest = pl.ds(half_rows, half_rows)
    x_rest = pltpu.make_async_copy(x_hbm.at[rest], x_v.at[rest], x_sem.at[KC])
    for c in range(KC):
        x_copy(c).start()
        w_copy(0, c).start()
        w_copy(1, c).start()
    x_rest.start()

    msg[...] = jnp.zeros_like(msg)

    top = me // (sp // 2)
    half = sp // 2
    quarter = sp // 4
    lead = lax.rem(mt, 2)
    outer = lax.rem(me // quarter, 3) == 0
    inner = jnp.logical_not(outer)
    home = me // quarter == 0
    chips = tp // 2
    far_outer = (1 - top) * 3 * quarter
    far_inner = quarter + (1 - top) * quarter
    near = [flip(me, k) for k in range(quarter, half)]
    inward = [far_inner + flip(lax.rem(me, 2), j) for j in range(quarter)]
    outward = [far_outer + flip(lax.rem(me, 2), j) for j in range(quarter)]
    same = [flip(me, k) for k in range(1, quarter)]
    early = [jnp.where(outer, a, b) for a, b in zip(outward, near)]
    late = [jnp.where(outer, a, b) for a, b in zip(near, outward)]
    urgent = [jnp.where(top == 0, a, b) for a, b in zip(near, outward)]
    relaxed = [jnp.where(top == 0, a, b) for a, b in zip(outward, near)]

    barrier = pltpu.get_barrier_semaphore()
    for k in range(sp - 1, 0, -1):
        pl.semaphore_signal(barrier, inc=1, device_id={"sp": flip(me, k)}, device_id_type=MESH)
    for k in range(1, tp):
        pl.semaphore_signal(barrier, inc=1, device_id={"tp": lax.rem(mt + k, tp)}, device_id_type=MESH)

    @pl.when(home)
    def _():
        for t in range(1, tp, 2):
            for to in range(quarter, 3 * quarter):

                @pl.when(t != mt)
                def _():
                    pl.semaphore_signal(barrier, inc=1, device_id={"sp": to, "tp": t}, device_id_type=MESH)

    def ask(owners):
        for owner in owners:
            pl.semaphore_signal(barrier, inc=1, device_id={"sp": owner, "tp": mt + 1}, device_id_type=MESH)

    @pl.when(lead == 0)
    def _():
        ask(inward)

        @pl.when(inner)
        def _():
            ask(near + outward)

    def wait_bytes(ref, sem):
        pltpu.make_async_copy(ref, ref, sem).wait()

    def pack(rows, base):
        for i in range(seqs // 2):
            for part in range(per_seq):
                out = []
                for p in range(pairs):
                    c0 = (part * pairs + p) * hd
                    out.append(rows[i * sub:(i + 1) * sub, c0:c0 + hd])
                    out.append(rows[i * sub:(i + 1) * sub, kv_width + c0:kv_width + c0 + hd])
                send[base + i * per_seq + part] = jnp.concatenate(out, axis=1).astype(jnp.bfloat16)

    def send_block(to):
        near_class = jnp.where(outer, 1, 2)
        place = jnp.where(to // half == top, near_class, jnp.where(to // quarter == far_outer // quarter, near_class, 2))
        place = jnp.where(to // quarter == me // quarter, 0, place)

        @pl.when(to != me)
        def _():
            pltpu.make_async_remote_copy(
                src_ref=send.at[to], dst_ref=recv.at[me],
                send_sem=send_sem, recv_sem=recv_sem.at[place],
                device_id={"sp": to}, device_id_type=MESH,
            ).start()

    def send_blocks(base, count):
        for j in range(count):
            send_block(base + j)

    def query_copy(to, core, place):
        return pltpu.make_async_remote_copy(
            src_ref=q_pad, dst_ref=q_all.at[me],
            send_sem=send_sem, recv_sem=qrecv_sem.at[place],
            device_id={"sp": to, "tp": mt - core}, device_id_type=MESH,
        )

    def enter():
        pl.semaphore_wait(barrier, sp + tp - 2 + lead * (half + jnp.where(inner, quarter * (tp - 1), 0)))

        @pl.when(lead == 1)
        def _():
            for group_of in (inward, late):
                for core in range(2):
                    for to in group_of:
                        query_copy(to, core, jnp.where(outer, 1 + top, 0)).start()

    q_copy.wait()
    for p in range(pairs):
        qp = q_v[:, p, :].astype(jnp.float32)
        qp = jnp.concatenate([qp, jnp.zeros((group, hd), jnp.float32)], axis=1)
        qp = jnp.concatenate([qp, jnp.zeros((ROWS - group, 2 * hd), jnp.float32)], axis=0)
        q_pad[p * ROWS:(p + 1) * ROWS, :] = qp.astype(jnp.bfloat16)

    rows = None
    for c in range(KC):
        x_copy(c).wait()
        wait_bytes(w_v.at[pl.ds(c * kc, kc)], w_sem.at[c])
        part = jnp.dot(
            x_v[:half_rows, c * kc:(c + 1) * kc], w_v[c * kc:(c + 1) * kc, :],
            preferred_element_type=jnp.float32,
        )
        rows = part if rows is None else rows + part
    pack(rows, 0)

    @pl.when(top == 1)
    def _():
        enter()
        send_blocks(far_outer, quarter)

    x_rest.wait()
    pack(jnp.dot(x_v[half_rows:, :], w_v[...], preferred_element_type=jnp.float32), half)

    @pl.when(top == 0)
    def _():
        enter()

    own_base = me // quarter * quarter
    near_base = top * half + quarter - lax.rem(me // quarter, 2) * quarter
    send_blocks(own_base, quarter)

    @pl.when(jnp.logical_or(outer, lead == 0))
    def _():
        send_blocks(near_base, quarter)


    @pl.when(top == 0)
    def _():
        send_blocks(far_outer, quarter)

    @pl.when(outer)
    def _():
        send_blocks(far_inner, quarter)

    recv[pl.ds(me, 1)] = send[pl.ds(me, 1)]

    bias_copy.wait()
    eye = lax.broadcasted_iota(jnp.int32, (ROWS, group), 0) == lax.broadcasted_iota(jnp.int32, (ROWS, group), 1)

    def shift_of(owner):
        h0 = lax.rem(owner * pairs, kvh)
        shifts = []
        for p in range(pairs):
            row = bias_v[pl.ds(h0 + p, 1), :]
            shifts.append(jnp.sum(jnp.where(eye, jnp.broadcast_to(row, (ROWS, group)), 0.0), axis=1, keepdims=True))
        return jnp.concatenate(shifts, axis=0)

    scale = 1.0 / math.sqrt(hd)
    later = lax.broadcasted_iota(jnp.int32, (sub, 256), 0)
    column = lax.broadcasted_iota(jnp.int32, (sub, 256), 1)
    tri = ((later > column) | (column >= 128)).astype(jnp.float32).astype(jnp.bfloat16)
    left_half = lax.broadcasted_iota(jnp.int32, (pairs * ROWS, 2 * hd), 1) < hd

    late_lane = lax.broadcasted_iota(jnp.int32, (2 * packed_rows(pairs, group), 2 * hd), 1)

    def msg_copy(b, t):
        return pltpu.make_async_remote_copy(
            src_ref=msg.at[mt, b], dst_ref=msg.at[mt, b],
            send_sem=send_sem, recv_sem=mrecv_sem,
            device_id={"tp": t}, device_id_type=MESH,
        )

    def part_copy(i, t):
        return pltpu.make_async_remote_copy(
            src_ref=part_v.at[mt, i], dst_ref=part_v.at[mt, i],
            send_sem=send_sem, recv_sem=precv_sem.at[i],
            device_id={"tp": t}, device_id_type=MESH,
        )

    def late_copy(i, j, to, there, slot):
        return pltpu.make_async_remote_copy(
            src_ref=late_b.at[i, j], dst_ref=late_in.at[slot],
            send_sem=send_sem, recv_sem=lrecv_sem,
            device_id={"sp": to, "tp": there}, device_id_type=MESH,
        )

    def attend(items):
        scores = []
        shifts = []
        for queries, shift, rows, b in items:
            shifts.append(shift)
            for p in range(pairs):
                q = queries[p * ROWS:(p + 1) * ROWS, :]
                kv = rows[b, :, p * 2 * hd:(p + 1) * 2 * hd]
                scores.append(lax.dot_general(q, kv, (((1,), (1,)), ((), ())), preferred_element_type=jnp.float32))
        s = jnp.concatenate(scores, axis=0) * scale + jnp.concatenate(shifts, axis=0)
        low = jnp.log1p(jnp.exp(-jnp.abs(s)))
        keep = -(jnp.maximum(s, 0.0) + low)
        sig = jnp.minimum(s, 0.0) - low
        hi = keep.astype(jnp.bfloat16)
        rest = keep - hi.astype(jnp.float32)
        mid = rest.astype(jnp.bfloat16)
        lo = (rest - mid.astype(jnp.float32)).astype(jnp.bfloat16)
        sums = (
            jnp.dot(hi, tri, preferred_element_type=jnp.float32)
            + jnp.dot(mid, tri, preferred_element_type=jnp.float32)
            + jnp.dot(lo, tri, preferred_element_type=jnp.float32)
        )
        weights = jnp.exp(sig + sums[:, :sub]).astype(jnp.bfloat16)
        n = pairs * ROWS
        out = []
        for i, (_, _, rows, b) in enumerate(items):
            reads = []
            for p in range(pairs):
                kv = rows[b, :, p * 2 * hd:(p + 1) * 2 * hd]
                at = i * n + p * ROWS
                reads.append(jnp.dot(weights[at:at + ROWS], kv, preferred_element_type=jnp.float32))
            read = jnp.concatenate(reads, axis=0)
            both = jnp.where(left_half, sums[i * n:(i + 1) * n, 128:128 + 2 * hd], read)
            packed = [both[p * ROWS:p * ROWS + group] for p in range(pairs)]
            packed.append(jnp.zeros((packed_rows(pairs, group) - pairs * group, 2 * hd), jnp.float32))
            out.append(jnp.concatenate(packed, axis=0))
        return out

    shift = shift_of(me)

    def attend_blocks(blocks):
        for b, m in zip(blocks, attend([(q_pad, shift, recv, b) for b in blocks])):
            msg[mt, b] = m
            for t in range(1, tp):
                msg_copy(b, lax.rem(mt + t, tp)).start()

    def narrow(block):
        lane = late_lane[:block.shape[0]]
        high = block.astype(jnp.bfloat16).astype(jnp.float32)
        keep = jnp.where(lane < hd // 2, high, block - high)
        return jnp.where(lane < hd, keep, block).astype(jnp.bfloat16)

    def widen(ref):
        m = ref[...].astype(jnp.float32)
        lane = late_lane[:m.shape[0]]
        other = jnp.where(lane < hd // 2, pltpu.roll(m, 2 * hd - hd // 2, 1), pltpu.roll(m, hd // 2, 1))
        return jnp.where(lane < hd, m + other, m)

    def attend_late(i, owners):
        part_v[mt, i] = narrow(jnp.concatenate(
            attend([(q_all.at[owner], shift_of(owner), send, owner) for owner in owners]), axis=0
        ))

    def combine(parts):
        total = parts[0]
        acc = pltpu.roll(total, hd, 1)
        for m in parts[1:]:
            total = total + jnp.exp(acc) * m
            acc = acc + pltpu.roll(m, hd, 1)
        return jnp.where(late_lane < hd, pltpu.roll(acc, hd, 1), total)

    def send_late(i, owners, slot):
        wait_bytes(part_v.at[pl.ds(0, tp - 1), i], precv_sem.at[i])
        block = combine([widen(part_v.at[j, i]) for j in range(tp - 1, -1, -1)])
        late_b[i] = narrow(block).reshape(late_b.shape[1:])
        for j, owner in enumerate(owners):
            late_copy(i, j, owner, mt, (0, slot)).start()

    def send_urgent(i, owners):
        wait_bytes(part_v.at[0, i], precv_sem.at[i])
        block = combine([widen(part_v.at[mt, i]), widen(part_v.at[mt - 1, i])])
        late_b[i] = narrow(block).reshape(late_b.shape[1:])
        for j, owner in enumerate(owners):
            for t in range(tp):
                late_copy(i, j, owner, t, (mt // 2, me - quarter)).start()

    owners = inward + urgent + relaxed
    owners = [owners[i:i + 2] for i in range(0, 3 * quarter, 2)]
    first = quarter // 2

    def attend_class(place):
        wait_bytes(q_all.at[pl.ds(0, quarter)], qrecv_sem.at[place])
        for i in range(place * first, (place + 1) * first):
            attend_late(i, owners[i])
            if place != 1:
                for t in range(1, tp):
                    part_copy(i, lax.rem(mt + t, tp)).start()
            else:

                @pl.when(lead == 0)
                def _():
                    part_copy(i, mt + 1).start()

    @pl.when(inner)
    def _():
        attend_class(1)

    attend_class(0)

    @pl.when(inner)
    def _():
        attend_class(2)

    @pl.when(jnp.logical_and(inner, lead == 1))
    def _():
        for i in range(first, 2 * first):
            send_urgent(i, owners[i])
        send_blocks(near_base, quarter)

    @pl.when(inner)
    def _():
        send_blocks(far_inner, first)

    landed = [me] + same
    wait_bytes(recv.at[pl.ds(0, quarter - 1)], recv_sem.at[0])
    for i in range(0, quarter, 2):
        attend_blocks(landed[i:i + 2])

    def attend_early():
        wait_bytes(recv.at[pl.ds(0, quarter)], recv_sem.at[1])
        for i in range(0, quarter, 2):
            attend_blocks(early[i:i + 2])

    @pl.when(home)
    def _():
        attend_early()

    for i in range(first):
        send_late(i, owners[i], lax.rem(me, half))

    @pl.when(inner)
    def _():
        for i in range(2 * first, 3 * first):
            send_late(i, owners[i], me - quarter)
        send_blocks(far_inner + first, quarter - first)

    @pl.when(jnp.logical_not(home))
    def _():
        attend_early()

    some = pl.ds(0, half)
    others = pl.ds(0, tp - 1)
    wait_bytes(recv.at[some], recv_sem.at[2])
    wait_bytes(send.at[pl.ds(0, sp - 1)], send_sem)
    wait_bytes(part_v.at[others, pl.ds(0, first)], send_sem)
    wait_bytes(late_b.at[pl.ds(0, first)], send_sem)

    @pl.when(inner)
    def _():
        wait_bytes(part_v.at[others, pl.ds(2 * first, first)], send_sem)
        wait_bytes(late_b.at[pl.ds(2 * first, first)], send_sem)

        @pl.when(lead == 0)
        def _():
            wait_bytes(part_v.at[0, pl.ds(first, first)], send_sem)

        @pl.when(lead == 1)
        def _():
            for _ in range(tp):
                wait_bytes(late_b.at[pl.ds(first, first)], send_sem)

    @pl.when(lead == 1)
    def _():
        wait_bytes(q_all, send_sem)

    wait_bytes(msg.at[others, some], send_sem)
    wait_bytes(msg.at[others, some], mrecv_sem)

    @pl.when(home)
    def _():
        wait_bytes(late_in, lrecv_sem)
        for i in range(half):
            for k in range(chips):
                msg[2 * k + 1, quarter + i] = widen(late_in.at[k, i])

    @pl.when(jnp.logical_not(home))
    def _():
        wait_bytes(late_in.at[0], lrecv_sem)
        base = jnp.where(outer, quarter, (1 - top) * half)
        for i in range(half):
            msg[tp - 1, base + i] = widen(late_in.at[0, i])


def finish(sp, tp, hd, group, pairs, recv, msg, stored_hbm, first_hbm, fin, first_v, out_sem, first_sem):
    copies = [
        pltpu.make_async_copy(recv.at[b, :, pl.ds(p * 2 * hd, 2 * hd)], stored_hbm.at[p, b], out_sem)
        for b in range(sp)
        for p in range(pairs)
    ]
    for copy in copies:
        copy.start()
    left_half = lax.broadcasted_iota(jnp.int32, (packed_rows(pairs, group), 2 * hd), 1) < hd

    def add_block(i, carry):
        total, acc = carry
        b = sp - 1 - i
        for j in range(tp - 1, -1, -1):
            m = msg[j, b]
            total = total + jnp.exp(acc) * m
            acc = acc + pltpu.roll(m, hd, 1)
        return total, acc

    zero = jnp.zeros((packed_rows(pairs, group), 2 * hd), jnp.float32)
    total, _ = lax.fori_loop(0, sp, add_block, (zero, zero), unroll=True)
    total = jnp.where(left_half, 0.0, total)
    squares = jnp.sum(total * total, axis=1, keepdims=True) * (1.0 / hd)
    fin[...] = pltpu.roll(total * lax.rsqrt(squares + EPS_NORM), hd, 1)
    cols = [fin[pl.ds(g, pairs, stride=group), :][:, :hd] for g in range(group)]
    first_v[...] = jnp.concatenate(cols, axis=1).astype(first_v.dtype)
    first_copy = pltpu.make_async_copy(first_v, first_hbm, first_sem)
    first_copy.start()

    pltpu.make_async_copy(recv, recv, out_sem).wait()
    first_copy.wait()


def solution(mesh):
    sp, tp = mesh.shape["sp"], mesh.shape["tp"]

    def per_device(layer_input, key_weight, value_weight, queries, head_bias):
        seqs, sub, width = layer_input.shape
        pairs, group, hd = queries.shape
        kvh = head_bias.shape[0]
        x = layer_input.reshape(seqs * sub, width)
        block = pairs * 2 * hd
        any_spec = pl.BlockSpec(memory_space=pltpu.HBM)
        dma = pltpu.SemaphoreType.DMA
        handed = sp * sub * block * 2 + tp * sp * packed_rows(pairs, group) * 2 * hd * 4
        limit = VMEM_BYTES - handed
        late = sp // 4 * 3 // 2
        vmem_spec = pl.BlockSpec(memory_space=pltpu.VMEM)
        recv, msg = pl.pallas_call(
            functools.partial(kernel, sp, tp, seqs, sub, hd, kvh, group, pairs),
            out_shape=(
                pltpu.VMEM((sp, sub, block), jnp.bfloat16),
                pltpu.VMEM((tp, sp, packed_rows(pairs, group), 2 * hd), jnp.float32),
            ),
            in_specs=[any_spec] * 5,
            out_specs=(vmem_spec, vmem_spec),
            scratch_shapes=[
                pltpu.VMEM(x.shape, jnp.bfloat16),
                pltpu.VMEM((width, 2 * key_weight.shape[1]), jnp.bfloat16),
                pltpu.VMEM((group, pairs, hd), jnp.bfloat16),
                pltpu.VMEM(head_bias.shape, jnp.float32),
                pltpu.VMEM((sp, sub, block), jnp.bfloat16),
                pltpu.VMEM((pairs * ROWS, 2 * hd), jnp.bfloat16),
                pltpu.VMEM((sp, pairs * ROWS, 2 * hd), jnp.bfloat16),
                pltpu.VMEM((tp, late, 2 * packed_rows(pairs, group), 2 * hd), jnp.bfloat16),
                pltpu.VMEM((late, 2, packed_rows(pairs, group), 2 * hd), jnp.bfloat16),
                pltpu.VMEM((tp // 2, sp // 2, packed_rows(pairs, group), 2 * hd), jnp.bfloat16),
                dma((KC + 1,)),
                dma((KC,)),
                dma((2,)),
                dma(()),
                dma((3,)),
                dma(()),
                dma((3,)),
                dma((late,)),
                dma(()),
            ],
            compiler_params=pltpu.CompilerParams(
                collective_id=0, has_side_effects=True, vmem_limit_bytes=limit
            ),
        )(x, key_weight, value_weight, queries.transpose(1, 0, 2), head_bias)
        return pl.pallas_call(
            functools.partial(finish, sp, tp, hd, group, pairs),
            out_shape=(
                jax.ShapeDtypeStruct((pairs, sp, sub, 2 * hd), jnp.bfloat16),
                jax.ShapeDtypeStruct((pairs, group * hd), jnp.bfloat16),
            ),
            in_specs=[vmem_spec, vmem_spec],
            out_specs=(any_spec, any_spec),
            scratch_shapes=[
                pltpu.VMEM((packed_rows(pairs, group), 2 * hd), jnp.float32),
                pltpu.VMEM((pairs, group * hd), jnp.bfloat16),
                dma(()),
                dma(()),
            ],
            compiler_params=pltpu.CompilerParams(vmem_limit_bytes=VMEM_BYTES // 4),
        )(recv, msg)

    in_specs = (P(None, ("sp", "tp"), None), P(), P(), P("sp", None, None), P())
    out_specs = (P("sp", None, "tp", None), P("sp", None))
    return jax.shard_map(per_device, mesh=mesh, in_specs=in_specs, out_specs=out_specs, check_vma=False)
```

```python
import functools
import math

import jax
import jax.numpy as jnp
from jax import lax
from jax.experimental import pallas as pl
from jax.experimental.pallas import tpu as pltpu
from jax.sharding import PartitionSpec as P

EPS_NORM = 0.0001
MESH = pl.DeviceIdType.MESH
KC = 4
VMEM_BYTES = 60 * 1024 * 1024
ROWS = 8


def flip(index, k):
    bit = 1
    while bit <= k:
        if k & bit:
            index = index + (1 - 2 * ((index // bit) % 2)) * bit
        bit *= 2
    return index


def packed_rows(pairs, group):
    return pairs * group // 8 * 8 + 8


def kernel(
    sp, tp, seqs, sub, hd, kvh, group, pairs,
    x_hbm, wk_hbm, wv_hbm, q_hbm, bias_hbm,
    recv, msg,
    x_v, w_v, q_v, bias_v, send, q_pad, q_all, part_v, late_b, late_in,
    x_sem, w_sem, small_sem, send_sem, recv_sem, mrecv_sem, qrecv_sem, precv_sem, lrecv_sem,
):
    me = lax.axis_index("sp")
    mt = lax.axis_index("tp")
    per_seq = kvh // pairs
    width = x_hbm.shape[1]
    kc = width // KC
    lead_seqs = sp // 4 // per_seq
    lead_rows = lead_seqs * sub

    q_copy = pltpu.make_async_copy(q_hbm, q_v, small_sem.at[0])
    bias_copy = pltpu.make_async_copy(bias_hbm, bias_v, small_sem.at[1])
    q_copy.start()
    bias_copy.start()
    kv_width = wk_hbm.shape[1]

    def x_copy(c):
        at = (pl.ds(0, lead_rows), pl.ds(c * kc, kc))
        return pltpu.make_async_copy(x_hbm.at[at], x_v.at[at], x_sem.at[c])

    def w_copy(i, c):
        rows = pl.ds(c * kc, kc)
        w_hbm = (wk_hbm, wv_hbm)[i]
        return pltpu.make_async_copy(w_hbm.at[rows], w_v.at[rows, pl.ds(i * kv_width, kv_width)], w_sem.at[c])

    rest = pl.ds(lead_rows, seqs * sub - lead_rows)
    x_rest = pltpu.make_async_copy(x_hbm.at[rest], x_v.at[rest], x_sem.at[KC])
    for c in range(KC):
        x_copy(c).start()
        w_copy(0, c).start()
        w_copy(1, c).start()
    x_rest.start()

    msg[...] = jnp.zeros_like(msg)

    top = me // (sp // 2)
    half = sp // 2
    quarter = sp // 4
    lead = lax.rem(mt, 2)
    outer = lax.rem(me // quarter, 3) == 0
    inner = jnp.logical_not(outer)
    home = me // quarter == 0
    chips = tp // 2
    far_outer = (1 - top) * 3 * quarter
    far_inner = quarter + (1 - top) * quarter
    near = [flip(me, k) for k in range(quarter, half)]
    inward = [far_inner + flip(lax.rem(me, 2), j) for j in range(quarter)]
    outward = [far_outer + flip(lax.rem(me, 2), j) for j in range(quarter)]
    same = [flip(me, k) for k in range(1, quarter)]
    early = [jnp.where(outer, a, b) for a, b in zip(outward, near)]
    late = [jnp.where(outer, a, b) for a, b in zip(near, outward)]
    urgent = [jnp.where(top == 0, a, b) for a, b in zip(near, outward)]
    relaxed = [jnp.where(top == 0, a, b) for a, b in zip(outward, near)]

    barrier = pltpu.get_barrier_semaphore()
    for k in range(sp - 1, 0, -1):
        pl.semaphore_signal(barrier, inc=1, device_id={"sp": flip(me, k)}, device_id_type=MESH)
    for k in range(1, tp):
        pl.semaphore_signal(barrier, inc=1, device_id={"tp": lax.rem(mt + k, tp)}, device_id_type=MESH)

    @pl.when(home)
    def _():
        for t in range(1, tp, 2):
            for to in range(quarter, 3 * quarter):

                @pl.when(t != mt)
                def _():
                    pl.semaphore_signal(barrier, inc=1, device_id={"sp": to, "tp": t}, device_id_type=MESH)

    def ask(owners):
        for owner in owners:
            pl.semaphore_signal(barrier, inc=1, device_id={"sp": owner, "tp": mt + 1}, device_id_type=MESH)

    @pl.when(lead == 0)
    def _():
        ask(inward)

        @pl.when(inner)
        def _():
            ask(near + outward)

    def wait_bytes(ref, sem):
        pltpu.make_async_copy(ref, ref, sem).wait()

    def pack(rows, base):
        for i in range(rows.shape[0] // sub):
            for part in range(per_seq):
                out = []
                for p in range(pairs):
                    c0 = (part * pairs + p) * hd
                    out.append(rows[i * sub:(i + 1) * sub, c0:c0 + hd])
                    out.append(rows[i * sub:(i + 1) * sub, kv_width + c0:kv_width + c0 + hd])
                send[base + i * per_seq + part] = jnp.concatenate(out, axis=1).astype(jnp.bfloat16)

    def send_block(to):
        near_class = jnp.where(outer, 1, 2)
        place = jnp.where(to // half == top, near_class, jnp.where(to // quarter == far_outer // quarter, near_class, 2))
        place = jnp.where(to // quarter == me // quarter, 0, place)

        @pl.when(to != me)
        def _():
            pltpu.make_async_remote_copy(
                src_ref=send.at[to], dst_ref=recv.at[me],
                send_sem=send_sem, recv_sem=recv_sem.at[place],
                device_id={"sp": to}, device_id_type=MESH,
            ).start()

    def send_blocks(base, count):
        for j in range(count):
            send_block(base + j)

    def query_copy(to, core, place):
        return pltpu.make_async_remote_copy(
            src_ref=q_pad, dst_ref=q_all.at[me],
            send_sem=send_sem, recv_sem=qrecv_sem.at[place],
            device_id={"sp": to, "tp": mt - core}, device_id_type=MESH,
        )

    def enter():
        pl.semaphore_wait(barrier, sp + tp - 2 + lead * (half + jnp.where(inner, quarter * (tp - 1), 0)))

        @pl.when(lead == 1)
        def _():
            for group_of in (inward, late):
                for core in range(2):
                    for to in group_of:
                        query_copy(to, core, jnp.where(outer, 1 + top, 0)).start()

    q_copy.wait()
    for p in range(pairs):
        qp = q_v[:, p, :].astype(jnp.float32)
        qp = jnp.concatenate([qp, jnp.zeros((group, hd), jnp.float32)], axis=1)
        qp = jnp.concatenate([qp, jnp.zeros((ROWS - group, 2 * hd), jnp.float32)], axis=0)
        q_pad[p * ROWS:(p + 1) * ROWS, :] = qp.astype(jnp.bfloat16)

    rows = None
    for c in range(KC):
        x_copy(c).wait()
        wait_bytes(w_v.at[pl.ds(c * kc, kc)], w_sem.at[c])
        part = jnp.dot(
            x_v[:lead_rows, c * kc:(c + 1) * kc], w_v[c * kc:(c + 1) * kc, :],
            preferred_element_type=jnp.float32,
        )
        rows = part if rows is None else rows + part
    pack(rows, 0)

    @pl.when(top == 1)
    def _():
        enter()
        send_blocks(far_outer, quarter)

    x_rest.wait()
    pack(jnp.dot(x_v[lead_rows:, :], w_v[...], preferred_element_type=jnp.float32), quarter)

    @pl.when(top == 0)
    def _():
        enter()

    own_base = me // quarter * quarter
    near_base = top * half + quarter - lax.rem(me // quarter, 2) * quarter
    send_blocks(own_base, quarter)

    @pl.when(jnp.logical_or(outer, lead == 0))
    def _():
        send_blocks(near_base, quarter)


    @pl.when(top == 0)
    def _():
        send_blocks(far_outer, quarter)

    @pl.when(outer)
    def _():
        send_blocks(far_inner, quarter)

    recv[pl.ds(me, 1)] = send[pl.ds(me, 1)]

    bias_copy.wait()
    eye = lax.broadcasted_iota(jnp.int32, (ROWS, group), 0) == lax.broadcasted_iota(jnp.int32, (ROWS, group), 1)

    def shift_of(owner):
        h0 = lax.rem(owner * pairs, kvh)
        shifts = []
        for p in range(pairs):
            row = bias_v[pl.ds(h0 + p, 1), :]
            shifts.append(jnp.sum(jnp.where(eye, jnp.broadcast_to(row, (ROWS, group)), 0.0), axis=1, keepdims=True))
        return jnp.concatenate(shifts, axis=0)

    scale = 1.0 / math.sqrt(hd)
    later = lax.broadcasted_iota(jnp.int32, (sub, 256), 0)
    column = lax.broadcasted_iota(jnp.int32, (sub, 256), 1)
    tri = ((later > column) | (column >= 128)).astype(jnp.float32).astype(jnp.bfloat16)
    left_half = lax.broadcasted_iota(jnp.int32, (pairs * ROWS, 2 * hd), 1) < hd

    late_lane = lax.broadcasted_iota(jnp.int32, (2 * packed_rows(pairs, group), 2 * hd), 1)

    def msg_copy(b, t):
        return pltpu.make_async_remote_copy(
            src_ref=msg.at[mt, b], dst_ref=msg.at[mt, b],
            send_sem=send_sem, recv_sem=mrecv_sem,
            device_id={"tp": t}, device_id_type=MESH,
        )

    def part_copy(i, t):
        return pltpu.make_async_remote_copy(
            src_ref=part_v.at[mt, i], dst_ref=part_v.at[mt, i],
            send_sem=send_sem, recv_sem=precv_sem.at[i],
            device_id={"tp": t}, device_id_type=MESH,
        )

    def late_copy(i, j, to, there, slot):
        return pltpu.make_async_remote_copy(
            src_ref=late_b.at[i, j], dst_ref=late_in.at[slot],
            send_sem=send_sem, recv_sem=lrecv_sem,
            device_id={"sp": to, "tp": there}, device_id_type=MESH,
        )

    def attend(items):
        scores = []
        shifts = []
        for queries, shift, rows, b in items:
            shifts.append(shift)
            for p in range(pairs):
                q = queries[p * ROWS:(p + 1) * ROWS, :]
                kv = rows[b, :, p * 2 * hd:(p + 1) * 2 * hd]
                scores.append(lax.dot_general(q, kv, (((1,), (1,)), ((), ())), preferred_element_type=jnp.float32))
        s = jnp.concatenate(scores, axis=0) * scale + jnp.concatenate(shifts, axis=0)
        low = jnp.log1p(jnp.exp(-jnp.abs(s)))
        keep = -(jnp.maximum(s, 0.0) + low)
        sig = jnp.minimum(s, 0.0) - low
        hi = keep.astype(jnp.bfloat16)
        rest = keep - hi.astype(jnp.float32)
        mid = rest.astype(jnp.bfloat16)
        lo = (rest - mid.astype(jnp.float32)).astype(jnp.bfloat16)
        sums = (
            jnp.dot(hi, tri, preferred_element_type=jnp.float32)
            + jnp.dot(mid, tri, preferred_element_type=jnp.float32)
            + jnp.dot(lo, tri, preferred_element_type=jnp.float32)
        )
        weights = jnp.exp(sig + sums[:, :sub]).astype(jnp.bfloat16)
        n = pairs * ROWS
        out = []
        for i, (_, _, rows, b) in enumerate(items):
            reads = []
            for p in range(pairs):
                kv = rows[b, :, p * 2 * hd:(p + 1) * 2 * hd]
                at = i * n + p * ROWS
                reads.append(jnp.dot(weights[at:at + ROWS], kv, preferred_element_type=jnp.float32))
            read = jnp.concatenate(reads, axis=0)
            both = jnp.where(left_half, sums[i * n:(i + 1) * n, 128:128 + 2 * hd], read)
            packed = [both[p * ROWS:p * ROWS + group] for p in range(pairs)]
            packed.append(jnp.zeros((packed_rows(pairs, group) - pairs * group, 2 * hd), jnp.float32))
            out.append(jnp.concatenate(packed, axis=0))
        return out

    shift = shift_of(me)

    def attend_blocks(blocks):
        for b, m in zip(blocks, attend([(q_pad, shift, recv, b) for b in blocks])):
            msg[mt, b] = m
            for t in range(1, tp):
                msg_copy(b, lax.rem(mt + t, tp)).start()

    def narrow(block):
        lane = late_lane[:block.shape[0]]
        high = block.astype(jnp.bfloat16).astype(jnp.float32)
        keep = jnp.where(lane < hd // 2, high, block - high)
        return jnp.where(lane < hd, keep, block).astype(jnp.bfloat16)

    def widen(ref):
        m = ref[...].astype(jnp.float32)
        lane = late_lane[:m.shape[0]]
        other = jnp.where(lane < hd // 2, pltpu.roll(m, 2 * hd - hd // 2, 1), pltpu.roll(m, hd // 2, 1))
        return jnp.where(lane < hd, m + other, m)

    def attend_late(i, owners):
        part_v[mt, i] = narrow(jnp.concatenate(
            attend([(q_all.at[owner], shift_of(owner), send, owner) for owner in owners]), axis=0
        ))

    def combine(parts):
        total = parts[0]
        acc = pltpu.roll(total, hd, 1)
        for m in parts[1:]:
            total = total + jnp.exp(acc) * m
            acc = acc + pltpu.roll(m, hd, 1)
        return jnp.where(late_lane < hd, pltpu.roll(acc, hd, 1), total)

    def send_late(i, owners, slot):
        wait_bytes(part_v.at[pl.ds(0, tp - 1), i], precv_sem.at[i])
        block = combine([widen(part_v.at[j, i]) for j in range(tp - 1, -1, -1)])
        late_b[i] = narrow(block).reshape(late_b.shape[1:])
        for j, owner in enumerate(owners):
            late_copy(i, j, owner, mt, (0, slot)).start()

    def send_urgent(i, owners):
        wait_bytes(part_v.at[0, i], precv_sem.at[i])
        block = combine([widen(part_v.at[mt, i]), widen(part_v.at[mt - 1, i])])
        late_b[i] = narrow(block).reshape(late_b.shape[1:])
        for j, owner in enumerate(owners):
            for t in range(tp):
                late_copy(i, j, owner, t, (mt // 2, me - quarter)).start()

    owners = inward + urgent + relaxed
    owners = [owners[i:i + 2] for i in range(0, 3 * quarter, 2)]
    first = quarter // 2

    def attend_class(place):
        wait_bytes(q_all.at[pl.ds(0, quarter)], qrecv_sem.at[place])
        for i in range(place * first, (place + 1) * first):
            attend_late(i, owners[i])
            if place != 1:
                for t in range(1, tp):
                    part_copy(i, lax.rem(mt + t, tp)).start()
            else:

                @pl.when(lead == 0)
                def _():
                    part_copy(i, mt + 1).start()

    @pl.when(inner)
    def _():
        attend_class(1)

    attend_class(0)

    @pl.when(inner)
    def _():
        attend_class(2)

    @pl.when(jnp.logical_and(inner, lead == 1))
    def _():
        for i in range(first, 2 * first):
            send_urgent(i, owners[i])
        send_blocks(near_base, quarter)

    @pl.when(inner)
    def _():
        send_blocks(far_inner, first)

    landed = [me] + same
    wait_bytes(recv.at[pl.ds(0, quarter - 1)], recv_sem.at[0])
    for i in range(0, quarter, 2):
        attend_blocks(landed[i:i + 2])

    def attend_early():
        wait_bytes(recv.at[pl.ds(0, quarter)], recv_sem.at[1])
        for i in range(0, quarter, 2):
            attend_blocks(early[i:i + 2])

    @pl.when(home)
    def _():
        attend_early()

    for i in range(first):
        send_late(i, owners[i], lax.rem(me, half))

    @pl.when(inner)
    def _():
        for i in range(2 * first, 3 * first):
            send_late(i, owners[i], me - quarter)
        send_blocks(far_inner + first, quarter - first)

    @pl.when(jnp.logical_not(home))
    def _():
        attend_early()

    some = pl.ds(0, half)
    others = pl.ds(0, tp - 1)

    @pl.when(home)
    def _():
        wait_bytes(late_in, lrecv_sem)
        for i in range(half):
            for k in range(chips):
                msg[2 * k + 1, quarter + i] = widen(late_in.at[k, i])

    @pl.when(jnp.logical_not(home))
    def _():
        wait_bytes(late_in.at[0], lrecv_sem)
        base = jnp.where(outer, quarter, (1 - top) * half)
        for i in range(half):
            msg[tp - 1, base + i] = widen(late_in.at[0, i])

    wait_bytes(send.at[pl.ds(0, sp - 1)], send_sem)
    wait_bytes(part_v.at[others, pl.ds(0, first)], send_sem)
    wait_bytes(late_b.at[pl.ds(0, first)], send_sem)

    @pl.when(inner)
    def _():
        wait_bytes(part_v.at[others, pl.ds(2 * first, first)], send_sem)
        wait_bytes(late_b.at[pl.ds(2 * first, first)], send_sem)

        @pl.when(lead == 0)
        def _():
            wait_bytes(part_v.at[0, pl.ds(first, first)], send_sem)

        @pl.when(lead == 1)
        def _():
            for _ in range(tp):
                wait_bytes(late_b.at[pl.ds(first, first)], send_sem)

    @pl.when(lead == 1)
    def _():
        wait_bytes(q_all, send_sem)

    wait_bytes(msg.at[others, some], send_sem)
    wait_bytes(msg.at[others, some], mrecv_sem)
    wait_bytes(recv.at[some], recv_sem.at[2])


def finish(sp, tp, hd, group, pairs, recv, msg, stored_hbm, first_hbm, fin, first_v, out_sem, first_sem):
    copies = [
        pltpu.make_async_copy(recv.at[b, :, pl.ds(p * 2 * hd, 2 * hd)], stored_hbm.at[p, b], out_sem)
        for b in range(sp)
        for p in range(pairs)
    ]
    for copy in copies:
        copy.start()
    left_half = lax.broadcasted_iota(jnp.int32, (packed_rows(pairs, group), 2 * hd), 1) < hd

    def add_block(i, carry):
        total, acc = carry
        b = sp - 1 - i
        for j in range(tp - 1, -1, -1):
            m = msg[j, b]
            total = total + jnp.exp(acc) * m
            acc = acc + pltpu.roll(m, hd, 1)
        return total, acc

    zero = jnp.zeros((packed_rows(pairs, group), 2 * hd), jnp.float32)
    total, _ = lax.fori_loop(0, sp, add_block, (zero, zero), unroll=True)
    total = jnp.where(left_half, 0.0, total)
    squares = jnp.sum(total * total, axis=1, keepdims=True) * (1.0 / hd)
    fin[...] = pltpu.roll(total * lax.rsqrt(squares + EPS_NORM), hd, 1)
    cols = [fin[pl.ds(g, pairs, stride=group), :][:, :hd] for g in range(group)]
    first_v[...] = jnp.concatenate(cols, axis=1).astype(first_v.dtype)
    first_copy = pltpu.make_async_copy(first_v, first_hbm, first_sem)
    first_copy.start()

    pltpu.make_async_copy(recv, recv, out_sem).wait()
    first_copy.wait()


def solution(mesh):
    sp, tp = mesh.shape["sp"], mesh.shape["tp"]

    def per_device(layer_input, key_weight, value_weight, queries, head_bias):
        seqs, sub, width = layer_input.shape
        pairs, group, hd = queries.shape
        kvh = head_bias.shape[0]
        x = layer_input.reshape(seqs * sub, width)
        block = pairs * 2 * hd
        any_spec = pl.BlockSpec(memory_space=pltpu.HBM)
        dma = pltpu.SemaphoreType.DMA
        handed = sp * sub * block * 2 + tp * sp * packed_rows(pairs, group) * 2 * hd * 4
        limit = VMEM_BYTES - handed
        late = sp // 4 * 3 // 2
        vmem_spec = pl.BlockSpec(memory_space=pltpu.VMEM)
        recv, msg = pl.pallas_call(
            functools.partial(kernel, sp, tp, seqs, sub, hd, kvh, group, pairs),
            out_shape=(
                pltpu.VMEM((sp, sub, block), jnp.bfloat16),
                pltpu.VMEM((tp, sp, packed_rows(pairs, group), 2 * hd), jnp.float32),
            ),
            in_specs=[any_spec] * 5,
            out_specs=(vmem_spec, vmem_spec),
            scratch_shapes=[
                pltpu.VMEM(x.shape, jnp.bfloat16),
                pltpu.VMEM((width, 2 * key_weight.shape[1]), jnp.bfloat16),
                pltpu.VMEM((group, pairs, hd), jnp.bfloat16),
                pltpu.VMEM(head_bias.shape, jnp.float32),
                pltpu.VMEM((sp, sub, block), jnp.bfloat16),
                pltpu.VMEM((pairs * ROWS, 2 * hd), jnp.bfloat16),
                pltpu.VMEM((sp, pairs * ROWS, 2 * hd), jnp.bfloat16),
                pltpu.VMEM((tp, late, 2 * packed_rows(pairs, group), 2 * hd), jnp.bfloat16),
                pltpu.VMEM((late, 2, packed_rows(pairs, group), 2 * hd), jnp.bfloat16),
                pltpu.VMEM((tp // 2, sp // 2, packed_rows(pairs, group), 2 * hd), jnp.bfloat16),
                dma((KC + 1,)),
                dma((KC,)),
                dma((2,)),
                dma(()),
                dma((3,)),
                dma(()),
                dma((3,)),
                dma((late,)),
                dma(()),
            ],
            compiler_params=pltpu.CompilerParams(
                collective_id=0, has_side_effects=True, vmem_limit_bytes=limit
            ),
        )(x, key_weight, value_weight, queries.transpose(1, 0, 2), head_bias)
        return pl.pallas_call(
            functools.partial(finish, sp, tp, hd, group, pairs),
            out_shape=(
                jax.ShapeDtypeStruct((pairs, sp, sub, 2 * hd), jnp.bfloat16),
                jax.ShapeDtypeStruct((pairs, group * hd), jnp.bfloat16),
            ),
            in_specs=[vmem_spec, vmem_spec],
            out_specs=(any_spec, any_spec),
            scratch_shapes=[
                pltpu.VMEM((packed_rows(pairs, group), 2 * hd), jnp.float32),
                pltpu.VMEM((pairs, group * hd), jnp.bfloat16),
                dma(()),
                dma(()),
            ],
            compiler_params=pltpu.CompilerParams(vmem_limit_bytes=VMEM_BYTES // 4),
        )(recv, msg)

    in_specs = (P(None, ("sp", "tp"), None), P(), P(), P("sp", None, None), P())
    out_specs = (P("sp", None, "tp", None), P("sp", None))
    return jax.shard_map(per_device, mesh=mesh, in_specs=in_specs, out_specs=out_specs, check_vma=False)
```

```python
import functools
import math

import jax
import jax.numpy as jnp
from jax import lax
from jax.experimental import pallas as pl
from jax.experimental.pallas import tpu as pltpu
from jax.sharding import PartitionSpec as P

EPS_NORM = 0.0001
MESH = pl.DeviceIdType.MESH
KC = 4
VMEM_BYTES = 60 * 1024 * 1024
ROWS = 8


def flip(index, k):
    bit = 1
    while bit <= k:
        if k & bit:
            index = index + (1 - 2 * ((index // bit) % 2)) * bit
        bit *= 2
    return index


def packed_rows(pairs, group):
    return pairs * group // 8 * 8 + 8


def kernel(
    sp, tp, seqs, sub, hd, kvh, group, pairs,
    x_hbm, wk_hbm, wv_hbm, q_hbm, bias_hbm,
    recv, msg,
    x_v, w_v, q_v, bias_v, send, q_pad, q_msg, q_all, part_v, late_b, late_in,
    x_sem, w_sem, small_sem, send_sem, recv_sem, mrecv_sem, qrecv_sem, precv_sem, lrecv_sem,
):
    me = lax.axis_index("sp")
    mt = lax.axis_index("tp")
    per_seq = kvh // pairs
    width = x_hbm.shape[1]
    kc = width // KC
    lead_seqs = sp // 4 // per_seq
    lead_rows = lead_seqs * sub

    q_copy = pltpu.make_async_copy(q_hbm, q_v, small_sem.at[0])
    bias_copy = pltpu.make_async_copy(bias_hbm, bias_v, small_sem.at[1])
    q_copy.start()
    bias_copy.start()
    kv_width = wk_hbm.shape[1]

    def x_copy(c):
        at = (pl.ds(0, lead_rows), pl.ds(c * kc, kc))
        return pltpu.make_async_copy(x_hbm.at[at], x_v.at[at], x_sem.at[c])

    def w_copy(i, c):
        rows = pl.ds(c * kc, kc)
        w_hbm = (wk_hbm, wv_hbm)[i]
        return pltpu.make_async_copy(w_hbm.at[rows], w_v.at[rows, pl.ds(i * kv_width, kv_width)], w_sem.at[c])

    rest = pl.ds(lead_rows, seqs * sub - lead_rows)
    x_rest = pltpu.make_async_copy(x_hbm.at[rest], x_v.at[rest], x_sem.at[KC])
    for c in range(KC):
        x_copy(c).start()
        w_copy(0, c).start()
        w_copy(1, c).start()
    x_rest.start()

    msg[...] = jnp.zeros_like(msg)

    top = me // (sp // 2)
    half = sp // 2
    quarter = sp // 4
    lead = lax.rem(mt, 2)
    outer = lax.rem(me // quarter, 3) == 0
    inner = jnp.logical_not(outer)
    home = me // quarter == 0
    chips = tp // 2
    far_outer = (1 - top) * 3 * quarter
    far_inner = quarter + (1 - top) * quarter
    near = [flip(me, k) for k in range(quarter, half)]
    inward = [far_inner + flip(lax.rem(me, 2), j) for j in range(quarter)]
    outward = [far_outer + flip(lax.rem(me, 2), j) for j in range(quarter)]
    same = [flip(me, k) for k in range(1, quarter)]
    early = [jnp.where(outer, a, b) for a, b in zip(outward, near)]
    late = [jnp.where(outer, a, b) for a, b in zip(near, outward)]
    urgent = [jnp.where(top == 0, a, b) for a, b in zip(near, outward)]
    relaxed = [jnp.where(top == 0, a, b) for a, b in zip(outward, near)]

    barrier = pltpu.get_barrier_semaphore()
    for k in range(sp - 1, 0, -1):
        pl.semaphore_signal(barrier, inc=1, device_id={"sp": flip(me, k)}, device_id_type=MESH)
    for k in range(1, tp):
        pl.semaphore_signal(barrier, inc=1, device_id={"tp": lax.rem(mt + k, tp)}, device_id_type=MESH)

    @pl.when(home)
    def _():
        for t in range(1, tp, 2):
            for to in range(quarter, 3 * quarter):

                @pl.when(t != mt)
                def _():
                    pl.semaphore_signal(barrier, inc=1, device_id={"sp": to, "tp": t}, device_id_type=MESH)

    def ask(owners):
        for owner in owners:
            pl.semaphore_signal(barrier, inc=1, device_id={"sp": owner, "tp": mt + 1}, device_id_type=MESH)

    @pl.when(lead == 0)
    def _():
        ask(inward)

        @pl.when(inner)
        def _():
            ask(near + outward)

    def wait_bytes(ref, sem):
        pltpu.make_async_copy(ref, ref, sem).wait()

    def pack(rows, base):
        for i in range(rows.shape[0] // sub):
            for part in range(per_seq):
                out = []
                for p in range(pairs):
                    c0 = (part * pairs + p) * hd
                    out.append(rows[i * sub:(i + 1) * sub, c0:c0 + hd])
                    out.append(rows[i * sub:(i + 1) * sub, kv_width + c0:kv_width + c0 + hd])
                send[base + i * per_seq + part] = jnp.concatenate(out, axis=1).astype(jnp.bfloat16)

    def send_block(to):
        near_class = jnp.where(outer, 1, 2)
        place = jnp.where(to // half == top, near_class, jnp.where(to // quarter == far_outer // quarter, near_class, 2))
        place = jnp.where(to // quarter == me // quarter, 0, place)

        @pl.when(to != me)
        def _():
            pltpu.make_async_remote_copy(
                src_ref=send.at[to], dst_ref=recv.at[me],
                send_sem=send_sem, recv_sem=recv_sem.at[place],
                device_id={"sp": to}, device_id_type=MESH,
            ).start()

    def send_blocks(base, count):
        for j in range(count):
            send_block(base + j)

    def query_copy(to, core, place):
        return pltpu.make_async_remote_copy(
            src_ref=q_msg, dst_ref=q_all.at[me],
            send_sem=send_sem, recv_sem=qrecv_sem.at[place],
            device_id={"sp": to, "tp": mt - core}, device_id_type=MESH,
        )

    def enter():
        pl.semaphore_wait(barrier, sp + tp - 2 + lead * (half + jnp.where(inner, quarter * (tp - 1), 0)))

        @pl.when(lead == 1)
        def _():
            for group_of in (inward, late):
                for core in range(2):
                    for to in group_of:
                        query_copy(to, core, jnp.where(outer, 1 + top, 0)).start()

    def prepare_queries():
        q_copy.wait()
        blank = jnp.zeros((group, hd), jnp.float32)
        q_rows = [q_v[:, p, :].astype(jnp.float32) for p in range(pairs)] + [blank]
        below = jnp.zeros((ROWS - group, 2 * hd), jnp.float32)

        def q_tile(left, right):
            tile = jnp.concatenate([left, right], axis=1)
            return jnp.concatenate([tile, below], axis=0).astype(jnp.bfloat16)

        for p in range(0, pairs, 2):
            q_msg[p // 2 * ROWS:(p // 2 + 1) * ROWS, :] = q_tile(q_rows[p], q_rows[p + 1])
        for p in range(pairs):
            q_pad[p * ROWS:(p + 1) * ROWS, :] = q_tile(q_rows[p], blank)

    rows = None
    for c in range(KC):
        x_copy(c).wait()
        wait_bytes(w_v.at[pl.ds(c * kc, kc)], w_sem.at[c])
        part = jnp.dot(
            x_v[:lead_rows, c * kc:(c + 1) * kc], w_v[c * kc:(c + 1) * kc, :],
            preferred_element_type=jnp.float32,
        )
        rows = part if rows is None else rows + part
        if c == 0:
            prepare_queries()
    pack(rows, 0)

    @pl.when(top == 1)
    def _():
        enter()
        send_blocks(far_outer, quarter)

    x_rest.wait()
    pack(jnp.dot(x_v[lead_rows:, :], w_v[...], preferred_element_type=jnp.float32), quarter)

    @pl.when(top == 0)
    def _():
        enter()

    own_base = me // quarter * quarter
    near_base = top * half + quarter - lax.rem(me // quarter, 2) * quarter
    send_blocks(own_base, quarter)

    @pl.when(jnp.logical_or(outer, lead == 0))
    def _():
        send_blocks(near_base, quarter)


    @pl.when(top == 0)
    def _():
        send_blocks(far_outer, quarter)

    @pl.when(outer)
    def _():
        send_blocks(far_inner, quarter)

    recv[pl.ds(me, 1)] = send[pl.ds(me, 1)]

    bias_copy.wait()
    eye = lax.broadcasted_iota(jnp.int32, (ROWS, group), 0) == lax.broadcasted_iota(jnp.int32, (ROWS, group), 1)

    def shift_of(owner):
        h0 = lax.rem(owner * pairs, kvh)
        shifts = []
        for p in range(pairs):
            row = bias_v[pl.ds(h0 + p, 1), :]
            shifts.append(jnp.sum(jnp.where(eye, jnp.broadcast_to(row, (ROWS, group)), 0.0), axis=1, keepdims=True))
        return jnp.concatenate(shifts, axis=0)

    scale = 1.0 / math.sqrt(hd)
    later = lax.broadcasted_iota(jnp.int32, (sub, 256), 0)
    column = lax.broadcasted_iota(jnp.int32, (sub, 256), 1)
    tri = ((later > column) | (column >= 128)).astype(jnp.float32).astype(jnp.bfloat16)
    left_half = lax.broadcasted_iota(jnp.int32, (pairs * ROWS, 2 * hd), 1) < hd

    late_lane = lax.broadcasted_iota(jnp.int32, (2 * packed_rows(pairs, group), 2 * hd), 1)

    def msg_copy(b, t):
        return pltpu.make_async_remote_copy(
            src_ref=msg.at[mt, b], dst_ref=msg.at[mt, b],
            send_sem=send_sem, recv_sem=mrecv_sem,
            device_id={"tp": t}, device_id_type=MESH,
        )

    def part_copy(i, t):
        return pltpu.make_async_remote_copy(
            src_ref=part_v.at[mt, i], dst_ref=part_v.at[mt, i],
            send_sem=send_sem, recv_sem=precv_sem.at[i],
            device_id={"tp": t}, device_id_type=MESH,
        )

    def late_copy(i, j, to, there, slot):
        return pltpu.make_async_remote_copy(
            src_ref=late_b.at[i, j], dst_ref=late_in.at[slot],
            send_sem=send_sem, recv_sem=lrecv_sem,
            device_id={"sp": to, "tp": there}, device_id_type=MESH,
        )

    def attend(items):
        scores = []
        shifts = []
        for queries, shift, rows, b in items:
            shifts.append(shift)
            for p in range(pairs):
                q = queries[p * ROWS:(p + 1) * ROWS, :]
                kv = rows[b, :, p * 2 * hd:(p + 1) * 2 * hd]
                scores.append(lax.dot_general(q, kv, (((1,), (1,)), ((), ())), preferred_element_type=jnp.float32))
        s = jnp.concatenate(scores, axis=0) * scale + jnp.concatenate(shifts, axis=0)
        low = jnp.log1p(jnp.exp(-jnp.abs(s)))
        keep = -(jnp.maximum(s, 0.0) + low)
        sig = jnp.minimum(s, 0.0) - low
        hi = keep.astype(jnp.bfloat16)
        rest = keep - hi.astype(jnp.float32)
        mid = rest.astype(jnp.bfloat16)
        lo = (rest - mid.astype(jnp.float32)).astype(jnp.bfloat16)
        sums = (
            jnp.dot(hi, tri, preferred_element_type=jnp.float32)
            + jnp.dot(mid, tri, preferred_element_type=jnp.float32)
            + jnp.dot(lo, tri, preferred_element_type=jnp.float32)
        )
        weights = jnp.exp(sig + sums[:, :sub]).astype(jnp.bfloat16)
        n = pairs * ROWS
        out = []
        for i, (_, _, rows, b) in enumerate(items):
            reads = []
            for p in range(pairs):
                kv = rows[b, :, p * 2 * hd:(p + 1) * 2 * hd]
                at = i * n + p * ROWS
                reads.append(jnp.dot(weights[at:at + ROWS], kv, preferred_element_type=jnp.float32))
            read = jnp.concatenate(reads, axis=0)
            both = jnp.where(left_half, sums[i * n:(i + 1) * n, 128:128 + 2 * hd], read)
            packed = [both[p * ROWS:p * ROWS + group] for p in range(pairs)]
            packed.append(jnp.zeros((packed_rows(pairs, group) - pairs * group, 2 * hd), jnp.float32))
            out.append(jnp.concatenate(packed, axis=0))
        return out

    shift = shift_of(me)

    def attend_blocks(blocks):
        for b, m in zip(blocks, attend([(q_pad, shift, recv, b) for b in blocks])):
            msg[mt, b] = m
            for t in range(1, tp):
                msg_copy(b, lax.rem(mt + t, tp)).start()

    def narrow(block):
        lane = late_lane[:block.shape[0]]
        high = block.astype(jnp.bfloat16).astype(jnp.float32)
        keep = jnp.where(lane < hd // 2, high, block - high)
        return jnp.where(lane < hd, keep, block).astype(jnp.bfloat16)

    def widen(ref):
        m = ref[...].astype(jnp.float32)
        lane = late_lane[:m.shape[0]]
        other = jnp.where(lane < hd // 2, pltpu.roll(m, 2 * hd - hd // 2, 1), pltpu.roll(m, hd // 2, 1))
        return jnp.where(lane < hd, m + other, m)

    def spread(owner):
        tiles = q_all[owner].astype(jnp.float32)
        lane = lax.broadcasted_iota(jnp.int32, (ROWS, 2 * hd), 1)
        out = []
        for p in range(pairs):
            tile = tiles[p // 2 * ROWS:(p // 2 + 1) * ROWS]
            if p % 2:
                tile = pltpu.roll(tile, hd, 1)
            out.append(jnp.where(lane < hd, tile, 0.0))
        return jnp.concatenate(out, axis=0).astype(jnp.bfloat16)

    def attend_late(i, owners):
        part_v[mt, i] = narrow(jnp.concatenate(
            attend([(spread(owner), shift_of(owner), send, owner) for owner in owners]), axis=0
        ))

    def combine(parts):
        total = parts[0]
        acc = pltpu.roll(total, hd, 1)
        for m in parts[1:]:
            total = total + jnp.exp(acc) * m
            acc = acc + pltpu.roll(m, hd, 1)
        return jnp.where(late_lane < hd, pltpu.roll(acc, hd, 1), total)

    def send_late(i, owners, slot):
        wait_bytes(part_v.at[pl.ds(0, tp - 1), i], precv_sem.at[i])
        block = combine([widen(part_v.at[j, i]) for j in range(tp - 1, -1, -1)])
        late_b[i] = narrow(block).reshape(late_b.shape[1:])
        for j, owner in enumerate(owners):
            late_copy(i, j, owner, mt, (0, slot)).start()

    def send_urgent(i, owners):
        wait_bytes(part_v.at[0, i], precv_sem.at[i])
        block = combine([widen(part_v.at[mt, i]), widen(part_v.at[mt - 1, i])])
        late_b[i] = narrow(block).reshape(late_b.shape[1:])
        for j, owner in enumerate(owners):
            for t in range(tp):
                late_copy(i, j, owner, t, (mt // 2, me - quarter)).start()

    owners = inward + urgent + relaxed
    owners = [owners[i:i + 2] for i in range(0, 3 * quarter, 2)]
    first = quarter // 2

    def attend_class(place):
        wait_bytes(q_all.at[pl.ds(0, quarter)], qrecv_sem.at[place])
        for i in range(place * first, (place + 1) * first):
            attend_late(i, owners[i])
            if place != 1:
                for t in range(1, tp):
                    part_copy(i, lax.rem(mt + t, tp)).start()
            else:

                @pl.when(lead == 0)
                def _():
                    part_copy(i, mt + 1).start()

    @pl.when(inner)
    def _():
        attend_class(1)

    attend_class(0)

    @pl.when(inner)
    def _():
        attend_class(2)

    @pl.when(jnp.logical_and(inner, lead == 1))
    def _():
        for i in range(first, 2 * first):
            send_urgent(i, owners[i])
        send_blocks(near_base, quarter)

    @pl.when(inner)
    def _():
        send_blocks(far_inner, first)

    landed = [me] + same
    wait_bytes(recv.at[pl.ds(0, quarter - 1)], recv_sem.at[0])
    for i in range(0, quarter, 2):
        attend_blocks(landed[i:i + 2])

    def attend_early():
        wait_bytes(recv.at[pl.ds(0, quarter)], recv_sem.at[1])
        for i in range(0, quarter, 2):
            attend_blocks(early[i:i + 2])

    @pl.when(home)
    def _():
        attend_early()

    for i in range(first):
        send_late(i, owners[i], lax.rem(me, half))

    @pl.when(inner)
    def _():
        for i in range(2 * first, 3 * first):
            send_late(i, owners[i], me - quarter)
        send_blocks(far_inner + first, quarter - first)

    @pl.when(jnp.logical_not(home))
    def _():
        attend_early()

    some = pl.ds(0, half)
    others = pl.ds(0, tp - 1)

    @pl.when(home)
    def _():
        wait_bytes(late_in, lrecv_sem)
        for i in range(half):
            for k in range(chips):
                msg[2 * k + 1, quarter + i] = widen(late_in.at[k, i])

    @pl.when(jnp.logical_not(home))
    def _():
        wait_bytes(late_in.at[0], lrecv_sem)
        base = jnp.where(outer, quarter, (1 - top) * half)
        for i in range(half):
            msg[tp - 1, base + i] = widen(late_in.at[0, i])

    wait_bytes(send.at[pl.ds(0, sp - 1)], send_sem)
    wait_bytes(part_v.at[others, pl.ds(0, first)], send_sem)
    wait_bytes(late_b.at[pl.ds(0, first)], send_sem)

    @pl.when(inner)
    def _():
        wait_bytes(part_v.at[others, pl.ds(2 * first, first)], send_sem)
        wait_bytes(late_b.at[pl.ds(2 * first, first)], send_sem)

        @pl.when(lead == 0)
        def _():
            wait_bytes(part_v.at[0, pl.ds(first, first)], send_sem)

        @pl.when(lead == 1)
        def _():
            for _ in range(tp):
                wait_bytes(late_b.at[pl.ds(first, first)], send_sem)

    @pl.when(lead == 1)
    def _():
        wait_bytes(q_all, send_sem)

    wait_bytes(msg.at[others, some], send_sem)
    wait_bytes(msg.at[others, some], mrecv_sem)
    wait_bytes(recv.at[some], recv_sem.at[2])


def finish(sp, tp, hd, group, pairs, recv, msg, stored_hbm, first_hbm, fin, first_v, out_sem, first_sem):
    copies = [
        pltpu.make_async_copy(recv.at[b, :, pl.ds(p * 2 * hd, 2 * hd)], stored_hbm.at[p, b], out_sem)
        for b in range(sp)
        for p in range(pairs)
    ]
    for copy in copies:
        copy.start()
    left_half = lax.broadcasted_iota(jnp.int32, (packed_rows(pairs, group), 2 * hd), 1) < hd

    def add_block(i, carry):
        total, acc = carry
        b = sp - 1 - i
        for j in range(tp - 1, -1, -1):
            m = msg[j, b]
            total = total + jnp.exp(acc) * m
            acc = acc + pltpu.roll(m, hd, 1)
        return total, acc

    zero = jnp.zeros((packed_rows(pairs, group), 2 * hd), jnp.float32)
    total, _ = lax.fori_loop(0, sp, add_block, (zero, zero), unroll=True)
    total = jnp.where(left_half, 0.0, total)
    squares = jnp.sum(total * total, axis=1, keepdims=True) * (1.0 / hd)
    fin[...] = pltpu.roll(total * lax.rsqrt(squares + EPS_NORM), hd, 1)
    cols = [fin[pl.ds(g, pairs, stride=group), :][:, :hd] for g in range(group)]
    first_v[...] = jnp.concatenate(cols, axis=1).astype(first_v.dtype)
    first_copy = pltpu.make_async_copy(first_v, first_hbm, first_sem)
    first_copy.start()

    pltpu.make_async_copy(recv, recv, out_sem).wait()
    first_copy.wait()


def solution(mesh):
    sp, tp = mesh.shape["sp"], mesh.shape["tp"]

    def per_device(layer_input, key_weight, value_weight, queries, head_bias):
        seqs, sub, width = layer_input.shape
        pairs, group, hd = queries.shape
        kvh = head_bias.shape[0]
        x = layer_input.reshape(seqs * sub, width)
        block = pairs * 2 * hd
        any_spec = pl.BlockSpec(memory_space=pltpu.HBM)
        dma = pltpu.SemaphoreType.DMA
        handed = sp * sub * block * 2 + tp * sp * packed_rows(pairs, group) * 2 * hd * 4
        limit = VMEM_BYTES - handed
        late = sp // 4 * 3 // 2
        vmem_spec = pl.BlockSpec(memory_space=pltpu.VMEM)
        recv, msg = pl.pallas_call(
            functools.partial(kernel, sp, tp, seqs, sub, hd, kvh, group, pairs),
            out_shape=(
                pltpu.VMEM((sp, sub, block), jnp.bfloat16),
                pltpu.VMEM((tp, sp, packed_rows(pairs, group), 2 * hd), jnp.float32),
            ),
            in_specs=[any_spec] * 5,
            out_specs=(vmem_spec, vmem_spec),
            scratch_shapes=[
                pltpu.VMEM(x.shape, jnp.bfloat16),
                pltpu.VMEM((width, 2 * key_weight.shape[1]), jnp.bfloat16),
                pltpu.VMEM((group, pairs, hd), jnp.bfloat16),
                pltpu.VMEM(head_bias.shape, jnp.float32),
                pltpu.VMEM((sp, sub, block), jnp.bfloat16),
                pltpu.VMEM((pairs * ROWS, 2 * hd), jnp.bfloat16),
                pltpu.VMEM(((pairs + 1) // 2 * ROWS, 2 * hd), jnp.bfloat16),
                pltpu.VMEM((sp, (pairs + 1) // 2 * ROWS, 2 * hd), jnp.bfloat16),
                pltpu.VMEM((tp, late, 2 * packed_rows(pairs, group), 2 * hd), jnp.bfloat16),
                pltpu.VMEM((late, 2, packed_rows(pairs, group), 2 * hd), jnp.bfloat16),
                pltpu.VMEM((tp // 2, sp // 2, packed_rows(pairs, group), 2 * hd), jnp.bfloat16),
                dma((KC + 1,)),
                dma((KC,)),
                dma((2,)),
                dma(()),
                dma((3,)),
                dma(()),
                dma((3,)),
                dma((late,)),
                dma(()),
            ],
            compiler_params=pltpu.CompilerParams(
                collective_id=0, has_side_effects=True, vmem_limit_bytes=limit
            ),
        )(x, key_weight, value_weight, queries.transpose(1, 0, 2), head_bias)
        return pl.pallas_call(
            functools.partial(finish, sp, tp, hd, group, pairs),
            out_shape=(
                jax.ShapeDtypeStruct((pairs, sp, sub, 2 * hd), jnp.bfloat16),
                jax.ShapeDtypeStruct((pairs, group * hd), jnp.bfloat16),
            ),
            in_specs=[vmem_spec, vmem_spec],
            out_specs=(any_spec, any_spec),
            scratch_shapes=[
                pltpu.VMEM((packed_rows(pairs, group), 2 * hd), jnp.float32),
                pltpu.VMEM((pairs, group * hd), jnp.bfloat16),
                dma(()),
                dma(()),
            ],
            compiler_params=pltpu.CompilerParams(vmem_limit_bytes=VMEM_BYTES // 4),
        )(recv, msg)

    in_specs = (P(None, ("sp", "tp"), None), P(), P(), P("sp", None, None), P())
    out_specs = (P("sp", None, "tp", None), P("sp", None))
    return jax.shard_map(per_device, mesh=mesh, in_specs=in_specs, out_specs=out_specs, check_vma=False)
```

```python
import functools
import math

import jax
import jax.numpy as jnp
from jax import lax
from jax.experimental import pallas as pl
from jax.experimental.pallas import tpu as pltpu
from jax.sharding import PartitionSpec as P

EPS_NORM = 0.0001
MESH = pl.DeviceIdType.MESH
KC = 4
VMEM_BYTES = 60 * 1024 * 1024
ROWS = 8


def flip(index, k):
    bit = 1
    while bit <= k:
        if k & bit:
            index = index + (1 - 2 * ((index // bit) % 2)) * bit
        bit *= 2
    return index


def packed_rows(pairs, group):
    return pairs * group // 8 * 8 + 8


def kernel(
    sp, tp, seqs, sub, hd, kvh, group, pairs,
    x_hbm, wk_hbm, wv_hbm, q_hbm, bias_hbm,
    recv, msg,
    x_v, w_v, q_v, bias_v, send, q_pad, q_msg, q_all, part_v, late_b, late_in,
    x_sem, w_sem, small_sem, send_sem, recv_sem, mrecv_sem, qrecv_sem, precv_sem, lrecv_sem,
):
    me = lax.axis_index("sp")
    mt = lax.axis_index("tp")
    per_seq = kvh // pairs
    width = x_hbm.shape[1]
    kc = width // KC
    lead_seqs = sp // 4 // per_seq
    lead_rows = lead_seqs * sub

    q_copy = pltpu.make_async_copy(q_hbm, q_v, small_sem.at[0])
    bias_copy = pltpu.make_async_copy(bias_hbm, bias_v, small_sem.at[1])
    q_copy.start()
    bias_copy.start()
    kv_width = wk_hbm.shape[1]

    def x_copy(c):
        at = (pl.ds(0, lead_rows), pl.ds(c * kc, kc))
        return pltpu.make_async_copy(x_hbm.at[at], x_v.at[at], x_sem.at[c])

    def w_copy(i, c):
        rows = pl.ds(c * kc, kc)
        w_hbm = (wk_hbm, wv_hbm)[i]
        return pltpu.make_async_copy(w_hbm.at[rows], w_v.at[rows, pl.ds(i * kv_width, kv_width)], w_sem.at[c])

    rest = pl.ds(lead_rows, seqs * sub - lead_rows)
    x_rest = pltpu.make_async_copy(x_hbm.at[rest], x_v.at[rest], x_sem.at[KC])
    for c in range(KC):
        x_copy(c).start()
        w_copy(0, c).start()
        w_copy(1, c).start()
    x_rest.start()

    msg[...] = jnp.zeros_like(msg)

    top = me // (sp // 2)
    half = sp // 2
    quarter = sp // 4
    lead = lax.rem(mt, 2)
    outer = lax.rem(me // quarter, 3) == 0
    inner = jnp.logical_not(outer)
    home = me // quarter == 0
    chips = tp // 2
    far_outer = (1 - top) * 3 * quarter
    far_inner = quarter + (1 - top) * quarter
    near = [flip(me, k) for k in range(quarter, half)]
    inward = [far_inner + flip(lax.rem(me, 2), j) for j in range(quarter)]
    outward = [far_outer + flip(lax.rem(me, 2), j) for j in range(quarter)]
    same = [flip(me, k) for k in range(1, quarter)]
    early = [jnp.where(outer, a, b) for a, b in zip(outward, near)]
    late = [jnp.where(outer, a, b) for a, b in zip(near, outward)]
    urgent = [jnp.where(top == 0, a, b) for a, b in zip(near, outward)]
    relaxed = [jnp.where(top == 0, a, b) for a, b in zip(outward, near)]

    barrier = pltpu.get_barrier_semaphore()
    for k in range(sp - 1, 0, -1):
        pl.semaphore_signal(barrier, inc=1, device_id={"sp": flip(me, k)}, device_id_type=MESH)
    for k in range(1, tp):
        pl.semaphore_signal(barrier, inc=1, device_id={"tp": lax.rem(mt + k, tp)}, device_id_type=MESH)

    @pl.when(home)
    def _():
        for t in range(1, tp, 2):
            for to in range(quarter, 3 * quarter):

                @pl.when(t != mt)
                def _():
                    pl.semaphore_signal(barrier, inc=1, device_id={"sp": to, "tp": t}, device_id_type=MESH)

    def ask(owners):
        for owner in owners:
            pl.semaphore_signal(barrier, inc=1, device_id={"sp": owner, "tp": mt + 1}, device_id_type=MESH)

    @pl.when(lead == 0)
    def _():
        ask(inward)

        @pl.when(inner)
        def _():
            ask(near + outward)

    def wait_bytes(ref, sem):
        pltpu.make_async_copy(ref, ref, sem).wait()

    def pack(rows, base):
        for i in range(rows.shape[0] // sub):
            for part in range(per_seq):
                out = []
                for p in range(pairs):
                    c0 = (part * pairs + p) * hd
                    out.append(rows[i * sub:(i + 1) * sub, c0:c0 + hd])
                    out.append(rows[i * sub:(i + 1) * sub, kv_width + c0:kv_width + c0 + hd])
                send[base + i * per_seq + part] = jnp.concatenate(out, axis=1).astype(jnp.bfloat16)

    def send_block(to):
        near_class = jnp.where(outer, 1, 2)
        place = jnp.where(to // half == top, near_class, jnp.where(to // quarter == far_outer // quarter, near_class, 2))
        place = jnp.where(to // quarter == me // quarter, 0, place)

        @pl.when(to != me)
        def _():
            pltpu.make_async_remote_copy(
                src_ref=send.at[to], dst_ref=recv.at[me],
                send_sem=send_sem, recv_sem=recv_sem.at[place],
                device_id={"sp": to}, device_id_type=MESH,
            ).start()

    def send_blocks(base, count):
        for j in range(count):
            send_block(base + j)

    def query_copy(to, core, place):
        return pltpu.make_async_remote_copy(
            src_ref=q_msg, dst_ref=q_all.at[me],
            send_sem=send_sem, recv_sem=qrecv_sem.at[place],
            device_id={"sp": to, "tp": mt - core}, device_id_type=MESH,
        )

    def enter():
        pl.semaphore_wait(barrier, sp + tp - 2 + lead * (half + jnp.where(inner, quarter * (tp - 1), 0)))

        @pl.when(lead == 1)
        def _():
            for group_of in (inward, late):
                for core in range(2):
                    for to in group_of:
                        query_copy(to, core, jnp.where(outer, 1 + top, 0)).start()

    def prepare_queries():
        q_copy.wait()
        blank = jnp.zeros((group, hd), jnp.float32)
        q_rows = [q_v[:, p, :].astype(jnp.float32) for p in range(pairs)] + [blank]
        below = jnp.zeros((ROWS - group, 2 * hd), jnp.float32)

        def q_tile(left, right):
            tile = jnp.concatenate([left, right], axis=1)
            return jnp.concatenate([tile, below], axis=0).astype(jnp.bfloat16)

        for p in range(0, pairs, 2):
            q_msg[p // 2 * ROWS:(p // 2 + 1) * ROWS, :] = q_tile(q_rows[p], q_rows[p + 1])
        for p in range(pairs):
            q_pad[p * ROWS:(p + 1) * ROWS, :] = q_tile(q_rows[p], blank)

    rows = None
    for c in range(KC):
        x_copy(c).wait()
        wait_bytes(w_v.at[pl.ds(c * kc, kc)], w_sem.at[c])
        part = jnp.dot(
            x_v[:lead_rows, c * kc:(c + 1) * kc], w_v[c * kc:(c + 1) * kc, :],
            preferred_element_type=jnp.float32,
        )
        rows = part if rows is None else rows + part
        if c == 0:
            prepare_queries()
    pack(rows, 0)

    @pl.when(top == 1)
    def _():
        enter()
        send_blocks(far_outer, quarter)

    x_rest.wait()
    pack(jnp.dot(x_v[lead_rows:, :], w_v[...], preferred_element_type=jnp.float32), quarter)

    @pl.when(top == 0)
    def _():
        enter()

    own_base = me // quarter * quarter
    near_base = top * half + quarter - lax.rem(me // quarter, 2) * quarter
    send_blocks(own_base, quarter)

    @pl.when(jnp.logical_or(outer, lead == 0))
    def _():
        send_blocks(near_base, quarter)


    @pl.when(top == 0)
    def _():
        send_blocks(far_outer, quarter)

    @pl.when(outer)
    def _():
        send_blocks(far_inner, quarter)

    recv[pl.ds(me, 1)] = send[pl.ds(me, 1)]

    bias_copy.wait()
    eye = lax.broadcasted_iota(jnp.int32, (ROWS, group), 0) == lax.broadcasted_iota(jnp.int32, (ROWS, group), 1)

    def shift_of(owner):
        h0 = lax.rem(owner * pairs, kvh)
        shifts = []
        for p in range(pairs):
            row = bias_v[pl.ds(h0 + p, 1), :]
            shifts.append(jnp.sum(jnp.where(eye, jnp.broadcast_to(row, (ROWS, group)), 0.0), axis=1, keepdims=True))
        return jnp.concatenate(shifts, axis=0)

    scale = 1.0 / math.sqrt(hd)
    later = lax.broadcasted_iota(jnp.int32, (sub, 256), 0)
    column = lax.broadcasted_iota(jnp.int32, (sub, 256), 1)
    tri = ((later > column) | (column >= 128)).astype(jnp.float32).astype(jnp.bfloat16)
    left_half = lax.broadcasted_iota(jnp.int32, (pairs * ROWS, 2 * hd), 1) < hd

    late_lane = lax.broadcasted_iota(jnp.int32, (2 * packed_rows(pairs, group), 2 * hd), 1)

    def msg_copy(b, t):
        return pltpu.make_async_remote_copy(
            src_ref=msg.at[mt, b], dst_ref=msg.at[mt, b],
            send_sem=send_sem, recv_sem=mrecv_sem,
            device_id={"tp": t}, device_id_type=MESH,
        )

    def part_copy(i, t):
        return pltpu.make_async_remote_copy(
            src_ref=part_v.at[mt, i], dst_ref=part_v.at[mt, i],
            send_sem=send_sem, recv_sem=precv_sem.at[i],
            device_id={"tp": t}, device_id_type=MESH,
        )

    def late_copy(i, j, to, there, slot):
        return pltpu.make_async_remote_copy(
            src_ref=late_b.at[i, j], dst_ref=late_in.at[slot],
            send_sem=send_sem, recv_sem=lrecv_sem,
            device_id={"sp": to, "tp": there}, device_id_type=MESH,
        )

    def attend(items):
        scores = []
        shifts = []
        for queries, shift, rows, b in items:
            shifts.append(shift)
            for p in range(pairs):
                q = queries[p * ROWS:(p + 1) * ROWS, :]
                kv = rows[b, :, p * 2 * hd:(p + 1) * 2 * hd]
                scores.append(lax.dot_general(q, kv, (((1,), (1,)), ((), ())), preferred_element_type=jnp.float32))
        s = jnp.concatenate(scores, axis=0) * scale + jnp.concatenate(shifts, axis=0)
        low = jnp.log1p(jnp.exp(-jnp.abs(s)))
        keep = -(jnp.maximum(s, 0.0) + low)
        sig = jnp.minimum(s, 0.0) - low
        hi = keep.astype(jnp.bfloat16)
        rest = keep - hi.astype(jnp.float32)
        mid = rest.astype(jnp.bfloat16)
        lo = (rest - mid.astype(jnp.float32)).astype(jnp.bfloat16)
        sums = (
            jnp.dot(hi, tri, preferred_element_type=jnp.float32)
            + jnp.dot(mid, tri, preferred_element_type=jnp.float32)
            + jnp.dot(lo, tri, preferred_element_type=jnp.float32)
        )
        weights = jnp.exp(sig + sums[:, :sub]).astype(jnp.bfloat16)
        n = pairs * ROWS
        out = []
        for i, (_, _, rows, b) in enumerate(items):
            reads = []
            for p in range(pairs):
                kv = rows[b, :, p * 2 * hd:(p + 1) * 2 * hd]
                at = i * n + p * ROWS
                reads.append(jnp.dot(weights[at:at + ROWS], kv, preferred_element_type=jnp.float32))
            read = jnp.concatenate(reads, axis=0)
            both = jnp.where(left_half, sums[i * n:(i + 1) * n, 128:128 + 2 * hd], read)
            packed = [both[p * ROWS:p * ROWS + group] for p in range(pairs)]
            packed.append(jnp.zeros((packed_rows(pairs, group) - pairs * group, 2 * hd), jnp.float32))
            out.append(jnp.concatenate(packed, axis=0))
        return out

    shift = shift_of(me)

    def attend_blocks(blocks):
        for b, m in zip(blocks, attend([(q_pad, shift, recv, b) for b in blocks])):
            msg[mt, b] = m
            for t in range(1, tp):
                msg_copy(b, lax.rem(mt + t, tp)).start()

    def narrow(block):
        lane = late_lane[:block.shape[0]]
        high = block.astype(jnp.bfloat16).astype(jnp.float32)
        keep = jnp.where(lane < hd // 2, high, block - high)
        return jnp.where(lane < hd, keep, block).astype(jnp.bfloat16)

    def widen(ref):
        m = ref[...].astype(jnp.float32)
        lane = late_lane[:m.shape[0]]
        other = jnp.where(lane < hd // 2, pltpu.roll(m, 2 * hd - hd // 2, 1), pltpu.roll(m, hd // 2, 1))
        return jnp.where(lane < hd, m + other, m)

    def spread(owner):
        tiles = q_all[owner].astype(jnp.float32)
        lane = lax.broadcasted_iota(jnp.int32, (ROWS, 2 * hd), 1)
        out = []
        for p in range(pairs):
            tile = tiles[p // 2 * ROWS:(p // 2 + 1) * ROWS]
            if p % 2:
                tile = pltpu.roll(tile, hd, 1)
            out.append(jnp.where(lane < hd, tile, 0.0))
        return jnp.concatenate(out, axis=0).astype(jnp.bfloat16)

    def attend_late(i, owners):
        part_v[mt, i] = narrow(jnp.concatenate(
            attend([(spread(owner), shift_of(owner), send, owner) for owner in owners]), axis=0
        ))

    def combine(parts):
        total = parts[0]
        acc = pltpu.roll(total, hd, 1)
        for m in parts[1:]:
            total = total + jnp.exp(acc) * m
            acc = acc + pltpu.roll(m, hd, 1)
        return jnp.where(late_lane < hd, pltpu.roll(acc, hd, 1), total)

    def send_late(i, owners, slot):
        wait_bytes(part_v.at[pl.ds(0, tp - 1), i], precv_sem.at[i])
        block = combine([widen(part_v.at[j, i]) for j in range(tp - 1, -1, -1)])
        late_b[i] = narrow(block).reshape(late_b.shape[1:])
        for j, owner in enumerate(owners):
            late_copy(i, j, owner, mt, (0, slot)).start()

    def send_urgent(i, owners):
        wait_bytes(part_v.at[0, i], precv_sem.at[i])
        block = combine([widen(part_v.at[mt, i]), widen(part_v.at[mt - 1, i])])
        late_b[i] = narrow(block).reshape(late_b.shape[1:])
        for j, owner in enumerate(owners):
            for t in range(tp):
                late_copy(i, j, owner, t, (mt // 2, me - quarter)).start()

    owners = inward + urgent + relaxed
    owners = [owners[i:i + 2] for i in range(0, 3 * quarter, 2)]
    first = quarter // 2

    def attend_class(place):
        wait_bytes(q_all.at[pl.ds(0, quarter)], qrecv_sem.at[place])
        for i in range(place * first, (place + 1) * first):
            attend_late(i, owners[i])
            if place != 1:
                for t in range(1, tp):
                    part_copy(i, lax.rem(mt + t, tp)).start()
            else:

                @pl.when(lead == 0)
                def _():
                    part_copy(i, mt + 1).start()

    @pl.when(inner)
    def _():
        attend_class(1)

    attend_class(0)

    @pl.when(inner)
    def _():
        attend_class(2)

    @pl.when(jnp.logical_and(inner, lead == 0))
    def _():
        send_blocks(far_inner, first)

    @pl.when(jnp.logical_and(inner, lead == 1))
    def _():
        for i in range(first, 2 * first):
            send_urgent(i, owners[i])
        send_blocks(far_inner, first)
        send_blocks(near_base, quarter)

    landed = [me] + same
    wait_bytes(recv.at[pl.ds(0, quarter - 1)], recv_sem.at[0])
    for i in range(0, quarter, 2):
        attend_blocks(landed[i:i + 2])

    def attend_early():
        wait_bytes(recv.at[pl.ds(0, quarter)], recv_sem.at[1])
        for i in range(0, quarter, 2):
            attend_blocks(early[i:i + 2])

    @pl.when(home)
    def _():
        attend_early()

    for i in range(first):
        send_late(i, owners[i], lax.rem(me, half))

    @pl.when(inner)
    def _():
        for i in range(2 * first, 3 * first):
            send_late(i, owners[i], me - quarter)
        send_blocks(far_inner + first, quarter - first)

    @pl.when(jnp.logical_not(home))
    def _():
        attend_early()

    some = pl.ds(0, half)
    others = pl.ds(0, tp - 1)

    @pl.when(home)
    def _():
        wait_bytes(late_in, lrecv_sem)
        for i in range(half):
            for k in range(chips):
                msg[2 * k + 1, quarter + i] = widen(late_in.at[k, i])

    @pl.when(jnp.logical_not(home))
    def _():
        wait_bytes(late_in.at[0], lrecv_sem)
        base = jnp.where(outer, quarter, (1 - top) * half)
        for i in range(half):
            msg[tp - 1, base + i] = widen(late_in.at[0, i])

    wait_bytes(send.at[pl.ds(0, sp - 1)], send_sem)
    wait_bytes(part_v.at[others, pl.ds(0, first)], send_sem)
    wait_bytes(late_b.at[pl.ds(0, first)], send_sem)

    @pl.when(inner)
    def _():
        wait_bytes(part_v.at[others, pl.ds(2 * first, first)], send_sem)
        wait_bytes(late_b.at[pl.ds(2 * first, first)], send_sem)

        @pl.when(lead == 0)
        def _():
            wait_bytes(part_v.at[0, pl.ds(first, first)], send_sem)

        @pl.when(lead == 1)
        def _():
            for _ in range(tp):
                wait_bytes(late_b.at[pl.ds(first, first)], send_sem)

    @pl.when(lead == 1)
    def _():
        wait_bytes(q_all, send_sem)

    wait_bytes(msg.at[others, some], send_sem)
    wait_bytes(msg.at[others, some], mrecv_sem)
    wait_bytes(recv.at[some], recv_sem.at[2])


def finish(sp, tp, hd, group, pairs, recv, msg, stored_hbm, first_hbm, fin, first_v, out_sem, first_sem):
    copies = [
        pltpu.make_async_copy(recv.at[b, :, pl.ds(p * 2 * hd, 2 * hd)], stored_hbm.at[p, b], out_sem)
        for b in range(sp)
        for p in range(pairs)
    ]
    for copy in copies:
        copy.start()
    left_half = lax.broadcasted_iota(jnp.int32, (packed_rows(pairs, group), 2 * hd), 1) < hd

    def add_block(i, carry):
        total, acc = carry
        b = sp - 1 - i
        for j in range(tp - 1, -1, -1):
            m = msg[j, b]
            total = total + jnp.exp(acc) * m
            acc = acc + pltpu.roll(m, hd, 1)
        return total, acc

    zero = jnp.zeros((packed_rows(pairs, group), 2 * hd), jnp.float32)
    total, _ = lax.fori_loop(0, sp, add_block, (zero, zero), unroll=True)
    total = jnp.where(left_half, 0.0, total)
    squares = jnp.sum(total * total, axis=1, keepdims=True) * (1.0 / hd)
    fin[...] = pltpu.roll(total * lax.rsqrt(squares + EPS_NORM), hd, 1)
    cols = [fin[pl.ds(g, pairs, stride=group), :][:, :hd] for g in range(group)]
    first_v[...] = jnp.concatenate(cols, axis=1).astype(first_v.dtype)
    first_copy = pltpu.make_async_copy(first_v, first_hbm, first_sem)
    first_copy.start()

    pltpu.make_async_copy(recv, recv, out_sem).wait()
    first_copy.wait()


def solution(mesh):
    sp, tp = mesh.shape["sp"], mesh.shape["tp"]

    def per_device(layer_input, key_weight, value_weight, queries, head_bias):
        seqs, sub, width = layer_input.shape
        pairs, group, hd = queries.shape
        kvh = head_bias.shape[0]
        x = layer_input.reshape(seqs * sub, width)
        block = pairs * 2 * hd
        any_spec = pl.BlockSpec(memory_space=pltpu.HBM)
        dma = pltpu.SemaphoreType.DMA
        handed = sp * sub * block * 2 + tp * sp * packed_rows(pairs, group) * 2 * hd * 4
        limit = VMEM_BYTES - handed
        late = sp // 4 * 3 // 2
        vmem_spec = pl.BlockSpec(memory_space=pltpu.VMEM)
        recv, msg = pl.pallas_call(
            functools.partial(kernel, sp, tp, seqs, sub, hd, kvh, group, pairs),
            out_shape=(
                pltpu.VMEM((sp, sub, block), jnp.bfloat16),
                pltpu.VMEM((tp, sp, packed_rows(pairs, group), 2 * hd), jnp.float32),
            ),
            in_specs=[any_spec] * 5,
            out_specs=(vmem_spec, vmem_spec),
            scratch_shapes=[
                pltpu.VMEM(x.shape, jnp.bfloat16),
                pltpu.VMEM((width, 2 * key_weight.shape[1]), jnp.bfloat16),
                pltpu.VMEM((group, pairs, hd), jnp.bfloat16),
                pltpu.VMEM(head_bias.shape, jnp.float32),
                pltpu.VMEM((sp, sub, block), jnp.bfloat16),
                pltpu.VMEM((pairs * ROWS, 2 * hd), jnp.bfloat16),
                pltpu.VMEM(((pairs + 1) // 2 * ROWS, 2 * hd), jnp.bfloat16),
                pltpu.VMEM((sp, (pairs + 1) // 2 * ROWS, 2 * hd), jnp.bfloat16),
                pltpu.VMEM((tp, late, 2 * packed_rows(pairs, group), 2 * hd), jnp.bfloat16),
                pltpu.VMEM((late, 2, packed_rows(pairs, group), 2 * hd), jnp.bfloat16),
                pltpu.VMEM((tp // 2, sp // 2, packed_rows(pairs, group), 2 * hd), jnp.bfloat16),
                dma((KC + 1,)),
                dma((KC,)),
                dma((2,)),
                dma(()),
                dma((3,)),
                dma(()),
                dma((3,)),
                dma((late,)),
                dma(()),
            ],
            compiler_params=pltpu.CompilerParams(
                collective_id=0, has_side_effects=True, vmem_limit_bytes=limit
            ),
        )(x, key_weight, value_weight, queries.transpose(1, 0, 2), head_bias)
        return pl.pallas_call(
            functools.partial(finish, sp, tp, hd, group, pairs),
            out_shape=(
                jax.ShapeDtypeStruct((pairs, sp, sub, 2 * hd), jnp.bfloat16),
                jax.ShapeDtypeStruct((pairs, group * hd), jnp.bfloat16),
            ),
            in_specs=[vmem_spec, vmem_spec],
            out_specs=(any_spec, any_spec),
            scratch_shapes=[
                pltpu.VMEM((packed_rows(pairs, group), 2 * hd), jnp.float32),
                pltpu.VMEM((pairs, group * hd), jnp.bfloat16),
                dma(()),
                dma(()),
            ],
            compiler_params=pltpu.CompilerParams(vmem_limit_bytes=VMEM_BYTES // 4),
        )(recv, msg)

    in_specs = (P(None, ("sp", "tp"), None), P(), P(), P("sp", None, None), P())
    out_specs = (P("sp", None, "tp", None), P("sp", None))
    return jax.shard_map(per_device, mesh=mesh, in_specs=in_specs, out_specs=out_specs, check_vma=False)
```

```python
import functools
import math

import jax
import jax.numpy as jnp
from jax import lax
from jax.experimental import pallas as pl
from jax.experimental.pallas import tpu as pltpu
from jax.sharding import PartitionSpec as P

EPS_NORM = 0.0001
MESH = pl.DeviceIdType.MESH
EDGES = (0, 2, 5, 8)
KC = len(EDGES) - 1
VMEM_BYTES = 60 * 1024 * 1024
ROWS = 8


def flip(index, k):
    bit = 1
    while bit <= k:
        if k & bit:
            index = index + (1 - 2 * ((index // bit) % 2)) * bit
        bit *= 2
    return index


def packed_rows(pairs, group):
    return pairs * group // 8 * 8 + 8


def kernel(
    sp, tp, seqs, sub, hd, kvh, group, pairs,
    x_hbm, wk_hbm, wv_hbm, q_hbm, bias_hbm,
    recv, msg,
    x_v, w_v, q_v, bias_v, send, q_pad, q_msg, q_all, part_v, late_b, late_in,
    x_sem, w_sem, small_sem, send_sem, recv_sem, mrecv_sem, qrecv_sem, precv_sem, lrecv_sem,
):
    me = lax.axis_index("sp")
    mt = lax.axis_index("tp")
    per_seq = kvh // pairs
    width = x_hbm.shape[1]
    edges = [width * e // 8 for e in EDGES]
    lead_seqs = sp // 4 // per_seq
    lead_rows = lead_seqs * sub

    q_copy = pltpu.make_async_copy(q_hbm, q_v, small_sem.at[0])
    bias_copy = pltpu.make_async_copy(bias_hbm, bias_v, small_sem.at[1])
    q_copy.start()
    bias_copy.start()
    kv_width = wk_hbm.shape[1]

    def x_copy(c):
        at = (pl.ds(0, lead_rows), pl.ds(edges[c], edges[c + 1] - edges[c]))
        return pltpu.make_async_copy(x_hbm.at[at], x_v.at[at], x_sem.at[c])

    def w_copy(i, c):
        rows = pl.ds(edges[c], edges[c + 1] - edges[c])
        w_hbm = (wk_hbm, wv_hbm)[i]
        return pltpu.make_async_copy(w_hbm.at[rows], w_v.at[rows, pl.ds(i * kv_width, kv_width)], w_sem.at[c])

    rest = pl.ds(lead_rows, seqs * sub - lead_rows)
    x_rest = pltpu.make_async_copy(x_hbm.at[rest], x_v.at[rest], x_sem.at[KC])
    for c in range(KC):
        x_copy(c).start()
        w_copy(0, c).start()
        w_copy(1, c).start()
    x_rest.start()

    msg[...] = jnp.zeros_like(msg)

    top = me // (sp // 2)
    half = sp // 2
    quarter = sp // 4
    lead = lax.rem(mt, 2)
    outer = lax.rem(me // quarter, 3) == 0
    inner = jnp.logical_not(outer)
    home = me // quarter == 0
    chips = tp // 2
    far_outer = (1 - top) * 3 * quarter
    far_inner = quarter + (1 - top) * quarter
    near = [flip(me, k) for k in range(quarter, half)]
    inward = [far_inner + flip(lax.rem(me, 2), j) for j in range(quarter)]
    outward = [far_outer + flip(lax.rem(me, 2), j) for j in range(quarter)]
    same = [flip(me, k) for k in range(1, quarter)]
    early = [jnp.where(outer, a, b) for a, b in zip(outward, near)]
    late = [jnp.where(outer, a, b) for a, b in zip(near, outward)]
    urgent = [jnp.where(top == 0, a, b) for a, b in zip(near, outward)]
    relaxed = [jnp.where(top == 0, a, b) for a, b in zip(outward, near)]

    barrier = pltpu.get_barrier_semaphore()
    for k in range(sp - 1, 0, -1):
        pl.semaphore_signal(barrier, inc=1, device_id={"sp": flip(me, k)}, device_id_type=MESH)
    for k in range(1, tp):
        pl.semaphore_signal(barrier, inc=1, device_id={"tp": lax.rem(mt + k, tp)}, device_id_type=MESH)

    @pl.when(home)
    def _():
        for t in range(1, tp, 2):
            for to in range(quarter, 3 * quarter):

                @pl.when(t != mt)
                def _():
                    pl.semaphore_signal(barrier, inc=1, device_id={"sp": to, "tp": t}, device_id_type=MESH)

    def ask(owners):
        for owner in owners:
            pl.semaphore_signal(barrier, inc=1, device_id={"sp": owner, "tp": mt + 1}, device_id_type=MESH)

    @pl.when(lead == 0)
    def _():
        ask(inward)

        @pl.when(inner)
        def _():
            ask(near + outward)

    def wait_bytes(ref, sem):
        pltpu.make_async_copy(ref, ref, sem).wait()

    def pack(rows, base):
        for i in range(rows.shape[0] // sub):
            for part in range(per_seq):
                out = []
                for p in range(pairs):
                    c0 = (part * pairs + p) * hd
                    out.append(rows[i * sub:(i + 1) * sub, c0:c0 + hd])
                    out.append(rows[i * sub:(i + 1) * sub, kv_width + c0:kv_width + c0 + hd])
                send[base + i * per_seq + part] = jnp.concatenate(out, axis=1).astype(jnp.bfloat16)

    def send_block(to):
        near_class = jnp.where(outer, 1, 2)
        place = jnp.where(to // half == top, near_class, jnp.where(to // quarter == far_outer // quarter, near_class, 2))
        place = jnp.where(to // quarter == me // quarter, 0, place)

        @pl.when(to != me)
        def _():
            pltpu.make_async_remote_copy(
                src_ref=send.at[to], dst_ref=recv.at[me],
                send_sem=send_sem, recv_sem=recv_sem.at[place],
                device_id={"sp": to}, device_id_type=MESH,
            ).start()

    def send_blocks(base, count):
        for j in range(count):
            send_block(base + j)

    def query_copy(to, core, place):
        return pltpu.make_async_remote_copy(
            src_ref=q_msg, dst_ref=q_all.at[me],
            send_sem=send_sem, recv_sem=qrecv_sem.at[place],
            device_id={"sp": to, "tp": mt - core}, device_id_type=MESH,
        )

    def enter():
        pl.semaphore_wait(barrier, sp + tp - 2 + lead * (half + jnp.where(inner, quarter * (tp - 1), 0)))

        @pl.when(lead == 1)
        def _():
            for group_of in (inward, late):
                for core in range(2):
                    for to in group_of:
                        query_copy(to, core, jnp.where(outer, 1 + top, 0)).start()

    def prepare_queries():
        q_copy.wait()
        blank = jnp.zeros((group, hd), jnp.float32)
        q_rows = [q_v[:, p, :].astype(jnp.float32) for p in range(pairs)] + [blank]
        below = jnp.zeros((ROWS - group, 2 * hd), jnp.float32)

        def q_tile(left, right):
            tile = jnp.concatenate([left, right], axis=1)
            return jnp.concatenate([tile, below], axis=0).astype(jnp.bfloat16)

        for p in range(0, pairs, 2):
            q_msg[p // 2 * ROWS:(p // 2 + 1) * ROWS, :] = q_tile(q_rows[p], q_rows[p + 1])
        for p in range(pairs):
            q_pad[p * ROWS:(p + 1) * ROWS, :] = q_tile(q_rows[p], blank)

    rows = None
    for c in range(KC):
        x_copy(c).wait()
        wait_bytes(w_v.at[pl.ds(edges[c], edges[c + 1] - edges[c])], w_sem.at[c])
        part = jnp.dot(
            x_v[:lead_rows, edges[c]:edges[c + 1]], w_v[edges[c]:edges[c + 1], :],
            preferred_element_type=jnp.float32,
        )
        rows = part if rows is None else rows + part
        if c == 0:
            prepare_queries()
    pack(rows, 0)

    @pl.when(top == 1)
    def _():
        enter()
        send_blocks(far_outer, quarter)

    x_rest.wait()
    pack(jnp.dot(x_v[lead_rows:, :], w_v[...], preferred_element_type=jnp.float32), quarter)

    @pl.when(top == 0)
    def _():
        enter()

    own_base = me // quarter * quarter
    near_base = top * half + quarter - lax.rem(me // quarter, 2) * quarter
    send_blocks(own_base, quarter)

    @pl.when(jnp.logical_or(outer, lead == 0))
    def _():
        send_blocks(near_base, quarter)


    @pl.when(top == 0)
    def _():
        send_blocks(far_outer, quarter)

    @pl.when(outer)
    def _():
        send_blocks(far_inner, quarter)

    recv[pl.ds(me, 1)] = send[pl.ds(me, 1)]

    bias_copy.wait()
    eye = lax.broadcasted_iota(jnp.int32, (ROWS, group), 0) == lax.broadcasted_iota(jnp.int32, (ROWS, group), 1)

    def shift_of(owner):
        h0 = lax.rem(owner * pairs, kvh)
        shifts = []
        for p in range(pairs):
            row = bias_v[pl.ds(h0 + p, 1), :]
            shifts.append(jnp.sum(jnp.where(eye, jnp.broadcast_to(row, (ROWS, group)), 0.0), axis=1, keepdims=True))
        return jnp.concatenate(shifts, axis=0)

    scale = 1.0 / math.sqrt(hd)
    later = lax.broadcasted_iota(jnp.int32, (sub, 256), 0)
    column = lax.broadcasted_iota(jnp.int32, (sub, 256), 1)
    tri = ((later > column) | (column >= 128)).astype(jnp.float32).astype(jnp.bfloat16)
    left_half = lax.broadcasted_iota(jnp.int32, (pairs * ROWS, 2 * hd), 1) < hd

    late_lane = lax.broadcasted_iota(jnp.int32, (2 * packed_rows(pairs, group), 2 * hd), 1)

    def msg_copy(b, t):
        return pltpu.make_async_remote_copy(
            src_ref=msg.at[mt, b], dst_ref=msg.at[mt, b],
            send_sem=send_sem, recv_sem=mrecv_sem,
            device_id={"tp": t}, device_id_type=MESH,
        )

    def part_copy(i, t):
        return pltpu.make_async_remote_copy(
            src_ref=part_v.at[mt, i], dst_ref=part_v.at[mt, i],
            send_sem=send_sem, recv_sem=precv_sem.at[i],
            device_id={"tp": t}, device_id_type=MESH,
        )

    def late_copy(i, j, to, there, slot):
        return pltpu.make_async_remote_copy(
            src_ref=late_b.at[i, j], dst_ref=late_in.at[slot],
            send_sem=send_sem, recv_sem=lrecv_sem,
            device_id={"sp": to, "tp": there}, device_id_type=MESH,
        )

    def attend(items):
        scores = []
        shifts = []
        for queries, shift, rows, b in items:
            shifts.append(shift)
            for p in range(pairs):
                q = queries[p * ROWS:(p + 1) * ROWS, :]
                kv = rows[b, :, p * 2 * hd:(p + 1) * 2 * hd]
                scores.append(lax.dot_general(q, kv, (((1,), (1,)), ((), ())), preferred_element_type=jnp.float32))
        s = jnp.concatenate(scores, axis=0) * scale + jnp.concatenate(shifts, axis=0)
        low = jnp.log1p(jnp.exp(-jnp.abs(s)))
        keep = -(jnp.maximum(s, 0.0) + low)
        sig = jnp.minimum(s, 0.0) - low
        hi = keep.astype(jnp.bfloat16)
        rest = keep - hi.astype(jnp.float32)
        mid = rest.astype(jnp.bfloat16)
        lo = (rest - mid.astype(jnp.float32)).astype(jnp.bfloat16)
        sums = (
            jnp.dot(hi, tri, preferred_element_type=jnp.float32)
            + jnp.dot(mid, tri, preferred_element_type=jnp.float32)
            + jnp.dot(lo, tri, preferred_element_type=jnp.float32)
        )
        weights = jnp.exp(sig + sums[:, :sub]).astype(jnp.bfloat16)
        n = pairs * ROWS
        out = []
        for i, (_, _, rows, b) in enumerate(items):
            reads = []
            for p in range(pairs):
                kv = rows[b, :, p * 2 * hd:(p + 1) * 2 * hd]
                at = i * n + p * ROWS
                reads.append(jnp.dot(weights[at:at + ROWS], kv, preferred_element_type=jnp.float32))
            read = jnp.concatenate(reads, axis=0)
            both = jnp.where(left_half, sums[i * n:(i + 1) * n, 128:128 + 2 * hd], read)
            packed = [both[p * ROWS:p * ROWS + group] for p in range(pairs)]
            packed.append(jnp.zeros((packed_rows(pairs, group) - pairs * group, 2 * hd), jnp.float32))
            out.append(jnp.concatenate(packed, axis=0))
        return out

    shift = shift_of(me)

    def attend_blocks(blocks):
        for b, m in zip(blocks, attend([(q_pad, shift, recv, b) for b in blocks])):
            msg[mt, b] = m
            for t in range(1, tp):
                msg_copy(b, lax.rem(mt + t, tp)).start()

    def narrow(block):
        lane = late_lane[:block.shape[0]]
        high = block.astype(jnp.bfloat16).astype(jnp.float32)
        keep = jnp.where(lane < hd // 2, high, block - high)
        return jnp.where(lane < hd, keep, block).astype(jnp.bfloat16)

    def widen(ref):
        m = ref[...].astype(jnp.float32)
        lane = late_lane[:m.shape[0]]
        other = jnp.where(lane < hd // 2, pltpu.roll(m, 2 * hd - hd // 2, 1), pltpu.roll(m, hd // 2, 1))
        return jnp.where(lane < hd, m + other, m)

    def spread(owner):
        tiles = q_all[owner].astype(jnp.float32)
        lane = lax.broadcasted_iota(jnp.int32, (ROWS, 2 * hd), 1)
        out = []
        for p in range(pairs):
            tile = tiles[p // 2 * ROWS:(p // 2 + 1) * ROWS]
            if p % 2:
                tile = pltpu.roll(tile, hd, 1)
            out.append(jnp.where(lane < hd, tile, 0.0))
        return jnp.concatenate(out, axis=0).astype(jnp.bfloat16)

    def attend_late(i, owners):
        part_v[mt, i] = narrow(jnp.concatenate(
            attend([(spread(owner), shift_of(owner), send, owner) for owner in owners]), axis=0
        ))

    def combine(parts):
        total = parts[0]
        acc = pltpu.roll(total, hd, 1)
        for m in parts[1:]:
            total = total + jnp.exp(acc) * m
            acc = acc + pltpu.roll(m, hd, 1)
        return jnp.where(late_lane < hd, pltpu.roll(acc, hd, 1), total)

    def send_late(i, owners, slot):
        wait_bytes(part_v.at[pl.ds(0, tp - 1), i], precv_sem.at[i])
        block = combine([widen(part_v.at[j, i]) for j in range(tp - 1, -1, -1)])
        late_b[i] = narrow(block).reshape(late_b.shape[1:])
        for j, owner in enumerate(owners):
            late_copy(i, j, owner, mt, (0, slot)).start()

    def send_urgent(i, owners):
        wait_bytes(part_v.at[0, i], precv_sem.at[i])
        block = combine([widen(part_v.at[mt, i]), widen(part_v.at[mt - 1, i])])
        late_b[i] = narrow(block).reshape(late_b.shape[1:])
        for j, owner in enumerate(owners):
            for t in range(tp):
                late_copy(i, j, owner, t, (mt // 2, me - quarter)).start()

    owners = inward + urgent + relaxed
    owners = [owners[i:i + 2] for i in range(0, 3 * quarter, 2)]
    first = quarter // 2

    def attend_class(place):
        wait_bytes(q_all.at[pl.ds(0, quarter)], qrecv_sem.at[place])
        for i in range(place * first, (place + 1) * first):
            attend_late(i, owners[i])
            if place != 1:
                for t in range(1, tp):
                    part_copy(i, lax.rem(mt + t, tp)).start()
            else:

                @pl.when(lead == 0)
                def _():
                    part_copy(i, mt + 1).start()

    @pl.when(inner)
    def _():
        attend_class(1)

    attend_class(0)

    @pl.when(inner)
    def _():
        attend_class(2)

    @pl.when(jnp.logical_and(inner, lead == 1))
    def _():
        for i in range(first, 2 * first):
            send_urgent(i, owners[i])
        send_blocks(near_base, quarter)

    @pl.when(inner)
    def _():
        send_blocks(far_inner, first)

    landed = [me] + same
    wait_bytes(recv.at[pl.ds(0, quarter - 1)], recv_sem.at[0])
    for i in range(0, quarter, 2):
        attend_blocks(landed[i:i + 2])

    def attend_early():
        wait_bytes(recv.at[pl.ds(0, quarter)], recv_sem.at[1])
        for i in range(0, quarter, 2):
            attend_blocks(early[i:i + 2])

    @pl.when(home)
    def _():
        attend_early()

    for i in range(first):
        send_late(i, owners[i], lax.rem(me, half))

    @pl.when(inner)
    def _():
        for i in range(2 * first, 3 * first):
            send_late(i, owners[i], me - quarter)
        send_blocks(far_inner + first, quarter - first)

    @pl.when(jnp.logical_not(home))
    def _():
        attend_early()

    some = pl.ds(0, half)
    others = pl.ds(0, tp - 1)

    @pl.when(home)
    def _():
        wait_bytes(late_in, lrecv_sem)
        for i in range(half):
            for k in range(chips):
                msg[2 * k + 1, quarter + i] = widen(late_in.at[k, i])

    @pl.when(jnp.logical_not(home))
    def _():
        wait_bytes(late_in.at[0], lrecv_sem)
        base = jnp.where(outer, quarter, (1 - top) * half)
        for i in range(half):
            msg[tp - 1, base + i] = widen(late_in.at[0, i])

    wait_bytes(send.at[pl.ds(0, sp - 1)], send_sem)
    wait_bytes(part_v.at[others, pl.ds(0, first)], send_sem)
    wait_bytes(late_b.at[pl.ds(0, first)], send_sem)

    @pl.when(inner)
    def _():
        wait_bytes(part_v.at[others, pl.ds(2 * first, first)], send_sem)
        wait_bytes(late_b.at[pl.ds(2 * first, first)], send_sem)

        @pl.when(lead == 0)
        def _():
            wait_bytes(part_v.at[0, pl.ds(first, first)], send_sem)

        @pl.when(lead == 1)
        def _():
            for _ in range(tp):
                wait_bytes(late_b.at[pl.ds(first, first)], send_sem)

    @pl.when(lead == 1)
    def _():
        wait_bytes(q_all, send_sem)

    wait_bytes(msg.at[others, some], send_sem)
    wait_bytes(msg.at[others, some], mrecv_sem)
    wait_bytes(recv.at[some], recv_sem.at[2])


def finish(sp, tp, hd, group, pairs, recv, msg, stored_hbm, first_hbm, fin, first_v, out_sem, first_sem):
    copies = [
        pltpu.make_async_copy(recv.at[b, :, pl.ds(p * 2 * hd, 2 * hd)], stored_hbm.at[p, b], out_sem)
        for b in range(sp)
        for p in range(pairs)
    ]
    for copy in copies:
        copy.start()
    left_half = lax.broadcasted_iota(jnp.int32, (packed_rows(pairs, group), 2 * hd), 1) < hd

    def add_block(i, carry):
        total, acc = carry
        b = sp - 1 - i
        for j in range(tp - 1, -1, -1):
            m = msg[j, b]
            total = total + jnp.exp(acc) * m
            acc = acc + pltpu.roll(m, hd, 1)
        return total, acc

    zero = jnp.zeros((packed_rows(pairs, group), 2 * hd), jnp.float32)
    total, _ = lax.fori_loop(0, sp, add_block, (zero, zero), unroll=True)
    total = jnp.where(left_half, 0.0, total)
    squares = jnp.sum(total * total, axis=1, keepdims=True) * (1.0 / hd)
    fin[...] = pltpu.roll(total * lax.rsqrt(squares + EPS_NORM), hd, 1)
    cols = [fin[pl.ds(g, pairs, stride=group), :][:, :hd] for g in range(group)]
    first_v[...] = jnp.concatenate(cols, axis=1).astype(first_v.dtype)
    first_copy = pltpu.make_async_copy(first_v, first_hbm, first_sem)
    first_copy.start()

    pltpu.make_async_copy(recv, recv, out_sem).wait()
    first_copy.wait()


def solution(mesh):
    sp, tp = mesh.shape["sp"], mesh.shape["tp"]

    def per_device(layer_input, key_weight, value_weight, queries, head_bias):
        seqs, sub, width = layer_input.shape
        pairs, group, hd = queries.shape
        kvh = head_bias.shape[0]
        x = layer_input.reshape(seqs * sub, width)
        block = pairs * 2 * hd
        any_spec = pl.BlockSpec(memory_space=pltpu.HBM)
        dma = pltpu.SemaphoreType.DMA
        handed = sp * sub * block * 2 + tp * sp * packed_rows(pairs, group) * 2 * hd * 4
        limit = VMEM_BYTES - handed
        late = sp // 4 * 3 // 2
        vmem_spec = pl.BlockSpec(memory_space=pltpu.VMEM)
        recv, msg = pl.pallas_call(
            functools.partial(kernel, sp, tp, seqs, sub, hd, kvh, group, pairs),
            out_shape=(
                pltpu.VMEM((sp, sub, block), jnp.bfloat16),
                pltpu.VMEM((tp, sp, packed_rows(pairs, group), 2 * hd), jnp.float32),
            ),
            in_specs=[any_spec] * 5,
            out_specs=(vmem_spec, vmem_spec),
            scratch_shapes=[
                pltpu.VMEM(x.shape, jnp.bfloat16),
                pltpu.VMEM((width, 2 * key_weight.shape[1]), jnp.bfloat16),
                pltpu.VMEM((group, pairs, hd), jnp.bfloat16),
                pltpu.VMEM(head_bias.shape, jnp.float32),
                pltpu.VMEM((sp, sub, block), jnp.bfloat16),
                pltpu.VMEM((pairs * ROWS, 2 * hd), jnp.bfloat16),
                pltpu.VMEM(((pairs + 1) // 2 * ROWS, 2 * hd), jnp.bfloat16),
                pltpu.VMEM((sp, (pairs + 1) // 2 * ROWS, 2 * hd), jnp.bfloat16),
                pltpu.VMEM((tp, late, 2 * packed_rows(pairs, group), 2 * hd), jnp.bfloat16),
                pltpu.VMEM((late, 2, packed_rows(pairs, group), 2 * hd), jnp.bfloat16),
                pltpu.VMEM((tp // 2, sp // 2, packed_rows(pairs, group), 2 * hd), jnp.bfloat16),
                dma((KC + 1,)),
                dma((KC,)),
                dma((2,)),
                dma(()),
                dma((3,)),
                dma(()),
                dma((3,)),
                dma((late,)),
                dma(()),
            ],
            compiler_params=pltpu.CompilerParams(
                collective_id=0, has_side_effects=True, vmem_limit_bytes=limit
            ),
        )(x, key_weight, value_weight, queries.transpose(1, 0, 2), head_bias)
        return pl.pallas_call(
            functools.partial(finish, sp, tp, hd, group, pairs),
            out_shape=(
                jax.ShapeDtypeStruct((pairs, sp, sub, 2 * hd), jnp.bfloat16),
                jax.ShapeDtypeStruct((pairs, group * hd), jnp.bfloat16),
            ),
            in_specs=[vmem_spec, vmem_spec],
            out_specs=(any_spec, any_spec),
            scratch_shapes=[
                pltpu.VMEM((packed_rows(pairs, group), 2 * hd), jnp.float32),
                pltpu.VMEM((pairs, group * hd), jnp.bfloat16),
                dma(()),
                dma(()),
            ],
            compiler_params=pltpu.CompilerParams(vmem_limit_bytes=VMEM_BYTES // 4),
        )(recv, msg)

    in_specs = (P(None, ("sp", "tp"), None), P(), P(), P("sp", None, None), P())
    out_specs = (P("sp", None, "tp", None), P("sp", None))
    return jax.shard_map(per_device, mesh=mesh, in_specs=in_specs, out_specs=out_specs, check_vma=False)
```
